512 devices in a mesh: dp: 4 (over x), kv: 64 (over z, y), tp: 2 (over core).
Axes of the slice: x: 4, y: 8, z: 8, core: 2. Of those that a mesh axis runs over, the one named last changes fastest.
Arguments:
- tokens: bfloat16 [512, 4, 4096], P('dp', None, 'kv'), may hold values from -260 to 260
- norm_gain: bfloat16 [4096], replicated, may hold values from 0.099609375 to 1.8984375
- query_weight: bfloat16 [4096, 2048], P(None, ('tp', 'kv')), may hold values from -0.09375 to 0.09375
- key_weight: bfloat16 [4096, 2048], P(None, ('tp', 'kv')), may hold values from -0.09375 to 0.09375
- value_weight: bfloat16 [4096, 4096], P(None, ('tp', 'kv')), may hold values from -0.09375 to 0.09375
- gate_weight: bfloat16 [4096, 4096], P(None, ('tp', 'kv')), may hold values from -0.09375 to 0.09375
- out_weight: bfloat16 [4096, 4096], P('tp', 'kv'), may hold values from -0.09375 to 0.09375
- decay_rate: float32 [16], P('tp'), may hold values from 0.02 to 1
- prior_state: float32 [512, 16, 128, 256], P(('dp', 'kv'), 'tp'), may hold values from -0.6 to 0.6
- last_keys: bfloat16 [512, 4, 16, 128], P(('dp', 'kv'), None, 'tp'), may hold values from -0.5390625 to 0.5390625
- last_values: bfloat16 [512, 4, 16, 256], P(('dp', 'kv'), None, 'tp'), may hold values from -6 to 6
- accepted: int32 [512], P(('dp', 'kv')), may hold values from 0 to 4
- lengths: int32 [512], P(('dp', 'kv')), may hold values from 16 to 99999
Outputs:
- retained: bfloat16 [512, 4, 4096], P('dp', None, ('kv', 'tp'))
- new_state: float32 [512, 16, 128, 256], P(('dp', 'kv'), 'tp')
- new_keys: bfloat16 [512, 4, 16, 128], P(('dp', 'kv'), None, 'tp')
- new_values: bfloat16 [512, 4, 16, 256], P(('dp', 'kv'), None, 'tp')
The draws below stay inside these ranges and needn't reach their ends.
Inputs may be any that keep to these rules, and one draw needn't show every extreme that they name: `accepted`: how many of the last step's 4 proposals were taken.
All inputs are finite; a program needn't handle non-finite values.
Results may differ from the reference program's by a relative error of at most 0.012.
Values may be sent and summed in bfloat16 or wider, within the bound.
A program may use at most 64 MiB of HBM per device.

```python
import math
import jax
import jax.numpy as jnp
from jax import lax

D = 4096
HEADS = 16
HEAD_K = 128
HEAD_V = 256
PROPOSALS = 4
SEQS = 512
N_TP = 2


def draw_tokens(key, part):
    first_key, second_key, third_key = jax.random.split(jax.random.fold_in(key, 11), 3)
    base = jax.random.normal(first_key, (SEQS, PROPOSALS, D), jnp.float32)
    base = jnp.clip(base, -6.0, 6.0)
    row_scales = jnp.exp(jax.random.uniform(second_key, (SEQS, PROPOSALS, 1), jnp.float32, 0.0, math.log(10.0)))
    ramp = jnp.exp(math.log(3.0) * jnp.arange(D, dtype=jnp.float32) / D)
    column_scales = jnp.exp(jax.random.uniform(third_key, (D,), jnp.float32, -0.35, 0.35))
    return (base * row_scales * ramp * column_scales).astype(jnp.bfloat16)


def plant(entries, stream_key, low, top_value):
    place = [jax.random.randint(jax.random.fold_in(stream_key, axis), (), 0, length) for axis, length in enumerate(entries.shape)]
    longest = entries.shape.index(max(entries.shape))
    next_to = place[:longest] + [(place[longest] + 1) % entries.shape[longest]] + place[longest + 1:]
    return entries.at[tuple(place)].set(low).at[tuple(next_to)].set(top_value)


def levels(key, shape, shards, least, top_value):
    gain, own = 1.0, jax.random.fold_in(key, 6)
    for position, parts in shards:
        draws = jnp.exp(jax.random.uniform(jax.random.fold_in(own, position), (parts,), jnp.float32, least / len(shards), top_value / len(shards)))
        gain = gain * jnp.repeat(draws, shape[position] // parts).reshape([-1 if axis == position else 1 for axis in range(len(shape))])
    return gain


def scatter_about(key, shape, scale, bound, shards=(), kind=jnp.bfloat16):
    result = jax.random.normal(key, shape, jnp.float32) * scale
    if len(shards) > 0:
        result = levels(key, shape, shards, -0.22, 0.18) * result
    return jnp.clip(result, min=-bound, max=bound).astype(kind)


def setup_inputs(seed: int = 0) -> dict:
    keys = jax.random.split(jax.random.key(seed), 14)
    tokens = draw_tokens(jax.random.fold_in(keys[13], 71), 0)
    norm_gain = jnp.clip(1.0 + 0.18 * jax.random.normal(keys[1], (D,), jnp.float32), 0.099609375, 1.8984375).astype(jnp.bfloat16)
    query_weight = scatter_about(keys[2], (D, HEADS * HEAD_K), D ** -0.5, 0.09375, ((1, 128),))
    key_weight = scatter_about(keys[3], (D, HEADS * HEAD_K), D ** -0.5, 0.09375, ((1, 128),))
    value_weight = scatter_about(keys[4], (D, HEADS * HEAD_V), D ** -0.5, 0.09375, ((1, 128),))
    gate_weight = scatter_about(keys[5], (D, HEADS * HEAD_V), D ** -0.5, 0.09375, ((1, 128),))
    out_weight = scatter_about(keys[6], (HEADS * HEAD_V, D), (HEADS * HEAD_V) ** -0.5, 0.09375, ((0, 2), (1, 64)))
    decay_rate = jnp.clip(jnp.exp(math.log(1.0) - 3.912023 * jax.random.uniform(keys[7], (HEADS,), jnp.float32) ** levels(keys[7], (HEADS,), ((0, 2),), -0.2, 0.2)), 0.02, 1.0)
    prior_state = scatter_about(keys[8], (SEQS, HEADS, HEAD_K, HEAD_V), 0.1, 0.6, ((0, 256), (1, 2)), jnp.float32)
    last_keys = scatter_about(keys[9], (SEQS, PROPOSALS, HEADS, HEAD_K), 0.09, 0.5390625, ((0, 256), (2, 2)))
    last_values = scatter_about(keys[10], (SEQS, PROPOSALS, HEADS, HEAD_V), 1.0, 6.0, ((0, 256), (2, 2)))
    accepted = plant(jax.random.randint(keys[11], (SEQS,), 0, PROPOSALS + 1), jax.random.fold_in(keys[11], 1), 0, PROPOSALS).astype(jnp.int32)
    lengths = plant(jax.random.randint(keys[12], (SEQS,), 16, 100000), jax.random.fold_in(keys[12], 1), 16, 99999).astype(jnp.int32)
    return dict(tokens=tokens, norm_gain=norm_gain, query_weight=query_weight, key_weight=key_weight, value_weight=value_weight, gate_weight=gate_weight, out_weight=out_weight, decay_rate=decay_rate, prior_state=prior_state, last_keys=last_keys, last_values=last_values, accepted=accepted, lengths=lengths)


epsilon = 1e-06

def rotate(field_in, positions):
    half_size = field_in.shape[-1] // 2
    frequency = jnp.power(10000.0, -jnp.arange(half_size, dtype=jnp.float32) / half_size)
    angles = positions.astype(jnp.float32)[:, :, None, None] * frequency
    cosine, sine_part = (jnp.cos(angles), jnp.sin(angles))
    floats = field_in.astype(jnp.float32)
    first_half, second = (floats[..., :half_size], floats[..., half_size:])
    return jnp.concatenate([first_half * cosine - second * sine_part, first_half * sine_part + second * cosine], axis=-1)

def retain(query_rot, key_rot, value_rows, prior_state, last_keys, last_values, accepted, log_decay):
    highest = lax.Precision.HIGHEST
    proposals = query_rot.shape[1]
    step_ids = jnp.arange(proposals, dtype=jnp.int32)
    taken_mask = step_ids[None, :] < accepted[:, None]
    power_exp = jnp.maximum(accepted[:, None] - 1 - step_ids[None, :], 0).astype(jnp.float32)
    weight = jnp.where(taken_mask[:, :, None], jnp.exp(log_decay[None, None, :] * power_exp[:, :, None]), 0.0)
    carried = jnp.exp(log_decay[None, :] * accepted[:, None].astype(jnp.float32))
    weighted_keys = last_keys.astype(jnp.float32) * weight[..., None]
    taken_state = carried[:, :, None, None] * prior_state + jnp.einsum('sphd,sphe->shde', weighted_keys, last_values.astype(jnp.float32), precision=highest)
    scores = jnp.einsum('sthd,smhd->shtm', query_rot.astype(jnp.float32), key_rot.astype(jnp.float32), precision=highest)
    offset = (step_ids[:, None] - step_ids[None, :]).astype(jnp.float32)
    decay_grid = jnp.where(offset[None] >= 0.0, jnp.exp(log_decay[:, None, None] * jnp.maximum(offset, 0.0)[None]), 0.0)
    inner_sum = jnp.einsum('shtm,smhe->sthe', scores * decay_grid[None], value_rows.astype(jnp.float32), precision=highest)
    query_decay = jnp.exp(log_decay[None, :] * (step_ids[:, None].astype(jnp.float32) + 1.0))
    cross_sum = jnp.einsum('sthd,shde->sthe', query_rot.astype(jnp.float32) * query_decay[None, :, :, None], taken_state, precision=highest)
    return (inner_sum + cross_sum, taken_state)

def reference(tokens, norm_gain, query_weight, key_weight, value_weight, gate_weight, out_weight, decay_rate, prior_state, last_keys, last_values, accepted, lengths):
    seq_count, proposals, width = tokens.shape
    heads = decay_rate.shape[0]
    key_size = last_keys.shape[-1]
    value_size = last_values.shape[-1]
    floats = tokens.astype(jnp.float32)
    row_stat = lax.rsqrt(lax.optimization_barrier(jnp.mean(floats * floats, axis=-1)) + epsilon)
    normed = (floats * row_stat[..., None] * norm_gain.astype(jnp.float32)).astype(jnp.bfloat16)
    normed = normed.reshape(seq_count * proposals, width)

    def project(weight, last_size):
        product = jnp.dot(normed, weight, preferred_element_type=jnp.float32).astype(jnp.bfloat16)
        return product.reshape(seq_count, proposals, heads, last_size)
    query_rows = project(query_weight, key_size)
    key_rows = project(key_weight, key_size)
    value_rows = project(value_weight, value_size)
    gate_rows = project(gate_weight, value_size)
    positions = (lengths + accepted)[:, None] + jnp.arange(proposals, dtype=jnp.int32)[None, :]
    query_rot = rotate(query_rows, positions).astype(jnp.bfloat16)
    key_rot = (rotate(key_rows, positions) * key_size ** (-0.5)).astype(jnp.bfloat16)
    heads_out, taken_state = retain(query_rot, key_rot, value_rows, prior_state, last_keys, last_values, accepted, -decay_rate)
    head_norm = heads_out * lax.rsqrt(lax.optimization_barrier(jnp.mean(heads_out * heads_out, axis=-1, keepdims=True)) + epsilon)
    gated = (jax.nn.silu(gate_rows.astype(jnp.float32)) * head_norm).astype(jnp.bfloat16)
    gated = gated.reshape(seq_count * proposals, heads * value_size)
    group_rows = heads * value_size // N_TP
    summed = jnp.zeros((seq_count * proposals, width), jnp.float32)
    for block in range(N_TP):
        partial_sum = jnp.dot(gated[:, block * group_rows:(block + 1) * group_rows], out_weight[block * group_rows:(block + 1) * group_rows], preferred_element_type=jnp.float32)
        rounded = lax.optimization_barrier(partial_sum.astype(jnp.bfloat16))
        summed = summed + rounded.astype(jnp.float32)
    retained = summed.astype(jnp.bfloat16).reshape(seq_count, proposals, width)
    return (retained, taken_state, key_rot, value_rows)
```

```python
import functools

import jax
import jax.numpy as jnp
from jax import lax
from jax.experimental import pallas as pl
from jax.experimental.pallas import tpu as pltpu
from jax.sharding import Mesh
from jax.sharding import PartitionSpec as P

KV = ("kv_0", "kv_1")
TP_KV = ("tp", "kv_0", "kv_1")
DP_KV = ("dp", "kv_0", "kv_1")
KV_TP = ("kv_0", "kv_1", "tp")
MESH = pl.DeviceIdType.MESH
F32, BF16 = jnp.float32, jnp.bfloat16

epsilon = 1e-06


def ring_place(i, n):
    odd = lax.rem(i, 2)
    return odd * ((i + 1) // 2) + (1 - odd) * lax.rem(n - i // 2, n)


class TorusGather:
    def __init__(self, own, held, arrived, first_sent, ring_sent, nz, ny):
        self.own, self.held, self.arrived = own, held, arrived
        self.first_sent, self.ring_sent = first_sent, ring_sent
        z, y = lax.axis_index("kv_0"), lax.axis_index("kv_1")
        self.partner = {"tp": 1 - lax.axis_index("tp")}
        self.first = ((y, ny, "kv_1"), (z, nz, "kv_0"))
        self.second = ((z, nz, "kv_0"), (y, ny, "kv_1"))

    def at(self, ref, p, f, s):
        return ref.at[p, s, f] if p == 0 else ref.at[p, f, s]

    def copy(self, p, f, s, source, sent, device):
        return pltpu.make_async_remote_copy(
            src_ref=source,
            dst_ref=self.at(self.held, p, f, s),
            send_sem=sent,
            recv_sem=self.at(self.arrived, p, f, s),
            device_id=device,
            device_id_type=MESH,
        )

    def wait(self, p, f, s):
        chunk = self.at(self.held, p, f, s)
        self.copy(p, f, s, chunk, self.first_sent.at[0, 0], self.partner).wait_recv()

    def first_copy(self, p, d):
        (f, n, axis), (s, _, _) = self.first[p], self.second[p]
        return self.copy(
            p, f, s, self.own(p), self.first_sent.at[p, d], {axis: lax.rem(f + d, n)}
        )

    def start_first(self):
        for p in range(2):
            n = self.first[p][1]

            def send(i, _, p=p, n=n):
                self.first_copy(p, ring_place(i, n)).start()
                return 0

            lax.fori_loop(1, n, send, 0)

    def ring_copy(self, p, k, i, way):
        (f, nf, _), (s, ns, axis) = self.first[p], self.second[p]
        other = lax.rem(f + ring_place(i, nf), nf)
        origin = lax.rem(s - way * k + ns, ns)
        chunk = self.at(self.held, p, other, origin)
        if k == 0:
            source = self.own(p) if isinstance(i, int) and i == 0 else chunk
        else:
            source = chunk
        sent = self.ring_sent.at[p, (1 + way) // 2, k, i]
        return self.copy(p, other, origin, source, sent, {axis: lax.rem(s + way + ns, ns)})

    def pass_on(self, k, i, ways):
        for p in range(2):
            (f, nf, _), (s, ns, _) = self.first[p], self.second[p]
            other = lax.rem(f + ring_place(i, nf), nf)
            if k == 0:
                if not (isinstance(i, int) and i == 0):
                    self.wait(p, other, s)
                for way in ways:
                    self.ring_copy(p, k, i, way).start()
            else:
                for way in (1, -1):
                    self.wait(p, other, lax.rem(s - way * k + ns, ns))
                    if way in ways:
                        self.ring_copy(p, k, i, way).start()

    def hops(self):
        return self.second[0][1] // 2

    def start_ring(self):
        self.pass_on(0, 0, (1, -1))

    def loop(self, low, high, step):
        def body(i, _):
            step(i)
            return 0

        lax.fori_loop(low, high, body, 0)

    def round(self, k):
        n = self.first[0][1]
        if k < self.hops() - 1:
            self.loop(1 if k == 0 else 0, n, lambda i: self.pass_on(k, i, (1, -1)))
        else:
            self.loop(0, n // 2, lambda i: self.pass_on(k, i, (1,)))
            self.loop(n // 2, n, lambda i: self.pass_on(k, i, (-1,)))

    def last_arrivals(self):
        k = self.hops()

        def take(i):
            for p in range(2):
                (f, nf, _), (s, ns, _) = self.first[p], self.second[p]
                self.wait(p, lax.rem(f + ring_place(i, nf), nf), lax.rem(s + k, ns))

        self.loop(0, self.first[0][1], take)

    def finish(self):
        n = self.first[0][1]
        for p in range(2):
            self.loop(1, n, lambda d, p=p: self.first_copy(p, d).wait_send())
        for k in range(self.hops()):
            last = k == self.hops() - 1

            def done(i, ways, k=k):
                for p in range(2):
                    for way in ways:
                        self.ring_copy(p, k, i, way).wait_send()

            if last:
                self.loop(0, n // 2, lambda i: done(i, (1,)))
                self.loop(n // 2, n, lambda i: done(i, (-1,)))
            else:
                self.loop(0, n, lambda i: done(i, (1, -1)))


def iota(shape, dim):
    return lax.broadcasted_iota(jnp.int32, shape, dim)


def kernel(
    nz,
    ny,
    tok,
    wq,
    wk,
    wv,
    wg,
    wo,
    prior,
    gain,
    last_k,
    last_v,
    cos_tab,
    sin_tab,
    grid,
    query_decay,
    key_weights,
    carried,
    ret_out,
    state_out,
    keys_out,
    values_out,
    tok_v,
    weights,
    wo_v,
    prior_v,
    state_v,
    state_b,
    tokens_all,
    place,
    order,
    out_a,
    in_a,
    mid,
    out_b,
    in_b,
    rows_f,
    chunk,
    gated_all,
    sent_out,
    got_out,
    ret_v,
    keys_v,
    values_v,
    local,
    tok_arrived,
    tok_first,
    tok_ring,
    gat_arrived,
    gat_first,
    gat_ring,
    pair_sems,
    a_sent,
    a_got,
    b_sent,
    b_got,
):
    z, y, tp = lax.axis_index("kv_0"), lax.axis_index("kv_1"), lax.axis_index("tp")
    heads, seqs = nz, 2 * nz * ny
    kc = wq.shape[0]
    vc = wv.shape[0]
    span = 2 * kc + 2 * vc
    partner = {"tp": 1 - tp}

    loads = [
        pltpu.make_async_copy(tok.at[pl.ds(2 * tp, 2)], tok_v, local.at[0]),
        pltpu.make_async_copy(wq, weights.at[tp, pl.ds(0, kc)], local.at[1]),
        pltpu.make_async_copy(wk, weights.at[tp, pl.ds(kc, kc)], local.at[2]),
        pltpu.make_async_copy(wv, weights.at[tp, pl.ds(2 * kc, vc)], local.at[3]),
        pltpu.make_async_copy(wg, weights.at[tp, pl.ds(2 * kc + vc, vc)], local.at[4]),
        pltpu.make_async_copy(prior, prior_v, local.at[5]),
        pltpu.make_async_copy(wo, wo_v, local.at[6]),
    ]
    for load in loads:
        load.start()

    barrier = pltpu.get_barrier_semaphore()

    def greet(device):
        pl.semaphore_signal(barrier, inc=1, device_id=device, device_id_type=MESH)

    def greet_y(d, _):
        other = lax.rem(y + d, ny)
        greet({"kv_1": other})
        greet({"kv_1": other, "tp": 1 - tp})
        return 0

    def greet_z(d, _):
        greet({"kv_0": lax.rem(z + d, nz)})
        return 0

    lax.fori_loop(1, ny, greet_y, 0)
    lax.fori_loop(1, nz, greet_z, 0)
    greet(partner)
    pl.semaphore_wait(barrier, 2 * (ny - 1) + (nz - 1) + 1)

    loads[0].wait()
    tokens = TorusGather(
        lambda p: tok_v.at[p], tokens_all, tok_arrived, tok_first, tok_ring, nz, ny
    )
    tokens.start_first()
    tokens.start_ring()
    keep = [
        pltpu.make_async_copy(tok_v.at[p], tokens_all.at[p, z, y], local.at[7 + p]) for p in range(2)
    ]
    for each in keep:
        each.start()
    for load in loads[1:5]:
        load.wait()
    swap = pltpu.make_async_remote_copy(
        src_ref=weights.at[tp],
        dst_ref=weights.at[tp],
        send_sem=pair_sems.at[0],
        recv_sem=pair_sems.at[1],
        device_id=partner,
        device_id_type=MESH,
    )
    swap.start()

    loads[5].wait()
    rows = 4 * heads
    head_of = lax.rem(iota((rows, 1), 0), heads)
    for s in range(2):
        weighted = last_k[s].astype(F32) * key_weights[s]
        high = weighted.astype(BF16).astype(F32)
        low = weighted - high

        def one_head(h, _, s=s, high=high, low=low):
            mine = head_of == h
            both = jnp.concatenate([jnp.where(mine, high, 0.0), jnp.where(mine, low, 0.0)], axis=0)
            values = jnp.concatenate([last_v[s], last_v[s]], axis=0)
            update = lax.dot_general(
                both.astype(BF16), values, (((0,), (0,)), ((), ())), preferred_element_type=F32
            )
            at = s * heads + h
            fresh = carried[at] * prior_v[at] + update
            state_v[at] = fresh
            state_b[at] = fresh.astype(BF16)
            return 0

        lax.fori_loop(0, heads, one_head, 0)
    state_store = pltpu.make_async_copy(state_v, state_out, local.at[9])
    state_store.start()

    tokens.round(0)

    key_size, value_size = ny * kc, ny * vc
    lane = iota((128, 2 * key_size + 2 * value_size), 0)
    column = iota((128, 2 * key_size + 2 * value_size), 1)
    for j in range(ny):
        goal = jnp.where(
            lane < kc,
            kc * j + lane,
            jnp.where(
                lane < 2 * kc,
                key_size + kc * j + lane - kc,
                jnp.where(
                    lane < 2 * kc + vc,
                    2 * key_size + vc * j + lane - 2 * kc,
                    2 * key_size + value_size + vc * j + lane - 2 * kc - vc,
                ),
            ),
        )
        hit = (goal == column) & (lane < span)
        place[pl.ds(128 * j, 128)] = jnp.where(hit, 1.0, 0.0).astype(BF16)
    swap.wait()

    def scale_rows(i, _):
        at = pl.ds(pl.multiple_of(i * 16, 16), 16)
        for side in range(2):
            weights[side, at] = (weights[side, at].astype(F32) * gain[...]).astype(BF16)
        return 0

    lax.fori_loop(0, span // 16, scale_rows, 0)
    for k in range(1, tokens.hops()):
        tokens.round(k)
    source = iota((4 * seqs, seqs), 0)
    target = iota((4 * seqs, seqs), 1)
    for p in range(4):
        row_seq = 2 * (source // 8) + lax.rem(source // 2, 2)
        row_prop = 2 * (lax.rem(source, 8) // 4) + lax.rem(source, 2)
        hit = (row_seq == target) & (row_prop == p)
        order[:, pl.ds(seqs * p, seqs)] = jnp.where(hit, 1.0, 0.0).astype(BF16)
    tokens.last_arrivals()
    for each in keep:
        each.wait()

    depth = tok_v.shape[1]
    width = nz * ny * depth
    for p in range(2):
        total = jnp.zeros((2 * span, seqs), F32)
        squares = jnp.zeros((1, seqs), F32)
        for c in range(nz):
            block = tokens_all[p, c].reshape(ny * depth, seqs)
            cut = pl.ds(c * ny * depth, ny * depth)
            total += jnp.dot(
                weights[:, :, cut].reshape(2 * span, ny * depth), block, preferred_element_type=F32
            )
            floats = block.astype(F32)
            squares += jnp.sum(floats * floats, axis=0, keepdims=True)
        scaled = total * lax.rsqrt(squares / width + epsilon)
        for side in range(2):
            part = jnp.concatenate(
                [scaled[side * span : (side + 1) * span], jnp.zeros((128 - span, seqs), F32)], axis=0
            )
            turned = part.T.astype(BF16)
            for to in range(nz):
                out_a[to, side, p] = turned[2 * ny * to : 2 * ny * (to + 1)]

    def a_copy(d):
        to = lax.rem(z + d, nz)
        return pltpu.make_async_remote_copy(
            src_ref=out_a.at[to],
            dst_ref=in_a.at[z],
            send_sem=a_sent.at[d],
            recv_sem=a_got.at[z],
            device_id={"kv_0": to},
            device_id_type=MESH,
        )

    def a_wait(d):
        came = lax.rem(z + d, nz)
        pltpu.make_async_remote_copy(
            src_ref=in_a.at[came],
            dst_ref=in_a.at[came],
            send_sem=a_sent.at[0],
            recv_sem=a_got.at[came],
            device_id=partner,
            device_id_type=MESH,
        ).wait_recv()

    tokens.loop(1, nz, lambda d: a_copy(d).start())
    own_a = pltpu.make_async_copy(out_a.at[z], in_a.at[z], local.at[10])
    own_a.start()
    own_a.wait()
    tokens.loop(1, nz, a_wait)

    mid[...] = in_a[...].reshape(nz * 4 * 2 * ny, 128).astype(F32)
    stride = 4 * 2 * ny
    for to in range(ny):
        for side in range(2):
            for s in range(2):
                parts = [
                    mid[pl.ds(side * 4 * ny + p * 2 * ny + 2 * to + s, nz, stride=stride), :]
                    for p in range(2)
                ]
                out_b[to, side, s] = jnp.concatenate(parts, axis=0).astype(BF16)

    def b_copy(d, same):
        to = lax.rem(y + d, ny)
        side = tp if same else 1 - tp
        return pltpu.make_async_remote_copy(
            src_ref=out_b.at[to, side],
            dst_ref=in_b.at[y, tp],
            send_sem=b_sent.at[d, side],
            recv_sem=b_got.at[y, tp],
            device_id={"kv_1": to, "tp": side},
            device_id_type=MESH,
        )

    def b_wait(d, same):
        came = lax.rem(y + d, ny)
        side = tp if same else 1 - tp
        pltpu.make_async_remote_copy(
            src_ref=in_b.at[came, side],
            dst_ref=in_b.at[came, side],
            send_sem=b_sent.at[0, 0],
            recv_sem=b_got.at[came, side],
            device_id=partner,
            device_id_type=MESH,
        ).wait_recv()

    def b_start(d):
        b_copy(d, True).start()
        b_copy(d, False).start()

    tokens.loop(1, ny, b_start)
    b_copy(0, False).start()
    own_b = pltpu.make_async_copy(out_b.at[y, tp], in_b.at[y, tp], local.at[11])
    own_b.start()
    own_b.wait()
    b_wait(0, False)

    def b_take(d):
        b_wait(d, True)
        b_wait(d, False)

    tokens.loop(1, ny, b_take)

    count = 8 * heads
    packed = jnp.concatenate([in_b[j].reshape(count, 128) for j in range(ny)], axis=1)
    fields = jnp.dot(packed, place[...], preferred_element_type=F32)
    query = fields[:, :key_size]
    key = fields[:, key_size : 2 * key_size]
    value = fields[:, 2 * key_size : 2 * key_size + value_size]
    gate = fields[:, 2 * key_size + value_size :]
    cosine, sine = cos_tab[...], sin_tab[...]
    half = key_size // 2

    def turned_by(x):
        swapped = jnp.concatenate([x[:, half:], x[:, :half]], axis=1)
        return x * cosine + swapped * sine

    query_rot = turned_by(query).astype(BF16)
    key_f = turned_by(key) * key_size ** (-0.5)
    key_rot = key_f.astype(BF16)
    value_b = value.astype(BF16)
    scores = lax.dot_general(
        query_rot, key_rot, (((1,), (1,)), ((), ())), preferred_element_type=F32
    )
    inner = jnp.dot((scores * grid[...]).astype(BF16), value_b, preferred_element_type=F32)
    decayed = query_rot.astype(F32) * query_decay[...]
    row = iota((count, 1), 0)
    row_at = lax.rem(row // (2 * heads), 2) * heads + lax.rem(row, heads)
    spread = jnp.concatenate(
        [jnp.where(row_at == at, decayed, 0.0).astype(BF16) for at in range(2 * heads)], axis=1
    )
    states = state_b[...].reshape(2 * heads * key_size, value_size)
    heads_out = inner + jnp.dot(spread, states, preferred_element_type=F32)
    normed = heads_out * lax.rsqrt(jnp.mean(heads_out * heads_out, axis=-1, keepdims=True) + epsilon)
    product = gate / (1.0 + jnp.exp(-gate)) * normed
    for c in range(value_size // 128):
        rows_f[c] = product[:, 128 * c : 128 * (c + 1)]
    for i in range(8):
        prop, seq = 2 * (i // 4) + i % 2, (i // 2) % 2
        keys_v[seq, prop] = key_f[i * heads : (i + 1) * heads].astype(BF16)
        values_v[seq, prop] = value[i * heads : (i + 1) * heads].astype(BF16)
    cut = heads * value_size // 2
    for h in range(heads):
        part, at = divmod(h * value_size, cut)
        for c in range(value_size // 128):
            piece = rows_f[c, pl.ds(h, 8, stride=heads), :]
            chunk[part, :, at + 128 * c : at + 128 * (c + 1)] = piece.astype(BF16)
    small = [
        pltpu.make_async_copy(keys_v, keys_out, local.at[12]),
        pltpu.make_async_copy(values_v, values_out, local.at[13]),
    ]
    for each in small:
        each.start()

    gated = TorusGather(
        lambda p: chunk.at[p], gated_all, gat_arrived, gat_first, gat_ring, nz, ny
    )
    gated.start_first()
    gated.start_ring()
    keep = [
        pltpu.make_async_copy(chunk.at[p], gated_all.at[p, z, y], local.at[14 + p]) for p in range(2)
    ]
    for each in keep:
        each.start()
    for k in range(gated.hops()):
        gated.round(k)
    gated.last_arrivals()
    for each in keep:
        each.wait()
    loads[6].wait()
    total = jnp.zeros((wo_v.shape[0], 4 * seqs), F32)
    for part in range(2):
        total += lax.dot_general(
            wo_v[:, part * cut : (part + 1) * cut],
            gated_all[part].reshape(4 * seqs, cut),
            (((1,), (1,)), ((), ())),
            preferred_element_type=F32,
        )
    rounded = total.astype(BF16)
    mine = rounded.shape[0] // 2
    sent_out[0] = rounded[:mine]
    sent_out[1] = rounded[mine:]
    trade = pltpu.make_async_remote_copy(
        src_ref=sent_out.at[1 - tp],
        dst_ref=got_out,
        send_sem=pair_sems.at[2],
        recv_sem=pair_sems.at[3],
        device_id=partner,
        device_id_type=MESH,
    )
    trade.start()
    trade.wait()
    summed = (sent_out[tp].astype(F32) + got_out[...].astype(F32)).astype(BF16)
    result = jnp.dot(summed, order[...], preferred_element_type=F32).astype(BF16)
    for p in range(4):
        ret_v[p] = result[:, p * seqs : (p + 1) * seqs]
    last = pltpu.make_async_copy(ret_v, ret_out, local.at[16])
    last.start()
    tokens.finish()
    gated.finish()
    tokens.loop(1, nz, lambda d: a_copy(d).wait_send())

    def b_done(d):
        b_copy(d, True).wait_send()
        b_copy(d, False).wait_send()

    tokens.loop(1, ny, b_done)
    b_copy(0, False).wait_send()
    for each in small:
        each.wait()
    state_store.wait()
    last.wait()


def shards(
    nz,
    ny,
    tokens,
    norm_gain,
    query_weight,
    key_weight,
    value_weight,
    gate_weight,
    out_weight,
    decay_rate,
    prior_state,
    last_keys,
    last_values,
    accepted,
    lengths,
):
    _, heads, key_size, value_size = prior_state.shape
    seqs, _, depth = tokens.shape
    width = norm_gain.shape[0]
    kc, vc = query_weight.shape[1], value_weight.shape[1]
    span = 2 * kc + 2 * vc
    log_decay = -decay_rate
    count = 8 * heads

    def to_rows(table):
        table = table.reshape(2, 2, 2, heads, table.shape[-1])
        return table.transpose(1, 0, 2, 3, 4).reshape(count, -1)

    half = key_size // 2
    steps = jnp.arange(4, dtype=jnp.int32)
    positions = (lengths + accepted)[:, None] + steps[None, :]
    frequency = jnp.power(10000.0, -jnp.arange(half, dtype=F32) / half)
    angles = positions.astype(F32)[:, :, None] * frequency
    cosine, sine = jnp.cos(angles), jnp.sin(angles)

    def all_heads(table):
        return to_rows(jnp.broadcast_to(table[:, :, None, :], (2, 4, heads, key_size)))

    cos_tab = all_heads(jnp.concatenate([cosine, cosine], axis=-1))
    sin_tab = all_heads(jnp.concatenate([-sine, sine], axis=-1))
    row = jnp.arange(count, dtype=jnp.int32)
    row_prop = 2 * (row // (4 * heads)) + (row // heads) % 2
    row_seq = (row // (2 * heads)) % 2
    row_head = row % heads
    row_decay = jnp.tile(log_decay, 8)
    offset = (row_prop[:, None] - row_prop[None, :]).astype(F32)
    same = (row_seq[:, None] == row_seq[None, :]) & (row_head[:, None] == row_head[None, :])
    grid = jnp.where(
        same & (offset >= 0.0), jnp.exp(row_decay[:, None] * jnp.maximum(offset, 0.0)), 0.0
    )
    query_decay = jnp.broadcast_to(
        jnp.exp(row_decay * (row_prop.astype(F32) + 1.0))[:, None], (count, key_size)
    )
    power = jnp.maximum(accepted[:, None] - 1 - steps[None, :], 0).astype(F32)
    taken = steps[None, :] < accepted[:, None]
    weight = jnp.where(
        taken[:, :, None], jnp.exp(log_decay[None, None, :] * power[:, :, None]), 0.0
    )
    key_weights = jnp.broadcast_to(
        weight.reshape(2, 4 * heads, 1), (2, 4 * heads, key_size)
    )
    carried = jnp.exp(log_decay[None, :] * accepted[:, None].astype(F32)).reshape(2 * heads)

    any_ref = pl.BlockSpec(memory_space=pl.ANY)
    vmem = pl.BlockSpec(memory_space=pltpu.VMEM)
    smem = pl.BlockSpec(memory_space=pltpu.SMEM)
    dma = pltpu.SemaphoreType.DMA
    cut = heads * value_size // 2
    out_cols = out_weight.shape[1]
    retained, state, new_keys, new_values = pl.pallas_call(
        functools.partial(kernel, nz, ny),
        out_shape=(
            jax.ShapeDtypeStruct((4, out_cols // 2, seqs), BF16),
            jax.ShapeDtypeStruct((2 * heads, key_size, value_size), F32),
            jax.ShapeDtypeStruct((2, 4, heads, key_size), BF16),
            jax.ShapeDtypeStruct((2, 4, heads, value_size), BF16),
        ),
        in_specs=[any_ref] * 7 + [vmem] * 8 + [smem],
        out_specs=(any_ref,) * 4,
        scratch_shapes=[
            pltpu.VMEM((2, depth, seqs), BF16),
            pltpu.VMEM((2, span, width), BF16),
            pltpu.VMEM((out_cols, heads * value_size), BF16),
            pltpu.VMEM((2 * heads, key_size, value_size), F32),
            pltpu.VMEM((2 * heads, key_size, value_size), F32),
            pltpu.VMEM((2 * heads, key_size, value_size), BF16),
            pltpu.VMEM((2, nz, ny, depth, seqs), BF16),
            pltpu.VMEM((128 * ny, 2 * key_size + 2 * value_size), BF16),
            pltpu.VMEM((4 * seqs, 4 * seqs), BF16),
            pltpu.VMEM((nz, 2, 2, 2 * ny, 128), BF16),
            pltpu.VMEM((nz, 2, 2, 2 * ny, 128), BF16),
            pltpu.VMEM((nz * 8 * ny, 128), F32),
            pltpu.VMEM((ny, 2, 2, 2 * nz, 128), BF16),
            pltpu.VMEM((ny, 2, 2, 2 * nz, 128), BF16),
            pltpu.VMEM((value_size // 128, count, 128), F32),
            pltpu.VMEM((2, 8, cut), BF16),
            pltpu.VMEM((2, nz, ny, 8, cut), BF16),
            pltpu.VMEM((2, out_cols // 2, 4 * seqs), BF16),
            pltpu.VMEM((out_cols // 2, 4 * seqs), BF16),
            pltpu.VMEM((4, out_cols // 2, seqs), BF16),
            pltpu.VMEM((2, 4, heads, key_size), BF16),
            pltpu.VMEM((2, 4, heads, value_size), BF16),
            dma((17,)),
            dma((2, nz, ny)),
            dma((2, max(nz, ny))),
            dma((2, 2, nz // 2, ny)),
            dma((2, nz, ny)),
            dma((2, max(nz, ny))),
            dma((2, 2, nz // 2, ny)),
            dma((4,)),
            dma((nz,)),
            dma((nz,)),
            dma((ny, 2)),
            dma((ny, 2)),
        ],
        compiler_params=pltpu.CompilerParams(
            collective_id=0, has_side_effects=True, vmem_limit_bytes=48 * 1024 * 1024
        ),
    )(
        tokens.transpose(1, 2, 0),
        query_weight.T,
        key_weight.T,
        value_weight.T,
        gate_weight.T,
        out_weight.T,
        prior_state.reshape(2 * heads, key_size, value_size),
        norm_gain.astype(F32)[None, :],
        last_keys.reshape(2, 4 * heads, key_size),
        last_values.reshape(2, 4 * heads, value_size),
        cos_tab,
        sin_tab,
        grid,
        query_decay,
        key_weights,
        carried,
    )
    return (
        retained.transpose(2, 0, 1),
        state.reshape(prior_state.shape),
        new_keys,
        new_values,
    )


def solution(mesh):
    nz = ny = 8
    finer = Mesh(
        mesh.devices.reshape(mesh.shape["dp"], nz, ny, mesh.shape["tp"]),
        ("dp", "kv_0", "kv_1", "tp"),
    )
    return jax.shard_map(
        functools.partial(shards, nz, ny),
        mesh=finer,
        in_specs=(
            P("dp", None, KV),
            P(),
            P(None, TP_KV),
            P(None, TP_KV),
            P(None, TP_KV),
            P(None, TP_KV),
            P("tp", KV),
            P("tp"),
            P(DP_KV, "tp", None, None),
            P(DP_KV, None, "tp", None),
            P(DP_KV, None, "tp", None),
            P(DP_KV),
            P(DP_KV),
        ),
        out_specs=(
            P("dp", None, KV_TP),
            P(DP_KV, "tp", None, None),
            P(DP_KV, None, "tp", None),
            P(DP_KV, None, "tp", None),
        ),
        check_vma=False,
    )
```

```python
import functools

import jax
import jax.numpy as jnp
from jax import lax
from jax.experimental import pallas as pl
from jax.experimental.pallas import tpu as pltpu
from jax.sharding import Mesh
from jax.sharding import PartitionSpec as P

KV = ("kv_0", "kv_1")
TP_KV = ("tp", "kv_0", "kv_1")
DP_KV = ("dp", "kv_0", "kv_1")
KV_TP = ("kv_0", "kv_1", "tp")
MESH = pl.DeviceIdType.MESH
F32, BF16 = jnp.float32, jnp.bfloat16

epsilon = 1e-06


def wrap(i, n):
    return i & (n - 1)


def ring_place(i, n):
    if isinstance(i, int):
        return (i + 1) // 2 if i % 2 else (n - i // 2) % n
    odd = i & 1
    return wrap(odd * ((i + 1) >> 1) + (1 - odd) * (n - (i >> 1)), n)


class TorusGather:
    def __init__(self, own, held, arrived, first_sent, ring_sent, nz, ny):
        self.own, self.held, self.arrived = own, held, arrived
        self.first_sent, self.ring_sent = first_sent, ring_sent
        z, y = lax.axis_index("kv_0"), lax.axis_index("kv_1")
        self.partner = {"tp": 1 - lax.axis_index("tp")}
        self.first = ((y, ny, "kv_1"), (z, nz, "kv_0"))
        self.second = ((z, nz, "kv_0"), (y, ny, "kv_1"))

    def at(self, ref, p, f, s):
        return ref.at[p, s, f] if p == 0 else ref.at[p, f, s]

    def copy(self, p, f, s, source, sent, device):
        return pltpu.make_async_remote_copy(
            src_ref=source,
            dst_ref=self.at(self.held, p, f, s),
            send_sem=sent,
            recv_sem=self.at(self.arrived, p, f, s),
            device_id=device,
            device_id_type=MESH,
        )

    def wait(self, p, f, s):
        chunk = self.at(self.held, p, f, s)
        self.copy(p, f, s, chunk, self.first_sent.at[0, 0], self.partner).wait_recv()

    def first_copy(self, p, d):
        (f, n, axis), (s, _, _) = self.first[p], self.second[p]
        return self.copy(
            p, f, s, self.own(p), self.first_sent.at[p, d], {axis: wrap(f + d, n)}
        )

    def start_first(self):
        for p in range(2):
            n = self.first[p][1]

            def send(i, _, p=p, n=n):
                self.first_copy(p, ring_place(i, n)).start()
                return 0

            lax.fori_loop(1, n, send, 0)

    def ring_copy(self, p, k, i, way):
        (f, nf, _), (s, ns, axis) = self.first[p], self.second[p]
        other = wrap(f + ring_place(i, nf), nf)
        origin = wrap(s - way * k + ns, ns)
        chunk = self.at(self.held, p, other, origin)
        if k == 0:
            source = self.own(p) if isinstance(i, int) and i == 0 else chunk
        else:
            source = chunk
        sent = self.ring_sent.at[p, (1 + way) // 2, k, i]
        return self.copy(p, other, origin, source, sent, {axis: wrap(s + way + ns, ns)})

    def pass_on(self, k, i, ways):
        for p in range(2):
            (f, nf, _), (s, ns, _) = self.first[p], self.second[p]
            other = wrap(f + ring_place(i, nf), nf)
            if k == 0:
                if not (isinstance(i, int) and i == 0):
                    self.wait(p, other, s)
                for way in ways:
                    self.ring_copy(p, k, i, way).start()
            else:
                for way in (1, -1):
                    self.wait(p, other, wrap(s - way * k + ns, ns))
                    if way in ways:
                        self.ring_copy(p, k, i, way).start()

    def hops(self):
        return self.second[0][1] // 2

    def start_ring(self):
        self.pass_on(0, 0, (1, -1))

    def loop(self, low, high, step):
        def body(i, _):
            step(i)
            return 0

        lax.fori_loop(low, high, body, 0)

    def round(self, k, beside=None):
        n = self.first[0][1]

        def both(i, ways):
            self.pass_on(k, i, ways)
            if beside is not None:
                beside(i)

        if k < self.hops() - 1:
            self.loop(1 if k == 0 else 0, n, lambda i: both(i, (1, -1)))
        else:
            self.loop(0, n // 2, lambda i: both(i, (1,)))
            self.loop(n // 2, n, lambda i: both(i, (-1,)))

    def last_arrivals(self):
        k = self.hops()

        def take(i):
            for p in range(2):
                (f, nf, _), (s, ns, _) = self.first[p], self.second[p]
                self.wait(p, wrap(f + ring_place(i, nf), nf), wrap(s + k, ns))

        self.loop(0, self.first[0][1], take)

    def finish(self):
        n = self.first[0][1]
        for p in range(2):
            self.loop(1, n, lambda d, p=p: self.first_copy(p, d).wait_send())
        for k in range(self.hops()):
            last = k == self.hops() - 1

            def done(i, ways, k=k):
                for p in range(2):
                    for way in ways:
                        self.ring_copy(p, k, i, way).wait_send()

            if last:
                self.loop(0, n // 2, lambda i: done(i, (1,)))
                self.loop(n // 2, n, lambda i: done(i, (-1,)))
            else:
                self.loop(0, n, lambda i: done(i, (1, -1)))


def iota(shape, dim):
    return lax.broadcasted_iota(jnp.int32, shape, dim)


def kernel(
    nz,
    ny,
    tok,
    wq,
    wk,
    wv,
    wg,
    wo,
    prior,
    last_k_in,
    last_v_in,
    decay_in,
    accepted_in,
    lengths_in,
    gain,
    frequency,
    ret_out,
    state_out,
    keys_out,
    values_out,
    tok_v,
    weights,
    wo_v,
    prior_v,
    last_k,
    last_v,
    decay,
    accepted,
    lengths,
    weighted_keys,
    state_b,
    tokens_all,
    place,
    order,
    out_a,
    in_a,
    mid,
    out_b,
    in_b,
    rows_f,
    chunk,
    gated_all,
    sent_out,
    got_out,
    local,
    tok_arrived,
    tok_first,
    tok_ring,
    gat_arrived,
    gat_first,
    gat_ring,
    pair_sems,
    a_sent,
    a_got,
    b_sent,
    b_got,
):
    z, y, tp = lax.axis_index("kv_0"), lax.axis_index("kv_1"), lax.axis_index("tp")
    heads, seqs = nz, 2 * nz * ny
    kc = wq.shape[0]
    vc = wv.shape[0]
    span = 2 * kc + 2 * vc
    partner = {"tp": 1 - tp}

    loads = [
        pltpu.make_async_copy(tok.at[pl.ds(2 * tp, 2)], tok_v, local.at[0]),
        pltpu.make_async_copy(wq, weights.at[tp, pl.ds(0, kc)], local.at[1]),
        pltpu.make_async_copy(wk, weights.at[tp, pl.ds(kc, kc)], local.at[2]),
        pltpu.make_async_copy(wv, weights.at[tp, pl.ds(2 * kc, vc)], local.at[3]),
        pltpu.make_async_copy(wg, weights.at[tp, pl.ds(2 * kc + vc, vc)], local.at[4]),
        pltpu.make_async_copy(prior, prior_v, local.at[5]),
        pltpu.make_async_copy(wo, wo_v, local.at[6]),
    ]
    small_loads = [
        pltpu.make_async_copy(source, target, local.at[17 + i])
        for i, (source, target) in enumerate(
            (
                (last_k_in, last_k),
                (last_v_in, last_v),
                (decay_in, decay),
                (accepted_in, accepted),
                (lengths_in, lengths),
            )
        )
    ]
    for load in loads + small_loads:
        load.start()

    barrier = pltpu.get_barrier_semaphore()

    def greet(device):
        pl.semaphore_signal(barrier, inc=1, device_id=device, device_id_type=MESH)

    def greet_y(d, _):
        other = wrap(y + d, ny)
        greet({"kv_1": other})
        greet({"kv_1": other, "tp": 1 - tp})
        return 0

    def greet_z(d, _):
        greet({"kv_0": wrap(z + d, nz)})
        return 0

    lax.fori_loop(1, ny, greet_y, 0)
    lax.fori_loop(1, nz, greet_z, 0)
    greet(partner)
    pl.semaphore_wait(barrier, 2 * (ny - 1) + (nz - 1) + 1)

    loads[0].wait()
    tokens = TorusGather(
        lambda p: tok_v.at[p], tokens_all, tok_arrived, tok_first, tok_ring, nz, ny
    )
    tokens.start_first()
    tokens.start_ring()
    keep = [
        pltpu.make_async_copy(tok_v.at[p], tokens_all.at[p, z, y], local.at[7 + p]) for p in range(2)
    ]
    for each in keep:
        each.start()
    for load in loads[1:5]:
        load.wait()
    swap = pltpu.make_async_remote_copy(
        src_ref=weights.at[tp],
        dst_ref=weights.at[tp],
        send_sem=pair_sems.at[0],
        recv_sem=pair_sems.at[1],
        device_id=partner,
        device_id_type=MESH,
    )
    swap.start()

    key_size, value_size = ny * kc, ny * vc

    loads[5].wait()
    for load in small_loads:
        load.wait()
    rows, count = 4 * heads, 8 * heads
    head_of = iota((rows, 1), 0) & (heads - 1)

    def by_head(shape):
        head = iota(shape, 0) & (heads - 1)
        table = jnp.zeros(shape, F32)
        for h in range(heads):
            table = jnp.where(head == h, -decay[h], table)
        return table

    taken_decay = by_head((rows, 128))
    before = iota((rows, 128), 0) >> (heads.bit_length() - 1)
    for s in range(2):
        power = jnp.maximum(accepted[s] - 1 - before, 0).astype(F32)
        key_weights = jnp.where(before < accepted[s], jnp.exp(taken_decay * power), 0.0)
        weighted = last_k[s].astype(F32) * key_weights
        high = weighted.astype(BF16).astype(F32)
        weighted_keys[s, 0] = high
        weighted_keys[s, 1] = weighted - high

    def one_head(h):
        mine = head_of == h
        for s in range(2):
            both = jnp.concatenate(
                [jnp.where(mine, weighted_keys[s, part], 0.0) for part in range(2)], axis=0
            )
            values = jnp.concatenate([last_v[s], last_v[s]], axis=0)
            update = lax.dot_general(
                both.astype(BF16), values, (((0,), (0,)), ((), ())), preferred_element_type=F32
            )
            at = s * heads + h
            power = jnp.full((1, value_size), -decay[h] * accepted[s].astype(F32), F32)
            fresh = jnp.exp(power) * prior_v[at] + update
            state_out[at] = fresh
            state_b[at] = fresh.astype(BF16)

    one_head(0)
    tokens.round(0, one_head)

    swap.wait()

    blocks = span // 16

    def scale_rows(i):
        @pl.when(i < blocks)
        def _():
            at = pl.ds(pl.multiple_of(i * 16, 16), 16)
            for side in range(2):
                weights[side, at] = (weights[side, at].astype(F32) * gain[...]).astype(BF16)

    for k in range(1, tokens.hops()):
        tokens.round(k, scale_rows if k == 1 else None)
    tokens.last_arrivals()
    for each in keep:
        each.wait()

    depth = tok_v.shape[1]
    width = nz * ny * depth
    for p in range(2):
        total = jnp.zeros((2 * span, seqs), F32)
        squares = jnp.zeros((1, seqs), F32)
        for c in range(nz):
            block = tokens_all[p, c].reshape(ny * depth, seqs)
            cut = pl.ds(c * ny * depth, ny * depth)
            total += jnp.dot(
                weights[:, :, cut].reshape(2 * span, ny * depth), block, preferred_element_type=F32
            )
            floats = block.astype(F32)
            squares += jnp.sum(floats * floats, axis=0, keepdims=True)
        scaled = total * lax.rsqrt(squares / width + epsilon)
        for side in range(2):
            part = jnp.concatenate(
                [scaled[side * span : (side + 1) * span], jnp.zeros((128 - span, seqs), F32)], axis=0
            )
            turned = part.T.astype(BF16)
            for to in range(nz):
                out_a[to, side, p] = turned[2 * ny * to : 2 * ny * (to + 1)]

    def a_copy(d):
        to = wrap(z + d, nz)
        return pltpu.make_async_remote_copy(
            src_ref=out_a.at[to],
            dst_ref=in_a.at[z],
            send_sem=a_sent.at[d],
            recv_sem=a_got.at[z],
            device_id={"kv_0": to},
            device_id_type=MESH,
        )

    def a_wait(d):
        came = wrap(z + d, nz)
        pltpu.make_async_remote_copy(
            src_ref=in_a.at[came],
            dst_ref=in_a.at[came],
            send_sem=a_sent.at[0],
            recv_sem=a_got.at[came],
            device_id=partner,
            device_id_type=MESH,
        ).wait_recv()

    tokens.loop(1, nz, lambda d: a_copy(d).start())
    own_a = pltpu.make_async_copy(out_a.at[z], in_a.at[z], local.at[10])
    own_a.start()

    shift = heads.bit_length() - 1

    def prop_of(i):
        return 2 * (i >> (shift + 2)) + ((i >> shift) & 1)

    def at_of(i):
        return ((i >> (shift + 1)) & 1) * heads + (i & (heads - 1))

    row = iota((count, 128), 0)
    first = jnp.where((row >> (shift + 1)) & 1 == 0, lengths[0] + accepted[0], lengths[1] + accepted[1])
    angles = (first + prop_of(row)).astype(F32) * frequency[...]
    cosine = jnp.cos(angles)
    lane_sign = jnp.where(iota((count, 128), 1) < key_size // 2, -1.0, 1.0)
    sine = jnp.sin(angles) * lane_sign
    decays = by_head((count, 128))
    query_decay = jnp.exp(decays * (prop_of(row) + 1).astype(F32))
    other = iota((count, count), 1)
    here = row[:, :count]
    offset = prop_of(here) - prop_of(other)
    grid = jnp.where(
        (at_of(here) == at_of(other)) & (offset >= 0),
        jnp.exp(decays[:, :count] * jnp.maximum(offset, 0).astype(F32)),
        0.0,
    )

    own_a.wait()
    tokens.loop(1, nz, a_wait)

    mid[...] = in_a[...].reshape(nz * 4 * 2 * ny, 128).astype(F32)
    stride = 4 * 2 * ny
    for to in range(ny):
        for side in range(2):
            for s in range(2):
                parts = [
                    mid[pl.ds(side * 4 * ny + p * 2 * ny + 2 * to + s, nz, stride=stride), :]
                    for p in range(2)
                ]
                out_b[to, side, s] = jnp.concatenate(parts, axis=0).astype(BF16)

    def b_copy(d, same):
        to = wrap(y + d, ny)
        side = tp if same else 1 - tp
        return pltpu.make_async_remote_copy(
            src_ref=out_b.at[to, side],
            dst_ref=in_b.at[y, tp],
            send_sem=b_sent.at[d, side],
            recv_sem=b_got.at[y, tp],
            device_id={"kv_1": to, "tp": side},
            device_id_type=MESH,
        )

    def b_wait(d, same):
        came = wrap(y + d, ny)
        side = tp if same else 1 - tp
        pltpu.make_async_remote_copy(
            src_ref=in_b.at[came, side],
            dst_ref=in_b.at[came, side],
            send_sem=b_sent.at[0, 0],
            recv_sem=b_got.at[came, side],
            device_id=partner,
            device_id_type=MESH,
        ).wait_recv()

    def b_start(d):
        b_copy(d, True).start()
        b_copy(d, False).start()

    tokens.loop(1, ny, b_start)
    b_copy(0, False).start()
    own_b = pltpu.make_async_copy(out_b.at[y, tp], in_b.at[y, tp], local.at[11])
    own_b.start()

    lane = iota((128, 2 * key_size + 2 * value_size), 0)
    column = iota((128, 2 * key_size + 2 * value_size), 1)
    for j in range(ny):
        goal = jnp.where(
            lane < kc,
            kc * j + lane,
            jnp.where(
                lane < 2 * kc,
                key_size + kc * j + lane - kc,
                jnp.where(
                    lane < 2 * kc + vc,
                    2 * key_size + vc * j + lane - 2 * kc,
                    2 * key_size + value_size + vc * j + lane - 2 * kc - vc,
                ),
            ),
        )
        hit = (goal == column) & (lane < span)
        place[pl.ds(128 * j, 128)] = jnp.where(hit, 1.0, 0.0).astype(BF16)
    own_b.wait()
    b_wait(0, False)

    def b_take(d):
        b_wait(d, True)
        b_wait(d, False)

    tokens.loop(1, ny, b_take)

    packed = jnp.concatenate([in_b[j].reshape(count, 128) for j in range(ny)], axis=1)
    fields = jnp.dot(packed, place[...], preferred_element_type=F32)
    query = fields[:, :key_size]
    key = fields[:, key_size : 2 * key_size]
    value = fields[:, 2 * key_size : 2 * key_size + value_size]
    gate = fields[:, 2 * key_size + value_size :]
    half = key_size // 2

    def turned_by(x):
        swapped = jnp.concatenate([x[:, half:], x[:, :half]], axis=1)
        return x * cosine + swapped * sine

    query_rot = turned_by(query).astype(BF16)
    key_f = turned_by(key) * key_size ** (-0.5)
    key_rot = key_f.astype(BF16)
    value_b = value.astype(BF16)
    scores = lax.dot_general(
        query_rot, key_rot, (((1,), (1,)), ((), ())), preferred_element_type=F32
    )
    inner = jnp.dot((scores * grid).astype(BF16), value_b, preferred_element_type=F32)
    decayed = query_rot.astype(F32) * query_decay
    row_at = at_of(iota((count, 1), 0))
    spread = jnp.concatenate(
        [jnp.where(row_at == at, decayed, 0.0).astype(BF16) for at in range(2 * heads)], axis=1
    )
    states = state_b[...].reshape(2 * heads * key_size, value_size)
    heads_out = inner + jnp.dot(spread, states, preferred_element_type=F32)
    normed = heads_out * lax.rsqrt(jnp.mean(heads_out * heads_out, axis=-1, keepdims=True) + epsilon)
    product = gate / (1.0 + jnp.exp(-gate)) * normed
    for c in range(value_size // 128):
        rows_f[c] = product[:, 128 * c : 128 * (c + 1)]
    for i in range(8):
        prop, seq = 2 * (i // 4) + i % 2, (i // 2) % 2
        keys_out[seq, prop] = key_f[i * heads : (i + 1) * heads].astype(BF16)
        values_out[seq, prop] = value[i * heads : (i + 1) * heads].astype(BF16)
    cut = heads * value_size // 2
    for h in range(heads):
        part, at = divmod(h * value_size, cut)
        for c in range(value_size // 128):
            piece = rows_f[c, pl.ds(h, 8, stride=heads), :]
            chunk[part, :, at + 128 * c : at + 128 * (c + 1)] = piece.astype(BF16)

    gated = TorusGather(
        lambda p: chunk.at[p], gated_all, gat_arrived, gat_first, gat_ring, nz, ny
    )
    gated.start_first()
    gated.start_ring()
    keep = [
        pltpu.make_async_copy(chunk.at[p], gated_all.at[p, z, y], local.at[14 + p]) for p in range(2)
    ]
    for each in keep:
        each.start()

    source = iota((4 * seqs, seqs), 0)
    target = iota((4 * seqs, seqs), 1)
    for p in range(4):
        row_seq = 2 * (source >> 3) + ((source >> 1) & 1)
        row_prop = 2 * ((source >> 2) & 1) + (source & 1)
        hit = (row_seq == target) & (row_prop == p)
        order[:, pl.ds(seqs * p, seqs)] = jnp.where(hit, 1.0, 0.0).astype(BF16)
    for k in range(gated.hops()):
        gated.round(k)
    gated.last_arrivals()
    for each in keep:
        each.wait()
    loads[6].wait()
    total = jnp.zeros((wo_v.shape[0], 4 * seqs), F32)
    for part in range(2):
        total += lax.dot_general(
            wo_v[:, part * cut : (part + 1) * cut],
            gated_all[part].reshape(4 * seqs, cut),
            (((1,), (1,)), ((), ())),
            preferred_element_type=F32,
        )
    rounded = total.astype(BF16)
    mine = rounded.shape[0] // 2
    sent_out[0] = rounded[:mine]
    sent_out[1] = rounded[mine:]
    trade = pltpu.make_async_remote_copy(
        src_ref=sent_out.at[1 - tp],
        dst_ref=got_out,
        send_sem=pair_sems.at[2],
        recv_sem=pair_sems.at[3],
        device_id=partner,
        device_id_type=MESH,
    )
    trade.start()
    trade.wait()
    summed = (sent_out[tp].astype(F32) + got_out[...].astype(F32)).astype(BF16)
    result = jnp.dot(summed, order[...], preferred_element_type=F32).astype(BF16)
    for p in range(4):
        ret_out[p] = result[:, p * seqs : (p + 1) * seqs]
    tokens.finish()
    gated.finish()
    tokens.loop(1, nz, lambda d: a_copy(d).wait_send())

    def b_done(d):
        b_copy(d, True).wait_send()
        b_copy(d, False).wait_send()

    tokens.loop(1, ny, b_done)
    b_copy(0, False).wait_send()


def in_hbm(value):
    return pltpu.with_memory_space_constraint(value, pltpu.HBM)


def put_kernel(*refs):
    count = (len(refs) - 1) // 2
    sems = refs[-1]
    copies = [
        pltpu.make_async_copy(refs[i], refs[count + i], sems.at[i]) for i in range(count)
    ]
    for copy in copies:
        copy.start()
    for copy in copies:
        copy.wait()


def put_out(*values):
    return pl.pallas_call(
        put_kernel,
        out_shape=tuple(jax.ShapeDtypeStruct(v.shape, v.dtype) for v in values),
        in_specs=[pl.BlockSpec(memory_space=pl.ANY)] * len(values),
        out_specs=(pl.BlockSpec(memory_space=pltpu.HBM),) * len(values),
        scratch_shapes=[pltpu.SemaphoreType.DMA((len(values),))],
        compiler_params=pltpu.CompilerParams(vmem_limit_bytes=8 * 1024 * 1024),
    )(*values)


def shards(
    nz,
    ny,
    tokens,
    norm_gain,
    query_weight,
    key_weight,
    value_weight,
    gate_weight,
    out_weight,
    decay_rate,
    prior_state,
    last_keys,
    last_values,
    accepted,
    lengths,
):
    _, heads, key_size, value_size = prior_state.shape
    seqs, _, depth = tokens.shape
    width = norm_gain.shape[0]
    kc, vc = query_weight.shape[1], value_weight.shape[1]
    span = 2 * kc + 2 * vc
    count = 8 * heads
    half = key_size // 2
    frequency = jnp.power(10000.0, -jnp.arange(half, dtype=F32) / half)
    frequency = jnp.concatenate([frequency, frequency])[None, :]

    hbm = pl.BlockSpec(memory_space=pltpu.HBM)
    vmem = pl.BlockSpec(memory_space=pltpu.VMEM)
    dma = pltpu.SemaphoreType.DMA
    cut = heads * value_size // 2
    out_cols = out_weight.shape[1]
    retained, state, new_keys, new_values = pl.pallas_call(
        functools.partial(kernel, nz, ny),
        out_shape=(
            jax.ShapeDtypeStruct((4, out_cols // 2, seqs), BF16),
            jax.ShapeDtypeStruct((2 * heads, key_size, value_size), F32),
            jax.ShapeDtypeStruct((2, 4, heads, key_size), BF16),
            jax.ShapeDtypeStruct((2, 4, heads, value_size), BF16),
        ),
        in_specs=[hbm] * 12 + [vmem] * 2,
        out_specs=(vmem,) * 4,
        scratch_shapes=[
            pltpu.VMEM((2, depth, seqs), BF16),
            pltpu.VMEM((2, span, width), BF16),
            pltpu.VMEM((out_cols, heads * value_size), BF16),
            pltpu.VMEM((2 * heads, key_size, value_size), F32),
            pltpu.VMEM((2, 4 * heads, key_size), BF16),
            pltpu.VMEM((2, 4 * heads, value_size), BF16),
            pltpu.SMEM((heads,), F32),
            pltpu.SMEM((2,), jnp.int32),
            pltpu.SMEM((2,), jnp.int32),
            pltpu.VMEM((2, 2, 4 * heads, key_size), F32),
            pltpu.VMEM((2 * heads, key_size, value_size), BF16),
            pltpu.VMEM((2, nz, ny, depth, seqs), BF16),
            pltpu.VMEM((128 * ny, 2 * key_size + 2 * value_size), BF16),
            pltpu.VMEM((4 * seqs, 4 * seqs), BF16),
            pltpu.VMEM((nz, 2, 2, 2 * ny, 128), BF16),
            pltpu.VMEM((nz, 2, 2, 2 * ny, 128), BF16),
            pltpu.VMEM((nz * 8 * ny, 128), F32),
            pltpu.VMEM((ny, 2, 2, 2 * nz, 128), BF16),
            pltpu.VMEM((ny, 2, 2, 2 * nz, 128), BF16),
            pltpu.VMEM((value_size // 128, count, 128), F32),
            pltpu.VMEM((2, 8, cut), BF16),
            pltpu.VMEM((2, nz, ny, 8, cut), BF16),
            pltpu.VMEM((2, out_cols // 2, 4 * seqs), BF16),
            pltpu.VMEM((out_cols // 2, 4 * seqs), BF16),
            dma((22,)),
            dma((2, nz, ny)),
            dma((2, max(nz, ny))),
            dma((2, 2, nz // 2, ny)),
            dma((2, nz, ny)),
            dma((2, max(nz, ny))),
            dma((2, 2, nz // 2, ny)),
            dma((4,)),
            dma((nz,)),
            dma((nz,)),
            dma((ny, 2)),
            dma((ny, 2)),
        ],
        compiler_params=pltpu.CompilerParams(
            collective_id=0, has_side_effects=True, vmem_limit_bytes=48 * 1024 * 1024
        ),
    )(
        *map(
            in_hbm,
            (
                tokens.transpose(1, 2, 0),
                query_weight.T,
                key_weight.T,
                value_weight.T,
                gate_weight.T,
                out_weight.T,
                prior_state.reshape(2 * heads, key_size, value_size),
                last_keys.reshape(2, 4 * heads, key_size),
                last_values.reshape(2, 4 * heads, value_size),
                decay_rate,
                accepted,
                lengths,
            ),
        ),
        norm_gain.astype(F32)[None, :],
        frequency,
    )
    retained, state, new_keys, new_values = put_out(retained, state, new_keys, new_values)
    return (
        retained.transpose(2, 0, 1),
        state.reshape(prior_state.shape),
        new_keys,
        new_values,
    )


def solution(mesh):
    nz = ny = 8
    finer = Mesh(
        mesh.devices.reshape(mesh.shape["dp"], nz, ny, mesh.shape["tp"]),
        ("dp", "kv_0", "kv_1", "tp"),
    )
    return jax.shard_map(
        functools.partial(shards, nz, ny),
        mesh=finer,
        in_specs=(
            P("dp", None, KV),
            P(),
            P(None, TP_KV),
            P(None, TP_KV),
            P(None, TP_KV),
            P(None, TP_KV),
            P("tp", KV),
            P("tp"),
            P(DP_KV, "tp", None, None),
            P(DP_KV, None, "tp", None),
            P(DP_KV, None, "tp", None),
            P(DP_KV),
            P(DP_KV),
        ),
        out_specs=(
            P("dp", None, KV_TP),
            P(DP_KV, "tp", None, None),
            P(DP_KV, None, "tp", None),
            P(DP_KV, None, "tp", None),
        ),
        check_vma=False,
    )
```

```python
import functools

import jax
import jax.numpy as jnp
from jax import lax
from jax.experimental import pallas as pl
from jax.experimental.pallas import tpu as pltpu
from jax.sharding import Mesh
from jax.sharding import PartitionSpec as P

KV = ("kv_0", "kv_1")
TP_KV = ("tp", "kv_0", "kv_1")
DP_KV = ("dp", "kv_0", "kv_1")
KV_TP = ("kv_0", "kv_1", "tp")
MESH = pl.DeviceIdType.MESH
F32, BF16 = jnp.float32, jnp.bfloat16

epsilon = 1e-06


def wrap(i, n):
    return i & (n - 1)


def far_first(i, n):
    return wrap(n // 2 + (1 - 2 * (i & 1)) * (i >> 1), n)


class TorusGather:
    groups = 4

    def __init__(self, own, held, arrived, ring_arrived, first_sent, ring_sent, nz, ny):
        self.own, self.held, self.arrived, self.ring_arrived = own, held, arrived, ring_arrived
        self.first_sent, self.ring_sent = first_sent, ring_sent
        z, y = lax.axis_index("kv_0"), lax.axis_index("kv_1")
        self.partner = {"tp": 1 - lax.axis_index("tp")}
        self.first = ((y, ny, "kv_1"), (z, nz, "kv_0"))
        self.second = ((z, nz, "kv_0"), (y, ny, "kv_1"))
        self.hops = nz // 2
        self.size = ny // self.groups

    def at(self, ref, p, f, s):
        return ref.at[p, s, f] if p == 0 else ref.at[p, f, s]

    def copy(self, target, source, sent, arrived, device):
        return pltpu.make_async_remote_copy(
            src_ref=source,
            dst_ref=target,
            send_sem=sent,
            recv_sem=arrived,
            device_id=device,
            device_id_type=MESH,
        )

    def first_copy(self, p, d):
        (f, n, axis), (s, _, _) = self.first[p], self.second[p]
        return self.copy(
            self.at(self.held, p, f, s),
            self.own(p),
            self.first_sent.at[p, d],
            self.at(self.arrived, p, f, s),
            {axis: wrap(f + d, n)},
        )

    def start_first(self):
        def send(i):
            for p in range(2):
                self.first_copy(p, far_first(i, self.first[p][1])).start()

        self.loop(1, self.first[0][1], send)
        for p in range(2):
            (f, _, _), (s, _, _) = self.first[p], self.second[p]
            pltpu.make_async_copy(
                self.own(p), self.at(self.held, p, f, s), self.at(self.arrived, p, f, s)
            ).start()

    def group(self, p, i):
        f = self.first[p][0]
        return wrap(f // self.size + i, self.groups)

    def group_at(self, p, q, s):
        return self.at(self.held, p, pl.ds(q * self.size, self.size), s)

    def ring_copy(self, p, k, i, way):
        s, n, axis = self.second[p]
        q, origin = self.group(p, i), wrap(s - way * k + n, n)
        block = self.group_at(p, q, origin)
        return self.copy(
            block,
            block,
            self.ring_sent.at[p, (1 + way) // 2, k, i],
            self.ring_arrived.at[p, origin, q],
            {axis: wrap(s + way + n, n)},
        )

    def wait_chunk(self, p, f, s):
        chunk = self.at(self.held, p, f, s)
        self.copy(
            chunk, chunk, self.first_sent.at[0, 0], self.at(self.arrived, p, f, s), self.partner
        ).wait_recv()

    def wait_group(self, p, i, s):
        q = self.group(p, i)
        block = self.group_at(p, q, s)
        self.copy(
            block, block, self.first_sent.at[0, 0], self.ring_arrived.at[p, s, q], self.partner
        ).wait_recv()

    def pass_on(self, k, i, ways):
        for p in range(2):
            s, n, _ = self.second[p]
            if k == 0:
                for e in range(self.size):
                    self.wait_chunk(p, self.group(p, i) * self.size + e, s)
                for way in ways:
                    self.ring_copy(p, k, i, way).start()
            else:
                for way in (1, -1):
                    self.wait_group(p, i, wrap(s - way * k + n, n))
                    if way in ways:
                        self.ring_copy(p, k, i, way).start()

    def loop(self, low, high, step):
        def body(i, _):
            step(i)
            return 0

        lax.fori_loop(low, high, body, 0)

    def over_groups(self, k, step):
        if k < self.hops - 1:
            self.loop(0, self.groups, lambda i: step(i, (1, -1)))
        else:
            self.loop(0, self.groups // 2, lambda i: step(i, (1,)))
            self.loop(self.groups // 2, self.groups, lambda i: step(i, (-1,)))

    def round(self, k, beside=None):
        def step(i, ways):
            self.pass_on(k, i, ways)
            if beside is not None:
                beside(i)

        self.over_groups(k, step)

    def last_arrivals(self):
        def take(i):
            for p in range(2):
                s, n, _ = self.second[p]
                self.wait_group(p, i, wrap(s + self.hops, n))

        self.loop(0, self.groups, take)

    def finish(self):
        def first_done(d):
            for p in range(2):
                self.first_copy(p, d).wait_send()

        self.loop(1, self.first[0][1], first_done)
        for k in range(self.hops):

            def done(i, ways, k=k):
                for p in range(2):
                    for way in ways:
                        self.ring_copy(p, k, i, way).wait_send()

            self.over_groups(k, done)


def iota(shape, dim):
    return lax.broadcasted_iota(jnp.int32, shape, dim)


def kernel(
    nz,
    ny,
    tok,
    wq,
    wk,
    wv,
    wg,
    wo,
    prior,
    last_k_in,
    last_v_in,
    decay_in,
    accepted_in,
    lengths_in,
    gain,
    frequency,
    ret_out,
    state_out,
    keys_out,
    values_out,
    tok_v,
    weights,
    wo_v,
    prior_v,
    last_k,
    last_v,
    decay,
    accepted,
    lengths,
    weighted_keys,
    state_b,
    tokens_all,
    place,
    order,
    out_a,
    in_a,
    mid,
    out_b,
    in_b,
    rows_f,
    chunk,
    gated_all,
    sent_out,
    got_out,
    local,
    tok_arrived,
    tok_passed,
    tok_first,
    tok_ring,
    gat_arrived,
    gat_passed,
    gat_first,
    gat_ring,
    pair_sems,
    a_sent,
    a_got,
    b_sent,
    b_got,
):
    z, y, tp = lax.axis_index("kv_0"), lax.axis_index("kv_1"), lax.axis_index("tp")
    heads, seqs = nz, 2 * nz * ny
    kc = wq.shape[0]
    vc = wv.shape[0]
    span = 2 * kc + 2 * vc
    partner = {"tp": 1 - tp}

    loads = [
        pltpu.make_async_copy(tok.at[pl.ds(2 * tp, 2)], tok_v, local.at[0]),
        pltpu.make_async_copy(wq, weights.at[tp, pl.ds(0, kc)], local.at[1]),
        pltpu.make_async_copy(wk, weights.at[tp, pl.ds(kc, kc)], local.at[2]),
        pltpu.make_async_copy(wv, weights.at[tp, pl.ds(2 * kc, vc)], local.at[3]),
        pltpu.make_async_copy(wg, weights.at[tp, pl.ds(2 * kc + vc, vc)], local.at[4]),
        pltpu.make_async_copy(prior, prior_v, local.at[5]),
        pltpu.make_async_copy(wo, wo_v, local.at[6]),
    ]
    small_loads = [
        pltpu.make_async_copy(source, target, local.at[17 + i])
        for i, (source, target) in enumerate(
            (
                (last_k_in, last_k),
                (last_v_in, last_v),
                (decay_in, decay),
                (accepted_in, accepted),
                (lengths_in, lengths),
            )
        )
    ]
    for load in loads + small_loads:
        load.start()

    barrier = pltpu.get_barrier_semaphore()

    def greet(device):
        pl.semaphore_signal(barrier, inc=1, device_id=device, device_id_type=MESH)

    def greet_y(d, _):
        other = wrap(y + d, ny)
        greet({"kv_1": other})
        greet({"kv_1": other, "tp": 1 - tp})
        return 0

    def greet_z(d, _):
        greet({"kv_0": wrap(z + d, nz)})
        return 0

    lax.fori_loop(1, ny, greet_y, 0)
    lax.fori_loop(1, nz, greet_z, 0)
    greet(partner)
    pl.semaphore_wait(barrier, 2 * (ny - 1) + (nz - 1) + 1)

    loads[0].wait()
    tokens = TorusGather(
        lambda p: tok_v.at[p], tokens_all, tok_arrived, tok_passed, tok_first, tok_ring, nz, ny
    )
    tokens.start_first()
    for load in loads[1:5]:
        load.wait()
    swap = pltpu.make_async_remote_copy(
        src_ref=weights.at[tp],
        dst_ref=weights.at[tp],
        send_sem=pair_sems.at[0],
        recv_sem=pair_sems.at[1],
        device_id=partner,
        device_id_type=MESH,
    )
    swap.start()

    key_size, value_size = ny * kc, ny * vc

    loads[5].wait()
    for load in small_loads:
        load.wait()
    rows, count = 4 * heads, 8 * heads
    head_of = iota((rows, 1), 0) & (heads - 1)

    def by_head(shape):
        head = iota(shape, 0) & (heads - 1)
        table = jnp.zeros(shape, F32)
        for h in range(heads):
            table = jnp.where(head == h, -decay[h], table)
        return table

    taken_decay = by_head((rows, 128))
    before = iota((rows, 128), 0) >> (heads.bit_length() - 1)
    for s in range(2):
        power = jnp.maximum(accepted[s] - 1 - before, 0).astype(F32)
        key_weights = jnp.where(before < accepted[s], jnp.exp(taken_decay * power), 0.0)
        weighted = last_k[s].astype(F32) * key_weights
        high = weighted.astype(BF16).astype(F32)
        weighted_keys[s, 0] = high
        weighted_keys[s, 1] = weighted - high

    def one_head(h):
        mine = head_of == h
        for s in range(2):
            both = jnp.concatenate(
                [jnp.where(mine, weighted_keys[s, part], 0.0) for part in range(2)], axis=0
            )
            values = jnp.concatenate([last_v[s], last_v[s]], axis=0)
            update = lax.dot_general(
                both.astype(BF16), values, (((0,), (0,)), ((), ())), preferred_element_type=F32
            )
            at = s * heads + h
            power = jnp.full((1, value_size), -decay[h] * accepted[s].astype(F32), F32)
            fresh = jnp.exp(power) * prior_v[at] + update
            state_out[at] = fresh
            state_b[at] = fresh.astype(BF16)

    def some_heads(i):
        for e in range(heads // tokens.groups):
            one_head(i * (heads // tokens.groups) + e)

    tokens.round(0, some_heads)

    swap.wait()

    blocks = span // 16

    def scale_rows(i):
        at = pl.ds(pl.multiple_of(i * 16, 16), 16)
        for side in range(2):
            weights[side, at] = (weights[side, at].astype(F32) * gain[...]).astype(BF16)

    for k in range(1, tokens.hops):
        tokens.round(k, scale_rows if k < tokens.hops - 1 else None)
        if k == 1:
            scale_rows = lambda i, first=scale_rows: pl.when(i + 4 < blocks)(lambda: first(i + 4))
    tokens.last_arrivals()

    depth = tok_v.shape[1]
    width = nz * ny * depth
    for p in range(2):
        total = jnp.zeros((2 * span, seqs), F32)
        squares = jnp.zeros((1, seqs), F32)
        for c in range(nz):
            block = tokens_all[p, c].reshape(ny * depth, seqs)
            cut = pl.ds(c * ny * depth, ny * depth)
            total += jnp.dot(
                weights[:, :, cut].reshape(2 * span, ny * depth), block, preferred_element_type=F32
            )
            floats = block.astype(F32)
            squares += jnp.sum(floats * floats, axis=0, keepdims=True)
        scaled = total * lax.rsqrt(squares / width + epsilon)
        for side in range(2):
            part = jnp.concatenate(
                [scaled[side * span : (side + 1) * span], jnp.zeros((128 - span, seqs), F32)], axis=0
            )
            turned = part.T.astype(BF16)
            for to in range(nz):
                out_a[to, side, p] = turned[2 * ny * to : 2 * ny * (to + 1)]

    def a_copy(d):
        to = wrap(z + d, nz)
        return pltpu.make_async_remote_copy(
            src_ref=out_a.at[to],
            dst_ref=in_a.at[z],
            send_sem=a_sent.at[d],
            recv_sem=a_got.at[z],
            device_id={"kv_0": to},
            device_id_type=MESH,
        )

    def a_wait(d):
        came = wrap(z + d, nz)
        pltpu.make_async_remote_copy(
            src_ref=in_a.at[came],
            dst_ref=in_a.at[came],
            send_sem=a_sent.at[0],
            recv_sem=a_got.at[came],
            device_id=partner,
            device_id_type=MESH,
        ).wait_recv()

    tokens.loop(1, nz, lambda i: a_copy(far_first(i, nz)).start())
    own_a = pltpu.make_async_copy(out_a.at[z], in_a.at[z], local.at[10])
    own_a.start()

    shift = heads.bit_length() - 1

    def prop_of(i):
        return 2 * (i >> (shift + 2)) + ((i >> shift) & 1)

    def at_of(i):
        return ((i >> (shift + 1)) & 1) * heads + (i & (heads - 1))

    row = iota((count, 128), 0)
    first = jnp.where((row >> (shift + 1)) & 1 == 0, lengths[0] + accepted[0], lengths[1] + accepted[1])
    angles = (first + prop_of(row)).astype(F32) * frequency[...]
    cosine = jnp.cos(angles)
    lane_sign = jnp.where(iota((count, 128), 1) < key_size // 2, -1.0, 1.0)
    sine = jnp.sin(angles) * lane_sign
    decays = by_head((count, 128))
    query_decay = jnp.exp(decays * (prop_of(row) + 1).astype(F32))
    other = iota((count, count), 1)
    here = row[:, :count]
    offset = prop_of(here) - prop_of(other)
    grid = jnp.where(
        (at_of(here) == at_of(other)) & (offset >= 0),
        jnp.exp(decays[:, :count] * jnp.maximum(offset, 0).astype(F32)),
        0.0,
    )

    own_a.wait()
    tokens.loop(1, nz, a_wait)

    mid[...] = in_a[...].reshape(nz * 4 * 2 * ny, 128).astype(F32)
    stride = 4 * 2 * ny
    for to in range(ny):
        for side in range(2):
            for s in range(2):
                parts = [
                    mid[pl.ds(side * 4 * ny + p * 2 * ny + 2 * to + s, nz, stride=stride), :]
                    for p in range(2)
                ]
                out_b[to, side, s] = jnp.concatenate(parts, axis=0).astype(BF16)

    def b_copy(d, same):
        to = wrap(y + d, ny)
        side = tp if same else 1 - tp
        return pltpu.make_async_remote_copy(
            src_ref=out_b.at[to, side],
            dst_ref=in_b.at[y, tp],
            send_sem=b_sent.at[d, side],
            recv_sem=b_got.at[y, tp],
            device_id={"kv_1": to, "tp": side},
            device_id_type=MESH,
        )

    def b_wait(d, same):
        came = wrap(y + d, ny)
        side = tp if same else 1 - tp
        pltpu.make_async_remote_copy(
            src_ref=in_b.at[came, side],
            dst_ref=in_b.at[came, side],
            send_sem=b_sent.at[0, 0],
            recv_sem=b_got.at[came, side],
            device_id=partner,
            device_id_type=MESH,
        ).wait_recv()

    def b_start(i):
        d = far_first(i, ny)
        b_copy(d, True).start()
        b_copy(d, False).start()

    tokens.loop(1, ny, b_start)
    b_copy(0, False).start()
    own_b = pltpu.make_async_copy(out_b.at[y, tp], in_b.at[y, tp], local.at[11])
    own_b.start()

    lane = iota((128, 2 * key_size + 2 * value_size), 0)
    column = iota((128, 2 * key_size + 2 * value_size), 1)
    for j in range(ny):
        goal = jnp.where(
            lane < kc,
            kc * j + lane,
            jnp.where(
                lane < 2 * kc,
                key_size + kc * j + lane - kc,
                jnp.where(
                    lane < 2 * kc + vc,
                    2 * key_size + vc * j + lane - 2 * kc,
                    2 * key_size + value_size + vc * j + lane - 2 * kc - vc,
                ),
            ),
        )
        hit = (goal == column) & (lane < span)
        place[pl.ds(128 * j, 128)] = jnp.where(hit, 1.0, 0.0).astype(BF16)
    own_b.wait()
    b_wait(0, False)

    def b_take(d):
        b_wait(d, True)
        b_wait(d, False)

    tokens.loop(1, ny, b_take)

    packed = jnp.concatenate([in_b[j].reshape(count, 128) for j in range(ny)], axis=1)
    fields = jnp.dot(packed, place[...], preferred_element_type=F32)
    query = fields[:, :key_size]
    key = fields[:, key_size : 2 * key_size]
    value = fields[:, 2 * key_size : 2 * key_size + value_size]
    gate = fields[:, 2 * key_size + value_size :]
    half = key_size // 2

    def turned_by(x):
        swapped = jnp.concatenate([x[:, half:], x[:, :half]], axis=1)
        return x * cosine + swapped * sine

    query_rot = turned_by(query).astype(BF16)
    key_f = turned_by(key) * key_size ** (-0.5)
    key_rot = key_f.astype(BF16)
    value_b = value.astype(BF16)
    scores = lax.dot_general(
        query_rot, key_rot, (((1,), (1,)), ((), ())), preferred_element_type=F32
    )
    inner = jnp.dot((scores * grid).astype(BF16), value_b, preferred_element_type=F32)
    decayed = query_rot.astype(F32) * query_decay
    row_at = at_of(iota((count, 1), 0))
    spread = jnp.concatenate(
        [jnp.where(row_at == at, decayed, 0.0).astype(BF16) for at in range(2 * heads)], axis=1
    )
    states = state_b[...].reshape(2 * heads * key_size, value_size)
    heads_out = inner + jnp.dot(spread, states, preferred_element_type=F32)
    normed = heads_out * lax.rsqrt(jnp.mean(heads_out * heads_out, axis=-1, keepdims=True) + epsilon)
    product = gate / (1.0 + jnp.exp(-gate)) * normed
    for c in range(value_size // 128):
        rows_f[c] = product[:, 128 * c : 128 * (c + 1)]
    for i in range(8):
        prop, seq = 2 * (i // 4) + i % 2, (i // 2) % 2
        keys_out[seq, prop] = key_f[i * heads : (i + 1) * heads].astype(BF16)
        values_out[seq, prop] = value[i * heads : (i + 1) * heads].astype(BF16)
    cut = heads * value_size // 2
    for h in range(heads):
        part, at = divmod(h * value_size, cut)
        for c in range(value_size // 128):
            piece = rows_f[c, pl.ds(h, 8, stride=heads), :]
            chunk[part, :, at + 128 * c : at + 128 * (c + 1)] = piece.astype(BF16)

    gated = TorusGather(
        lambda p: chunk.at[p], gated_all, gat_arrived, gat_passed, gat_first, gat_ring, nz, ny
    )
    gated.start_first()
    source = iota((4 * seqs, seqs), 0)
    target = iota((4 * seqs, seqs), 1)
    for p in range(4):
        row_seq = 2 * (source >> 3) + ((source >> 1) & 1)
        row_prop = 2 * ((source >> 2) & 1) + (source & 1)
        hit = (row_seq == target) & (row_prop == p)
        order[:, pl.ds(seqs * p, seqs)] = jnp.where(hit, 1.0, 0.0).astype(BF16)
    for k in range(gated.hops):
        gated.round(k)
    gated.last_arrivals()
    loads[6].wait()
    total = jnp.zeros((wo_v.shape[0], 4 * seqs), F32)
    for part in range(2):
        total += lax.dot_general(
            wo_v[:, part * cut : (part + 1) * cut],
            gated_all[part].reshape(4 * seqs, cut),
            (((1,), (1,)), ((), ())),
            preferred_element_type=F32,
        )
    rounded = total.astype(BF16)
    mine = rounded.shape[0] // 2
    sent_out[0] = rounded[:mine]
    sent_out[1] = rounded[mine:]
    trade = pltpu.make_async_remote_copy(
        src_ref=sent_out.at[1 - tp],
        dst_ref=got_out,
        send_sem=pair_sems.at[2],
        recv_sem=pair_sems.at[3],
        device_id=partner,
        device_id_type=MESH,
    )
    trade.start()
    trade.wait()
    summed = (sent_out[tp].astype(F32) + got_out[...].astype(F32)).astype(BF16)
    result = jnp.dot(summed, order[...], preferred_element_type=F32).astype(BF16)
    for p in range(4):
        ret_out[p] = result[:, p * seqs : (p + 1) * seqs]
    tokens.finish()
    gated.finish()
    tokens.loop(1, nz, lambda d: a_copy(d).wait_send())

    def b_done(d):
        b_copy(d, True).wait_send()
        b_copy(d, False).wait_send()

    tokens.loop(1, ny, b_done)
    b_copy(0, False).wait_send()


def in_hbm(value):
    return pltpu.with_memory_space_constraint(value, pltpu.HBM)


def put_kernel(*refs):
    count = (len(refs) - 1) // 2
    sems = refs[-1]
    copies = [
        pltpu.make_async_copy(refs[i], refs[count + i], sems.at[i]) for i in range(count)
    ]
    for copy in copies:
        copy.start()
    for copy in copies:
        copy.wait()


def put_out(*values):
    return pl.pallas_call(
        put_kernel,
        out_shape=tuple(jax.ShapeDtypeStruct(v.shape, v.dtype) for v in values),
        in_specs=[pl.BlockSpec(memory_space=pl.ANY)] * len(values),
        out_specs=(pl.BlockSpec(memory_space=pltpu.HBM),) * len(values),
        scratch_shapes=[pltpu.SemaphoreType.DMA((len(values),))],
        compiler_params=pltpu.CompilerParams(vmem_limit_bytes=8 * 1024 * 1024),
    )(*values)


def shards(
    nz,
    ny,
    tokens,
    norm_gain,
    query_weight,
    key_weight,
    value_weight,
    gate_weight,
    out_weight,
    decay_rate,
    prior_state,
    last_keys,
    last_values,
    accepted,
    lengths,
):
    _, heads, key_size, value_size = prior_state.shape
    seqs, _, depth = tokens.shape
    width = norm_gain.shape[0]
    kc, vc = query_weight.shape[1], value_weight.shape[1]
    span = 2 * kc + 2 * vc
    count = 8 * heads
    half = key_size // 2
    frequency = jnp.power(10000.0, -jnp.arange(half, dtype=F32) / half)
    frequency = jnp.concatenate([frequency, frequency])[None, :]

    hbm = pl.BlockSpec(memory_space=pltpu.HBM)
    vmem = pl.BlockSpec(memory_space=pltpu.VMEM)
    dma = pltpu.SemaphoreType.DMA
    cut = heads * value_size // 2
    out_cols = out_weight.shape[1]
    retained, state, new_keys, new_values = pl.pallas_call(
        functools.partial(kernel, nz, ny),
        out_shape=(
            jax.ShapeDtypeStruct((4, out_cols // 2, seqs), BF16),
            jax.ShapeDtypeStruct((2 * heads, key_size, value_size), F32),
            jax.ShapeDtypeStruct((2, 4, heads, key_size), BF16),
            jax.ShapeDtypeStruct((2, 4, heads, value_size), BF16),
        ),
        in_specs=[hbm] * 12 + [vmem] * 2,
        out_specs=(vmem,) * 4,
        scratch_shapes=[
            pltpu.VMEM((2, depth, seqs), BF16),
            pltpu.VMEM((2, span, width), BF16),
            pltpu.VMEM((out_cols, heads * value_size), BF16),
            pltpu.VMEM((2 * heads, key_size, value_size), F32),
            pltpu.VMEM((2, 4 * heads, key_size), BF16),
            pltpu.VMEM((2, 4 * heads, value_size), BF16),
            pltpu.SMEM((heads,), F32),
            pltpu.SMEM((2,), jnp.int32),
            pltpu.SMEM((2,), jnp.int32),
            pltpu.VMEM((2, 2, 4 * heads, key_size), F32),
            pltpu.VMEM((2 * heads, key_size, value_size), BF16),
            pltpu.VMEM((2, nz, ny, depth, seqs), BF16),
            pltpu.VMEM((128 * ny, 2 * key_size + 2 * value_size), BF16),
            pltpu.VMEM((4 * seqs, 4 * seqs), BF16),
            pltpu.VMEM((nz, 2, 2, 2 * ny, 128), BF16),
            pltpu.VMEM((nz, 2, 2, 2 * ny, 128), BF16),
            pltpu.VMEM((nz * 8 * ny, 128), F32),
            pltpu.VMEM((ny, 2, 2, 2 * nz, 128), BF16),
            pltpu.VMEM((ny, 2, 2, 2 * nz, 128), BF16),
            pltpu.VMEM((value_size // 128, count, 128), F32),
            pltpu.VMEM((2, 8, cut), BF16),
            pltpu.VMEM((2, nz, ny, 8, cut), BF16),
            pltpu.VMEM((2, out_cols // 2, 4 * seqs), BF16),
            pltpu.VMEM((out_cols // 2, 4 * seqs), BF16),
            dma((22,)),
            dma((2, nz, ny)),
            dma((2, max(nz, ny), TorusGather.groups)),
            dma((2, max(nz, ny))),
            dma((2, 2, nz // 2, TorusGather.groups)),
            dma((2, nz, ny)),
            dma((2, max(nz, ny), TorusGather.groups)),
            dma((2, max(nz, ny))),
            dma((2, 2, nz // 2, TorusGather.groups)),
            dma((4,)),
            dma((nz,)),
            dma((nz,)),
            dma((ny, 2)),
            dma((ny, 2)),
        ],
        compiler_params=pltpu.CompilerParams(
            collective_id=0, has_side_effects=True, vmem_limit_bytes=48 * 1024 * 1024
        ),
    )(
        *map(
            in_hbm,
            (
                tokens.transpose(1, 2, 0),
                query_weight.T,
                key_weight.T,
                value_weight.T,
                gate_weight.T,
                out_weight.T,
                prior_state.reshape(2 * heads, key_size, value_size),
                last_keys.reshape(2, 4 * heads, key_size),
                last_values.reshape(2, 4 * heads, value_size),
                decay_rate,
                accepted,
                lengths,
            ),
        ),
        norm_gain.astype(F32)[None, :],
        frequency,
    )
    retained, state, new_keys, new_values = put_out(retained, state, new_keys, new_values)
    return (
        retained.transpose(2, 0, 1),
        state.reshape(prior_state.shape),
        new_keys,
        new_values,
    )


def solution(mesh):
    nz = ny = 8
    finer = Mesh(
        mesh.devices.reshape(mesh.shape["dp"], nz, ny, mesh.shape["tp"]),
        ("dp", "kv_0", "kv_1", "tp"),
    )
    return jax.shard_map(
        functools.partial(shards, nz, ny),
        mesh=finer,
        in_specs=(
            P("dp", None, KV),
            P(),
            P(None, TP_KV),
            P(None, TP_KV),
            P(None, TP_KV),
            P(None, TP_KV),
            P("tp", KV),
            P("tp"),
            P(DP_KV, "tp", None, None),
            P(DP_KV, None, "tp", None),
            P(DP_KV, None, "tp", None),
            P(DP_KV),
            P(DP_KV),
        ),
        out_specs=(
            P("dp", None, KV_TP),
            P(DP_KV, "tp", None, None),
            P(DP_KV, None, "tp", None),
            P(DP_KV, None, "tp", None),
        ),
        check_vma=False,
    )
```

```python
import functools

import jax
import jax.numpy as jnp
from jax import lax
from jax.experimental import pallas as pl
from jax.experimental.pallas import tpu as pltpu
from jax.sharding import Mesh
from jax.sharding import PartitionSpec as P

KV = ("kv_0", "kv_1")
TP_KV = ("tp", "kv_0", "kv_1")
DP_KV = ("dp", "kv_0", "kv_1")
KV_TP = ("kv_0", "kv_1", "tp")
MESH = pl.DeviceIdType.MESH
F32, BF16 = jnp.float32, jnp.bfloat16

epsilon = 1e-06


def wrap(i, n):
    return i & (n - 1)


def far_first(i, n):
    return wrap(n // 2 + (1 - 2 * (i & 1)) * (i >> 1), n)


class TorusGather:
    groups = 4

    def __init__(self, own, held, arrived, ring_arrived, first_sent, ring_sent, nz, ny):
        self.own, self.held, self.arrived, self.ring_arrived = own, held, arrived, ring_arrived
        self.first_sent, self.ring_sent = first_sent, ring_sent
        z, y = lax.axis_index("kv_0"), lax.axis_index("kv_1")
        self.partner = {"tp": 1 - lax.axis_index("tp")}
        self.first = ((y, ny, "kv_1"), (z, nz, "kv_0"))
        self.second = ((z, nz, "kv_0"), (y, ny, "kv_1"))
        self.hops = nz // 2
        self.size = ny // self.groups

    def at(self, ref, p, f, s):
        return ref.at[p, s, f] if p == 0 else ref.at[p, f, s]

    def copy(self, target, source, sent, arrived, device):
        return pltpu.make_async_remote_copy(
            src_ref=source,
            dst_ref=target,
            send_sem=sent,
            recv_sem=arrived,
            device_id=device,
            device_id_type=MESH,
        )

    def first_copy(self, p, d):
        (f, n, axis), (s, _, _) = self.first[p], self.second[p]
        return self.copy(
            self.at(self.held, p, f, s),
            self.own(p),
            self.first_sent.at[p, d],
            self.at(self.arrived, p, f, s),
            {axis: wrap(f + d, n)},
        )

    def start_first(self):
        def send(i):
            for p in range(2):
                self.first_copy(p, far_first(i, self.first[p][1])).start()

        self.loop(1, self.first[0][1], send)
        for p in range(2):
            (f, _, _), (s, _, _) = self.first[p], self.second[p]
            pltpu.make_async_copy(
                self.own(p), self.at(self.held, p, f, s), self.at(self.arrived, p, f, s)
            ).start()

    def group(self, p, i):
        f = self.first[p][0]
        return wrap(f // self.size + i, self.groups)

    def group_at(self, p, q, s):
        return self.at(self.held, p, pl.ds(q * self.size, self.size), s)

    def ring_copy(self, p, k, i, way):
        s, n, axis = self.second[p]
        q, origin = self.group(p, i), wrap(s - way * k + n, n)
        block = self.group_at(p, q, origin)
        return self.copy(
            block,
            block,
            self.ring_sent.at[p, (1 + way) // 2, k, i],
            self.ring_arrived.at[p, origin, q],
            {axis: wrap(s + way + n, n)},
        )

    def wait_chunk(self, p, f, s):
        chunk = self.at(self.held, p, f, s)
        self.copy(
            chunk, chunk, self.first_sent.at[0, 0], self.at(self.arrived, p, f, s), self.partner
        ).wait_recv()

    def wait_group(self, p, i, s):
        q = self.group(p, i)
        block = self.group_at(p, q, s)
        self.copy(
            block, block, self.first_sent.at[0, 0], self.ring_arrived.at[p, s, q], self.partner
        ).wait_recv()

    def pass_on(self, k, i, ways):
        for p in range(2):
            s, n, _ = self.second[p]
            if k == 0:
                for e in range(self.size):
                    self.wait_chunk(p, self.group(p, i) * self.size + e, s)
                for way in ways:
                    self.ring_copy(p, k, i, way).start()
            else:
                for way in (1, -1):
                    self.wait_group(p, i, wrap(s - way * k + n, n))
                    if way in ways:
                        self.ring_copy(p, k, i, way).start()

    def loop(self, low, high, step):
        def body(i, _):
            step(i)
            return 0

        lax.fori_loop(low, high, body, 0)

    def over_groups(self, k, step):
        if k < self.hops - 1:
            self.loop(0, self.groups, lambda i: step(i, (1, -1)))
        else:
            self.loop(0, self.groups // 2, lambda i: step(i, (1,)))
            self.loop(self.groups // 2, self.groups, lambda i: step(i, (-1,)))

    def round(self, k, beside=None):
        def step(i, ways):
            self.pass_on(k, i, ways)
            if beside is not None:
                beside(i)

        self.over_groups(k, step)

    def last_arrivals(self):
        def take(i):
            for p in range(2):
                s, n, _ = self.second[p]
                self.wait_group(p, i, wrap(s + self.hops, n))

        self.loop(0, self.groups, take)

    def finish(self):
        def first_done(d):
            for p in range(2):
                self.first_copy(p, d).wait_send()

        self.loop(1, self.first[0][1], first_done)
        for k in range(self.hops):

            def done(i, ways, k=k):
                for p in range(2):
                    for way in ways:
                        self.ring_copy(p, k, i, way).wait_send()

            self.over_groups(k, done)


class WeightRing:
    def __init__(self, held, arrived, sent, side_arrived, side_sent, on_arrived, on_sent, nx, nz, ny):
        self.held, self.arrived, self.sent = held, arrived, sent
        self.side_arrived, self.side_sent = side_arrived, side_sent
        self.on_arrived, self.on_sent = on_arrived, on_sent
        self.x, self.nx = lax.axis_index("dp"), nx
        z, y = lax.axis_index("kv_0"), lax.axis_index("kv_1")
        self.partner = {"tp": 1 - lax.axis_index("tp")}
        self.second = ((z, nz, "kv_0"), (y, ny, "kv_1"))
        self.hops = nz // 2
        self.rows = held.shape[2] // nx

    def block(self, p, origin, x):
        return self.held.at[p, origin, pl.ds(pl.multiple_of(self.rows * x, self.rows), self.rows)]

    def copy(self, block, sent, arrived, device):
        return pltpu.make_async_remote_copy(
            src_ref=block,
            dst_ref=block,
            send_sem=sent,
            recv_sem=arrived,
            device_id=device,
            device_id_type=MESH,
        )

    def ring_copy(self, p, k, way):
        s, n, axis = self.second[p]
        origin = wrap(s - way * k + n, n)
        return self.copy(
            self.block(p, origin, self.x),
            self.sent.at[p, (1 + way) // 2, k],
            self.arrived.at[p, origin],
            {axis: wrap(s + way + n, n)},
        )

    def side_copy(self, p, origin, way):
        at = (1 + way) // 2
        return self.copy(
            self.block(p, origin, self.x),
            self.side_sent.at[p, at, origin],
            self.side_arrived.at[p, at, origin],
            {"dp": wrap(self.x + way + self.nx, self.nx)},
        )

    def on_way(self, p):
        return 1 - 2 * p

    def on_copy(self, p):
        way = self.on_way(p)
        x = wrap(self.x - way + self.nx, self.nx)
        block = self.held.at[p, :, pl.ds(pl.multiple_of(self.rows * x, self.rows), self.rows)]
        return self.copy(
            block,
            self.on_sent.at[p],
            self.on_arrived.at[p],
            {"dp": wrap(self.x + way + self.nx, self.nx)},
        )

    def forward_ways(self, p, k):
        if k < self.hops - 1:
            return (1, -1)
        return (self.on_way(p),) if k == self.hops - 1 else ()

    def step(self, k):
        for p in range(2):
            s, n, _ = self.second[p]
            for way in (1,) if k in (0, self.hops) else (1, -1):
                origin = wrap(s - way * k + n, n)
                if k > 0:
                    self.copy(
                        self.block(p, origin, self.x),
                        self.sent.at[0, 0, 0],
                        self.arrived.at[p, origin],
                        self.partner,
                    ).wait_recv()
                ways = self.forward_ways(p, k)
                for to in ways if k == 0 else (way,):
                    if to in ways:
                        self.ring_copy(p, k, to).start()
                for to in (1, -1):
                    self.side_copy(p, origin, to).start()

    def side_wait(self, p, way):
        x = wrap(self.x - way + self.nx, self.nx)

        def take(origin, _):
            self.copy(
                self.block(p, origin, x),
                self.sent.at[0, 0, 0],
                self.side_arrived.at[p, (1 + way) // 2, origin],
                self.partner,
            ).wait_recv()
            return 0

        lax.fori_loop(0, self.second[p][1], take, 0)

    def share_on(self):
        for p in range(2):
            self.side_wait(p, self.on_way(p))
            self.on_copy(p).start()

    def all_here(self):
        for p in range(2):
            self.side_wait(p, -self.on_way(p))
            self.on_copy(p).wait_recv()

    def finish(self):
        for p in range(2):
            for k in range(self.hops):
                for way in self.forward_ways(p, k):
                    self.ring_copy(p, k, way).wait_send()

            def done(origin, _, p=p):
                for way in (1, -1):
                    self.side_copy(p, origin, way).wait_send()
                return 0

            lax.fori_loop(0, self.second[p][1], done, 0)
            self.on_copy(p).wait_send()


def iota(shape, dim):
    return lax.broadcasted_iota(jnp.int32, shape, dim)


def kernel(
    nx,
    nz,
    ny,
    tok,
    wq,
    wk,
    wv,
    wg,
    wo,
    prior,
    last_k_in,
    last_v_in,
    decay_in,
    accepted_in,
    lengths_in,
    gain,
    frequency,
    ret_out,
    state_out,
    keys_out,
    values_out,
    tok_v,
    weights,
    wo_all,
    prior_v,
    last_k,
    last_v,
    decay,
    accepted,
    lengths,
    weighted_keys,
    state_b,
    tokens_all,
    place,
    order,
    out_a,
    in_a,
    mid,
    out_b,
    in_b,
    rows_f,
    chunk,
    gated_all,
    out_c,
    in_c,
    local,
    tok_arrived,
    tok_passed,
    tok_first,
    tok_ring,
    wo_arrived,
    wo_sent,
    wo_side,
    wo_side_sent,
    wo_on,
    wo_on_sent,
    g_sent,
    g_got,
    c_sent,
    c_got,
    pair_sems,
    a_sent,
    a_got,
    b_sent,
    b_got,
):
    x, z, y, tp = (lax.axis_index(axis) for axis in ("dp", "kv_0", "kv_1", "tp"))
    heads, seqs = nz, 2 * nz * ny
    kc = wq.shape[0]
    vc = wv.shape[0]
    span = 2 * kc + 2 * vc
    partner = {"tp": 1 - tp}

    loads = [
        pltpu.make_async_copy(tok.at[pl.ds(2 * tp, 2)], tok_v, local.at[0]),
        pltpu.make_async_copy(wq, weights.at[tp, pl.ds(0, kc)], local.at[1]),
        pltpu.make_async_copy(wk, weights.at[tp, pl.ds(kc, kc)], local.at[2]),
        pltpu.make_async_copy(wv, weights.at[tp, pl.ds(2 * kc, vc)], local.at[3]),
        pltpu.make_async_copy(wg, weights.at[tp, pl.ds(2 * kc + vc, vc)], local.at[4]),
        pltpu.make_async_copy(prior, prior_v, local.at[5]),
    ]
    small_loads = [
        pltpu.make_async_copy(source, target, local.at[17 + i])
        for i, (source, target) in enumerate(
            (
                (last_k_in, last_k),
                (last_v_in, last_v),
                (decay_in, decay),
                (accepted_in, accepted),
                (lengths_in, lengths),
            )
        )
    ]
    share = wo.shape[0] // nx
    mine = pl.ds(pl.multiple_of(share * x, share), share)
    half_k = wo.shape[1] // 2
    own_out = [
        pltpu.make_async_copy(
            wo.at[mine, pl.ds(p * half_k, half_k)], wo_all.at[p, (z, y)[p], mine], local.at[7 + p]
        )
        for p in range(2)
    ]
    for load in loads + own_out + small_loads:
        load.start()

    barrier = pltpu.get_barrier_semaphore()

    def greet(device):
        pl.semaphore_signal(barrier, inc=1, device_id=device, device_id_type=MESH)

    def greet_y(d, _):
        other = wrap(y + d, ny)
        greet({"kv_1": other})
        greet({"kv_1": other, "tp": 1 - tp})
        return 0

    def greet_z(d, _):
        greet({"kv_0": wrap(z + d, nz)})
        return 0

    lax.fori_loop(1, ny, greet_y, 0)
    lax.fori_loop(1, nz, greet_z, 0)
    def greet_tall(d, _):
        greet({"kv_0": wrap(z + d, nz), "tp": 1 - tp})
        return 0

    lax.fori_loop(1, nz, greet_tall, 0)
    greet(partner)
    for way in (1, nx - 1):
        greet({"dp": wrap(x + way, nx)})
    pl.semaphore_wait(barrier, 2 * (ny - 1) + 2 * (nz - 1) + 3)

    loads[0].wait()
    tokens = TorusGather(
        lambda p: tok_v.at[p], tokens_all, tok_arrived, tok_passed, tok_first, tok_ring, nz, ny
    )
    tokens.start_first()
    ring = WeightRing(
        wo_all, wo_arrived, wo_sent, wo_side, wo_side_sent, wo_on, wo_on_sent, nx, nz, ny
    )
    for load in own_out:
        load.wait()
    ring.step(0)
    for load in loads[1:5]:
        load.wait()
    swap = pltpu.make_async_remote_copy(
        src_ref=weights.at[tp],
        dst_ref=weights.at[tp],
        send_sem=pair_sems.at[0],
        recv_sem=pair_sems.at[1],
        device_id=partner,
        device_id_type=MESH,
    )
    swap.start()

    key_size, value_size = ny * kc, ny * vc

    loads[5].wait()
    for load in small_loads:
        load.wait()
    rows, count = 4 * heads, 8 * heads
    head_of = iota((rows, 1), 0) & (heads - 1)

    def by_head(shape):
        head = iota(shape, 0) & (heads - 1)
        table = jnp.zeros(shape, F32)
        for h in range(heads):
            table = jnp.where(head == h, -decay[h], table)
        return table

    taken_decay = by_head((rows, 128))
    before = iota((rows, 128), 0) >> (heads.bit_length() - 1)
    for s in range(2):
        power = jnp.maximum(accepted[s] - 1 - before, 0).astype(F32)
        key_weights = jnp.where(before < accepted[s], jnp.exp(taken_decay * power), 0.0)
        weighted = last_k[s].astype(F32) * key_weights
        high = weighted.astype(BF16).astype(F32)
        weighted_keys[s, 0] = high
        weighted_keys[s, 1] = weighted - high

    def one_head(h):
        mine = head_of == h
        for s in range(2):
            both = jnp.concatenate(
                [jnp.where(mine, weighted_keys[s, part], 0.0) for part in range(2)], axis=0
            )
            values = jnp.concatenate([last_v[s], last_v[s]], axis=0)
            update = lax.dot_general(
                both.astype(BF16), values, (((0,), (0,)), ((), ())), preferred_element_type=F32
            )
            at = s * heads + h
            power = jnp.full((1, value_size), -decay[h] * accepted[s].astype(F32), F32)
            fresh = jnp.exp(power) * prior_v[at] + update
            state_out[at] = fresh
            state_b[at] = fresh.astype(BF16)

    def some_heads(i):
        for e in range(heads // tokens.groups):
            one_head(i * (heads // tokens.groups) + e)

    tokens.round(0, some_heads)

    swap.wait()

    blocks = span // 16

    def scale_rows(i):
        at = pl.ds(pl.multiple_of(i * 16, 16), 16)
        for side in range(2):
            weights[side, at] = (weights[side, at].astype(F32) * gain[...]).astype(BF16)

    for k in range(1, tokens.hops):
        ring.step(k)
        tokens.round(k, scale_rows if k < tokens.hops - 1 else None)
        if k == 1:
            scale_rows = lambda i, first=scale_rows: pl.when(i + 4 < blocks)(lambda: first(i + 4))
    ring.step(tokens.hops)
    tokens.last_arrivals()

    depth = tok_v.shape[1]
    width = nz * ny * depth
    for p in range(2):
        total = jnp.zeros((2 * span, seqs), F32)
        squares = jnp.zeros((1, seqs), F32)
        for c in range(nz):
            block = tokens_all[p, c].reshape(ny * depth, seqs)
            cut = pl.ds(c * ny * depth, ny * depth)
            total += jnp.dot(
                weights[:, :, cut].reshape(2 * span, ny * depth), block, preferred_element_type=F32
            )
            floats = block.astype(F32)
            squares += jnp.sum(floats * floats, axis=0, keepdims=True)
        scaled = total * lax.rsqrt(squares / width + epsilon)
        for side in range(2):
            part = jnp.concatenate(
                [scaled[side * span : (side + 1) * span], jnp.zeros((128 - span, seqs), F32)], axis=0
            )
            turned = part.T.astype(BF16)
            for to in range(nz):
                out_a[to, side, p] = turned[2 * ny * to : 2 * ny * (to + 1)]

    def a_copy(d):
        to = wrap(z + d, nz)
        return pltpu.make_async_remote_copy(
            src_ref=out_a.at[to],
            dst_ref=in_a.at[z],
            send_sem=a_sent.at[d],
            recv_sem=a_got.at[z],
            device_id={"kv_0": to},
            device_id_type=MESH,
        )

    def a_wait(d):
        came = wrap(z + d, nz)
        pltpu.make_async_remote_copy(
            src_ref=in_a.at[came],
            dst_ref=in_a.at[came],
            send_sem=a_sent.at[0],
            recv_sem=a_got.at[came],
            device_id=partner,
            device_id_type=MESH,
        ).wait_recv()

    tokens.loop(1, nz, lambda i: a_copy(far_first(i, nz)).start())
    own_a = pltpu.make_async_copy(out_a.at[z], in_a.at[z], local.at[10])
    own_a.start()
    ring.share_on()

    shift = heads.bit_length() - 1

    def prop_of(i):
        return 2 * (i >> (shift + 2)) + ((i >> shift) & 1)

    def at_of(i):
        return ((i >> (shift + 1)) & 1) * heads + (i & (heads - 1))

    row = iota((count, 128), 0)
    first = jnp.where((row >> (shift + 1)) & 1 == 0, lengths[0] + accepted[0], lengths[1] + accepted[1])
    angles = (first + prop_of(row)).astype(F32) * frequency[...]
    cosine = jnp.cos(angles)
    lane_sign = jnp.where(iota((count, 128), 1) < key_size // 2, -1.0, 1.0)
    sine = jnp.sin(angles) * lane_sign
    decays = by_head((count, 128))
    query_decay = jnp.exp(decays * (prop_of(row) + 1).astype(F32))
    other = iota((count, count), 1)
    here = row[:, :count]
    offset = prop_of(here) - prop_of(other)
    grid = jnp.where(
        (at_of(here) == at_of(other)) & (offset >= 0),
        jnp.exp(decays[:, :count] * jnp.maximum(offset, 0).astype(F32)),
        0.0,
    )

    own_a.wait()
    tokens.loop(1, nz, a_wait)

    mid[...] = in_a[...].reshape(nz * 4 * 2 * ny, 128).astype(F32)
    stride = 4 * 2 * ny
    for to in range(ny):
        for side in range(2):
            for s in range(2):
                parts = [
                    mid[pl.ds(side * 4 * ny + p * 2 * ny + 2 * to + s, nz, stride=stride), :]
                    for p in range(2)
                ]
                out_b[to, side, s] = jnp.concatenate(parts, axis=0).astype(BF16)

    def b_copy(d, same):
        to = wrap(y + d, ny)
        side = tp if same else 1 - tp
        return pltpu.make_async_remote_copy(
            src_ref=out_b.at[to, side],
            dst_ref=in_b.at[y, tp],
            send_sem=b_sent.at[d, side],
            recv_sem=b_got.at[y, tp],
            device_id={"kv_1": to, "tp": side},
            device_id_type=MESH,
        )

    def b_wait(d, same):
        came = wrap(y + d, ny)
        side = tp if same else 1 - tp
        pltpu.make_async_remote_copy(
            src_ref=in_b.at[came, side],
            dst_ref=in_b.at[came, side],
            send_sem=b_sent.at[0, 0],
            recv_sem=b_got.at[came, side],
            device_id=partner,
            device_id_type=MESH,
        ).wait_recv()

    def b_start(i):
        d = far_first(i, ny)
        b_copy(d, True).start()
        b_copy(d, False).start()

    tokens.loop(1, ny, b_start)
    b_copy(0, False).start()
    own_b = pltpu.make_async_copy(out_b.at[y, tp], in_b.at[y, tp], local.at[11])
    own_b.start()

    lane = iota((128, 2 * key_size + 2 * value_size), 0)
    column = iota((128, 2 * key_size + 2 * value_size), 1)
    for j in range(ny):
        goal = jnp.where(
            lane < kc,
            kc * j + lane,
            jnp.where(
                lane < 2 * kc,
                key_size + kc * j + lane - kc,
                jnp.where(
                    lane < 2 * kc + vc,
                    2 * key_size + vc * j + lane - 2 * kc,
                    2 * key_size + value_size + vc * j + lane - 2 * kc - vc,
                ),
            ),
        )
        hit = (goal == column) & (lane < span)
        place[pl.ds(128 * j, 128)] = jnp.where(hit, 1.0, 0.0).astype(BF16)
    own_b.wait()
    b_wait(0, False)

    def b_take(d):
        b_wait(d, True)
        b_wait(d, False)

    tokens.loop(1, ny, b_take)

    packed = jnp.concatenate([in_b[j].reshape(count, 128) for j in range(ny)], axis=1)
    fields = jnp.dot(packed, place[...], preferred_element_type=F32)
    query = fields[:, :key_size]
    key = fields[:, key_size : 2 * key_size]
    value = fields[:, 2 * key_size : 2 * key_size + value_size]
    gate = fields[:, 2 * key_size + value_size :]
    half = key_size // 2

    def turned_by(x):
        swapped = jnp.concatenate([x[:, half:], x[:, :half]], axis=1)
        return x * cosine + swapped * sine

    query_rot = turned_by(query).astype(BF16)
    key_f = turned_by(key) * key_size ** (-0.5)
    key_rot = key_f.astype(BF16)
    value_b = value.astype(BF16)
    scores = lax.dot_general(
        query_rot, key_rot, (((1,), (1,)), ((), ())), preferred_element_type=F32
    )
    inner = jnp.dot((scores * grid).astype(BF16), value_b, preferred_element_type=F32)
    decayed = query_rot.astype(F32) * query_decay
    row_at = at_of(iota((count, 1), 0))
    spread = jnp.concatenate(
        [jnp.where(row_at == at, decayed, 0.0).astype(BF16) for at in range(2 * heads)], axis=1
    )
    states = state_b[...].reshape(2 * heads * key_size, value_size)
    heads_out = inner + jnp.dot(spread, states, preferred_element_type=F32)
    normed = heads_out * lax.rsqrt(jnp.mean(heads_out * heads_out, axis=-1, keepdims=True) + epsilon)
    product = gate / (1.0 + jnp.exp(-gate)) * normed
    for c in range(value_size // 128):
        rows_f[c] = product[:, 128 * c : 128 * (c + 1)]
    for i in range(8):
        prop, seq = 2 * (i // 4) + i % 2, (i // 2) % 2
        keys_out[seq, prop] = key_f[i * heads : (i + 1) * heads].astype(BF16)
        values_out[seq, prop] = value[i * heads : (i + 1) * heads].astype(BF16)
    cut = heads * value_size // 2
    for h in range(heads):
        part, at = divmod(h * value_size, cut)
        for c in range(value_size // 128):
            piece = rows_f[c, pl.ds(h, 8, stride=heads), :]
            chunk[part, :, at + 128 * c : at + 128 * (c + 1)] = piece.astype(BF16)

    first = ((y, ny, "kv_1"), (z, nz, "kv_0"))
    second = ((z, nz, "kv_0"), (y, ny, "kv_1"))

    def g_copy(p, d):
        f, n, axis = first[p]
        return pltpu.make_async_remote_copy(
            src_ref=chunk.at[p],
            dst_ref=gated_all.at[p, f],
            send_sem=g_sent.at[p, d],
            recv_sem=g_got.at[p, f],
            device_id={axis: wrap(f + d, n)},
            device_id_type=MESH,
        )

    def g_start(i):
        for p in range(2):
            g_copy(p, far_first(i, first[p][1])).start()

    tokens.loop(1, ny, g_start)
    for p in range(2):
        f = first[p][0]
        pltpu.make_async_copy(chunk.at[p], gated_all.at[p, f], g_got.at[p, f]).start()

    source = iota((4 * seqs, seqs), 0)
    target = iota((4 * seqs, seqs), 1)
    low_ring, high_ring = (source >> 3) & (ny - 1), source >> (2 + ny.bit_length())
    for part, group in enumerate((high_ring * ny + low_ring, low_ring * ny + high_ring)):
        row_seq = 2 * group + ((source >> 1) & 1)
        row_prop = 2 * ((source >> 2) & 1) + (source & 1)
        for p in range(4):
            hit = (row_seq == target) & (row_prop == p)
            order[part, :, pl.ds(seqs * p, seqs)] = jnp.where(hit, 1.0, 0.0).astype(BF16)
    ring.all_here()

    def c_copy(p, d, same):
        s, n, axis = second[p]
        to = wrap(s + d, n)
        side = tp if same else 1 - tp
        return pltpu.make_async_remote_copy(
            src_ref=out_c.at[p, to, side],
            dst_ref=in_c.at[p, tp, s],
            send_sem=c_sent.at[p, d, side],
            recv_sem=c_got.at[p, tp, s],
            device_id={axis: to, "tp": side},
            device_id_type=MESH,
        )

    def wait_for(block, arrived):
        pltpu.make_async_remote_copy(
            src_ref=block,
            dst_ref=block,
            send_sem=a_sent.at[0],
            recv_sem=arrived,
            device_id=partner,
            device_id_type=MESH,
        ).wait_recv()

    out_cols = wo.shape[0]
    for p in range(2):
        n = first[p][1]
        tokens.loop(0, n, lambda f, p=p: wait_for(gated_all.at[p, f], g_got.at[p, f]))
        product = lax.dot_general(
            wo_all[p].reshape(second[p][1] * out_cols, cut),
            gated_all[p].reshape(n * 8, cut),
            (((1,), (1,)), ((), ())),
            preferred_element_type=F32,
        )
        blank = jnp.zeros_like(product)
        lanes = jnp.where(
            (second[p][0] & 1) == 0,
            jnp.concatenate([product, blank], axis=1),
            jnp.concatenate([blank, product], axis=1),
        ).astype(BF16)
        part = out_cols // 2
        for to in range(second[p][1]):
            for side in range(2):
                at = to * out_cols + side * part
                out_c[p, to, side] = lanes[at : at + part]

        def c_start(i, p=p, n=n):
            d = far_first(i, n)
            c_copy(p, d, True).start()
            c_copy(p, d, False).start()

        tokens.loop(1, n, c_start)
        c_copy(p, 0, False).start()
        s = second[p][0]
        pltpu.make_async_copy(
            out_c.at[p, s, tp], in_c.at[p, tp, s], c_got.at[p, tp, s]
        ).start()
    result = jnp.zeros((out_cols // 2, 4 * seqs), F32)
    for p in range(2):
        n = second[p][1]
        for side in range(2):
            tokens.loop(
                0, n, lambda s, p=p, side=side: wait_for(in_c.at[p, side, s], c_got.at[p, side, s])
            )
        sums = jnp.concatenate(
            [
                jnp.concatenate(
                    [in_c[p, side, 2 * j] + in_c[p, side, 2 * j + 1] for j in range(n // 2)], axis=1
                )
                for side in range(2)
            ],
            axis=0,
        )
        moved = jnp.dot(sums, order[p], preferred_element_type=F32)
        result += moved[: out_cols // 2] + moved[out_cols // 2 :]
    result = result.astype(BF16)
    for p in range(4):
        ret_out[p] = result[:, p * seqs : (p + 1) * seqs]
    tokens.finish()
    ring.finish()

    def late_done(d):
        for p in range(2):
            g_copy(p, d).wait_send()
            for same in (True, False):
                c_copy(p, d, same).wait_send()

    tokens.loop(1, ny, late_done)
    for p in range(2):
        c_copy(p, 0, False).wait_send()
    tokens.loop(1, nz, lambda d: a_copy(d).wait_send())

    def b_done(d):
        b_copy(d, True).wait_send()
        b_copy(d, False).wait_send()

    tokens.loop(1, ny, b_done)
    b_copy(0, False).wait_send()


def in_hbm(value):
    return pltpu.with_memory_space_constraint(value, pltpu.HBM)


def put_kernel(*refs):
    count = (len(refs) - 1) // 2
    sems = refs[-1]
    copies = [
        pltpu.make_async_copy(refs[i], refs[count + i], sems.at[i]) for i in range(count)
    ]
    for copy in copies:
        copy.start()
    for copy in copies:
        copy.wait()


def put_out(*values):
    return pl.pallas_call(
        put_kernel,
        out_shape=tuple(jax.ShapeDtypeStruct(v.shape, v.dtype) for v in values),
        in_specs=[pl.BlockSpec(memory_space=pl.ANY)] * len(values),
        out_specs=(pl.BlockSpec(memory_space=pltpu.HBM),) * len(values),
        scratch_shapes=[pltpu.SemaphoreType.DMA((len(values),))],
        compiler_params=pltpu.CompilerParams(vmem_limit_bytes=8 * 1024 * 1024),
    )(*values)


def shards(
    nx,
    nz,
    ny,
    tokens,
    norm_gain,
    query_weight,
    key_weight,
    value_weight,
    gate_weight,
    out_weight,
    decay_rate,
    prior_state,
    last_keys,
    last_values,
    accepted,
    lengths,
):
    _, heads, key_size, value_size = prior_state.shape
    seqs, _, depth = tokens.shape
    width = norm_gain.shape[0]
    kc, vc = query_weight.shape[1], value_weight.shape[1]
    span = 2 * kc + 2 * vc
    count = 8 * heads
    half = key_size // 2
    frequency = jnp.power(10000.0, -jnp.arange(half, dtype=F32) / half)
    frequency = jnp.concatenate([frequency, frequency])[None, :]

    hbm = pl.BlockSpec(memory_space=pltpu.HBM)
    vmem = pl.BlockSpec(memory_space=pltpu.VMEM)
    dma = pltpu.SemaphoreType.DMA
    cut = heads * value_size // 2
    out_cols = out_weight.shape[1]
    retained, state, new_keys, new_values = pl.pallas_call(
        functools.partial(kernel, nx, nz, ny),
        out_shape=(
            jax.ShapeDtypeStruct((4, out_cols // 2, seqs), BF16),
            jax.ShapeDtypeStruct((2 * heads, key_size, value_size), F32),
            jax.ShapeDtypeStruct((2, 4, heads, key_size), BF16),
            jax.ShapeDtypeStruct((2, 4, heads, value_size), BF16),
        ),
        in_specs=[hbm] * 12 + [vmem] * 2,
        out_specs=(vmem,) * 4,
        scratch_shapes=[
            pltpu.VMEM((2, depth, seqs), BF16),
            pltpu.VMEM((2, span, width), BF16),
            pltpu.VMEM((2, nz, out_cols, cut), BF16),
            pltpu.VMEM((2 * heads, key_size, value_size), F32),
            pltpu.VMEM((2, 4 * heads, key_size), BF16),
            pltpu.VMEM((2, 4 * heads, value_size), BF16),
            pltpu.SMEM((heads,), F32),
            pltpu.SMEM((2,), jnp.int32),
            pltpu.SMEM((2,), jnp.int32),
            pltpu.VMEM((2, 2, 4 * heads, key_size), F32),
            pltpu.VMEM((2 * heads, key_size, value_size), BF16),
            pltpu.VMEM((2, nz, ny, depth, seqs), BF16),
            pltpu.VMEM((128 * ny, 2 * key_size + 2 * value_size), BF16),
            pltpu.VMEM((2, 4 * seqs, 4 * seqs), BF16),
            pltpu.VMEM((nz, 2, 2, 2 * ny, 128), BF16),
            pltpu.VMEM((nz, 2, 2, 2 * ny, 128), BF16),
            pltpu.VMEM((nz * 8 * ny, 128), F32),
            pltpu.VMEM((ny, 2, 2, 2 * nz, 128), BF16),
            pltpu.VMEM((ny, 2, 2, 2 * nz, 128), BF16),
            pltpu.VMEM((value_size // 128, count, 128), F32),
            pltpu.VMEM((2, 8, cut), BF16),
            pltpu.VMEM((2, nz, 8, cut), BF16),
            pltpu.VMEM((2, nz, 2, out_cols // 2, 128), BF16),
            pltpu.VMEM((2, 2, nz, out_cols // 2, 128), BF16),
            dma((22,)),
            dma((2, nz, ny)),
            dma((2, max(nz, ny), TorusGather.groups)),
            dma((2, max(nz, ny))),
            dma((2, 2, nz // 2, TorusGather.groups)),
            dma((2, nz)),
            dma((2, 2, nz // 2)),
            dma((2, 2, nz)),
            dma((2, 2, nz)),
            dma((2,)),
            dma((2,)),
            dma((2, nz)),
            dma((2, nz)),
            dma((2, nz, 2)),
            dma((2, 2, nz)),
            dma((4,)),
            dma((nz,)),
            dma((nz,)),
            dma((ny, 2)),
            dma((ny, 2)),
        ],
        compiler_params=pltpu.CompilerParams(
            collective_id=0, has_side_effects=True, vmem_limit_bytes=48 * 1024 * 1024
        ),
    )(
        *map(
            in_hbm,
            (
                tokens.transpose(1, 2, 0),
                query_weight.T,
                key_weight.T,
                value_weight.T,
                gate_weight.T,
                out_weight.T,
                prior_state.reshape(2 * heads, key_size, value_size),
                last_keys.reshape(2, 4 * heads, key_size),
                last_values.reshape(2, 4 * heads, value_size),
                decay_rate,
                accepted,
                lengths,
            ),
        ),
        norm_gain.astype(F32)[None, :],
        frequency,
    )
    retained, state, new_keys, new_values = put_out(retained, state, new_keys, new_values)
    return (
        retained.transpose(2, 0, 1),
        state.reshape(prior_state.shape),
        new_keys,
        new_values,
    )


def solution(mesh):
    nz = ny = 8
    finer = Mesh(
        mesh.devices.reshape(mesh.shape["dp"], nz, ny, mesh.shape["tp"]),
        ("dp", "kv_0", "kv_1", "tp"),
    )
    return jax.shard_map(
        functools.partial(shards, mesh.shape["dp"], nz, ny),
        mesh=finer,
        in_specs=(
            P("dp", None, KV),
            P(),
            P(None, TP_KV),
            P(None, TP_KV),
            P(None, TP_KV),
            P(None, TP_KV),
            P("tp", KV),
            P("tp"),
            P(DP_KV, "tp", None, None),
            P(DP_KV, None, "tp", None),
            P(DP_KV, None, "tp", None),
            P(DP_KV),
            P(DP_KV),
        ),
        out_specs=(
            P("dp", None, KV_TP),
            P(DP_KV, "tp", None, None),
            P(DP_KV, None, "tp", None),
            P(DP_KV, None, "tp", None),
        ),
        check_vma=False,
    )
```

```python
import functools

import jax
import jax.numpy as jnp
from jax import lax
from jax.experimental import pallas as pl
from jax.experimental.pallas import tpu as pltpu
from jax.sharding import Mesh
from jax.sharding import PartitionSpec as P

KV = ("kv_0", "kv_1")
TP_KV = ("tp", "kv_0", "kv_1")
DP_KV = ("dp", "kv_0", "kv_1")
KV_TP = ("kv_0", "kv_1", "tp")
MESH = pl.DeviceIdType.MESH
F32, BF16 = jnp.float32, jnp.bfloat16

epsilon = 1e-06


def wrap(i, n):
    return i & (n - 1)


def far_first(i, n):
    return wrap(n // 2 + (1 - 2 * (i & 1)) * (i >> 1), n)


def near_first(i, n):
    odd = i & 1
    return wrap(odd * ((i + 1) >> 1) + (1 - odd) * (n - (i >> 1)), n)


class TorusGather:
    groups = 4
    turn = (0, 1, 3, 2)

    def __init__(self, own, held, arrived, ring_arrived, first_sent, ring_sent, nz, ny):
        self.own, self.held, self.arrived, self.ring_arrived = own, held, arrived, ring_arrived
        self.first_sent, self.ring_sent = first_sent, ring_sent
        z, y = lax.axis_index("kv_0"), lax.axis_index("kv_1")
        self.partner = {"tp": 1 - lax.axis_index("tp")}
        self.first = ((y, ny, "kv_1"), (z, nz, "kv_0"))
        self.second = ((z, nz, "kv_0"), (y, ny, "kv_1"))
        self.hops = nz // 2
        self.size = ny // self.groups

    def at(self, ref, p, f, s):
        return ref.at[p, s, f] if p == 0 else ref.at[p, f, s]

    def copy(self, target, source, sent, arrived, device):
        return pltpu.make_async_remote_copy(
            src_ref=source,
            dst_ref=target,
            send_sem=sent,
            recv_sem=arrived,
            device_id=device,
            device_id_type=MESH,
        )

    def first_copy(self, p, d):
        (f, n, axis), (s, _, _) = self.first[p], self.second[p]
        return self.copy(
            self.at(self.held, p, f, s),
            self.own(p),
            self.first_sent.at[p, d],
            self.at(self.arrived, p, f, s),
            {axis: wrap(f + d, n)},
        )

    def start_first(self):
        def send(i):
            for p in range(2):
                self.first_copy(p, near_first(i, self.first[p][1])).start()

        self.loop(1, self.first[0][1], send)
        for p in range(2):
            (f, _, _), (s, _, _) = self.first[p], self.second[p]
            pltpu.make_async_copy(
                self.own(p), self.at(self.held, p, f, s), self.at(self.arrived, p, f, s)
            ).start()

    def group(self, p, i):
        f = self.first[p][0]
        return wrap(f // self.size + self.turn[i], self.groups)

    def group_at(self, p, q, s):
        return self.at(self.held, p, pl.ds(q * self.size, self.size), s)

    def ring_copy(self, p, k, i, way):
        s, n, axis = self.second[p]
        q, origin = self.group(p, i), wrap(s - way * k + n, n)
        block = self.group_at(p, q, origin)
        return self.copy(
            block,
            block,
            self.ring_sent.at[p, (1 + way) // 2, k, i],
            self.ring_arrived.at[p, origin, q],
            {axis: wrap(s + way + n, n)},
        )

    def wait_chunk(self, p, f, s):
        chunk = self.at(self.held, p, f, s)
        self.copy(
            chunk, chunk, self.first_sent.at[0, 0], self.at(self.arrived, p, f, s), self.partner
        ).wait_recv()

    def wait_group(self, p, i, s):
        q = self.group(p, i)
        block = self.group_at(p, q, s)
        self.copy(
            block, block, self.first_sent.at[0, 0], self.ring_arrived.at[p, s, q], self.partner
        ).wait_recv()

    def pass_on(self, k, i, ways):
        for p in range(2):
            s, n, _ = self.second[p]
            if k == 0:
                for e in range(self.size):
                    self.wait_chunk(p, self.group(p, i) * self.size + e, s)
                for way in ways:
                    self.ring_copy(p, k, i, way).start()
            else:
                for way in (1, -1):
                    self.wait_group(p, i, wrap(s - way * k + n, n))
                    if way in ways:
                        self.ring_copy(p, k, i, way).start()

    def loop(self, low, high, step):
        def body(i, _):
            step(i)
            return 0

        lax.fori_loop(low, high, body, 0)

    def ways(self, k, i):
        if k < self.hops - 1:
            return (1, -1)
        return (1,) if i < self.groups // 2 else (-1,)

    def wave(self, w, beside=None):
        for k in reversed(range(self.hops)):
            i = w - k
            if 0 <= i < self.groups:
                self.pass_on(k, i, self.ways(k, i))
                if beside is not None:
                    beside()

    def waves(self):
        return self.hops + self.groups - 1

    def last_arrivals(self):
        for i in range(self.groups):
            for p in range(2):
                s, n, _ = self.second[p]
                self.wait_group(p, i, wrap(s + self.hops, n))

    def finish(self):
        def first_done(d):
            for p in range(2):
                self.first_copy(p, d).wait_send()

        self.loop(1, self.first[0][1], first_done)
        for k in range(self.hops):
            for i in range(self.groups):
                for p in range(2):
                    for way in self.ways(k, i):
                        self.ring_copy(p, k, i, way).wait_send()


class WeightRing:
    def __init__(self, held, arrived, sent, side_arrived, side_sent, on_arrived, on_sent, nx, nz, ny):
        self.held, self.arrived, self.sent = held, arrived, sent
        self.side_arrived, self.side_sent = side_arrived, side_sent
        self.on_arrived, self.on_sent = on_arrived, on_sent
        self.x, self.nx = lax.axis_index("dp"), nx
        z, y = lax.axis_index("kv_0"), lax.axis_index("kv_1")
        self.partner = {"tp": 1 - lax.axis_index("tp")}
        self.second = ((z, nz, "kv_0"), (y, ny, "kv_1"))
        self.hops = nz // 2
        self.rows = held.shape[2] // nx

    def block(self, p, origin, x):
        return self.held.at[p, origin, pl.ds(pl.multiple_of(self.rows * x, self.rows), self.rows)]

    def copy(self, block, sent, arrived, device):
        return pltpu.make_async_remote_copy(
            src_ref=block,
            dst_ref=block,
            send_sem=sent,
            recv_sem=arrived,
            device_id=device,
            device_id_type=MESH,
        )

    def ring_copy(self, p, k, way):
        s, n, axis = self.second[p]
        origin = wrap(s - way * k + n, n)
        return self.copy(
            self.block(p, origin, self.x),
            self.sent.at[p, (1 + way) // 2, k],
            self.arrived.at[p, origin],
            {axis: wrap(s + way + n, n)},
        )

    def side_copy(self, p, origin, way):
        at = (1 + way) // 2
        return self.copy(
            self.block(p, origin, self.x),
            self.side_sent.at[p, at, origin],
            self.side_arrived.at[p, at, origin],
            {"dp": wrap(self.x + way + self.nx, self.nx)},
        )

    def on_way(self, p):
        return 1 - 2 * p

    def on_copy(self, p):
        way = self.on_way(p)
        x = wrap(self.x - way + self.nx, self.nx)
        block = self.held.at[p, :, pl.ds(pl.multiple_of(self.rows * x, self.rows), self.rows)]
        return self.copy(
            block,
            self.on_sent.at[p],
            self.on_arrived.at[p],
            {"dp": wrap(self.x + way + self.nx, self.nx)},
        )

    def forward_ways(self, p, k):
        if k < self.hops - 1:
            return (1, -1)
        return (self.on_way(p),) if k == self.hops - 1 else ()

    def step(self, k):
        for p in range(2):
            s, n, _ = self.second[p]
            for way in (1,) if k in (0, self.hops) else (1, -1):
                origin = wrap(s - way * k + n, n)
                if k > 0:
                    self.copy(
                        self.block(p, origin, self.x),
                        self.sent.at[0, 0, 0],
                        self.arrived.at[p, origin],
                        self.partner,
                    ).wait_recv()
                ways = self.forward_ways(p, k)
                for to in ways if k == 0 else (way,):
                    if to in ways:
                        self.ring_copy(p, k, to).start()
                for to in (1, -1):
                    self.side_copy(p, origin, to).start()

    def side_wait(self, p, way):
        x = wrap(self.x - way + self.nx, self.nx)

        def take(origin, _):
            self.copy(
                self.block(p, origin, x),
                self.sent.at[0, 0, 0],
                self.side_arrived.at[p, (1 + way) // 2, origin],
                self.partner,
            ).wait_recv()
            return 0

        lax.fori_loop(0, self.second[p][1], take, 0)

    def share_on(self):
        for p in range(2):
            self.side_wait(p, self.on_way(p))
            self.on_copy(p).start()

    def all_here(self):
        for p in range(2):
            self.side_wait(p, -self.on_way(p))
            self.on_copy(p).wait_recv()

    def finish(self):
        for p in range(2):
            for k in range(self.hops):
                for way in self.forward_ways(p, k):
                    self.ring_copy(p, k, way).wait_send()

            def done(origin, _, p=p):
                for way in (1, -1):
                    self.side_copy(p, origin, way).wait_send()
                return 0

            lax.fori_loop(0, self.second[p][1], done, 0)
            self.on_copy(p).wait_send()


def iota(shape, dim):
    return lax.broadcasted_iota(jnp.int32, shape, dim)


def kernel(
    nx,
    nz,
    ny,
    tok,
    wq,
    wk,
    wv,
    wg,
    wo,
    prior,
    last_k_in,
    last_v_in,
    decay_in,
    accepted_in,
    lengths_in,
    gain_in,
    frequency,
    ret_out,
    state_out,
    keys_out,
    values_out,
    tok_v,
    weights,
    wo_all,
    prior_v,
    last_k,
    last_v,
    decay,
    accepted,
    lengths,
    gain_v,
    gain,
    weighted_keys,
    state_b,
    tokens_all,
    place,
    order,
    out_a,
    in_a,
    mid,
    out_b,
    in_b,
    rows_f,
    chunk,
    gated_all,
    out_c,
    in_c,
    local,
    tok_arrived,
    tok_passed,
    tok_first,
    tok_ring,
    wo_arrived,
    wo_sent,
    wo_side,
    wo_side_sent,
    wo_on,
    wo_on_sent,
    g_sent,
    g_got,
    c_sent,
    c_got,
    pair_sems,
    a_sent,
    a_got,
    b_sent,
    b_got,
):
    x, z, y, tp = (lax.axis_index(axis) for axis in ("dp", "kv_0", "kv_1", "tp"))
    heads, seqs = nz, 2 * nz * ny
    kc = wq.shape[0]
    vc = wv.shape[0]
    span = 2 * kc + 2 * vc
    depth = tok_v.shape[1]
    width = nz * ny * depth
    partner = {"tp": 1 - tp}

    loads = [
        pltpu.make_async_copy(tok.at[pl.ds(2 * tp, 2)], tok_v, local.at[0]),
        pltpu.make_async_copy(wq, weights.at[tp, pl.ds(0, kc)], local.at[1]),
        pltpu.make_async_copy(wk, weights.at[tp, pl.ds(kc, kc)], local.at[2]),
        pltpu.make_async_copy(wv, weights.at[tp, pl.ds(2 * kc, vc)], local.at[3]),
        pltpu.make_async_copy(wg, weights.at[tp, pl.ds(2 * kc + vc, vc)], local.at[4]),
        pltpu.make_async_copy(prior, prior_v, local.at[5]),
    ]
    small_loads = [
        pltpu.make_async_copy(source, target, local.at[17 + i])
        for i, (source, target) in enumerate(
            (
                (last_k_in, last_k),
                (last_v_in, last_v),
                (decay_in, decay),
                (accepted_in, accepted),
                (lengths_in, lengths),
                (gain_in, gain_v),
            )
        )
    ]
    share = wo.shape[0] // nx
    mine = pl.ds(pl.multiple_of(share * x, share), share)
    half_k = wo.shape[1] // 2
    own_out = [
        pltpu.make_async_copy(
            wo.at[mine, pl.ds(p * half_k, half_k)], wo_all.at[p, (z, y)[p], mine], local.at[7 + p]
        )
        for p in range(2)
    ]
    for load in loads + own_out + small_loads:
        load.start()

    barrier = pltpu.get_barrier_semaphore()

    def greet(device):
        pl.semaphore_signal(barrier, inc=1, device_id=device, device_id_type=MESH)

    def greet_y(d, _):
        other = wrap(y + d, ny)
        greet({"kv_1": other})
        greet({"kv_1": other, "tp": 1 - tp})
        return 0

    def greet_z(d, _):
        greet({"kv_0": wrap(z + d, nz)})
        return 0

    lax.fori_loop(1, ny, greet_y, 0)
    lax.fori_loop(1, nz, greet_z, 0)
    def greet_tall(d, _):
        greet({"kv_0": wrap(z + d, nz), "tp": 1 - tp})
        return 0

    lax.fori_loop(1, nz, greet_tall, 0)
    greet(partner)
    for way in (1, nx - 1):
        greet({"dp": wrap(x + way, nx)})
    pl.semaphore_wait(barrier, 2 * (ny - 1) + 2 * (nz - 1) + 3)

    loads[0].wait()
    tokens = TorusGather(
        lambda p: tok_v.at[p], tokens_all, tok_arrived, tok_passed, tok_first, tok_ring, nz, ny
    )
    tokens.start_first()
    ring = WeightRing(
        wo_all, wo_arrived, wo_sent, wo_side, wo_side_sent, wo_on, wo_on_sent, nx, nz, ny
    )
    for load in own_out:
        load.wait()
    ring.step(0)
    for load in loads[1:5]:
        load.wait()
    swap = pltpu.make_async_remote_copy(
        src_ref=weights.at[tp],
        dst_ref=weights.at[tp],
        send_sem=pair_sems.at[0],
        recv_sem=pair_sems.at[1],
        device_id=partner,
        device_id_type=MESH,
    )
    swap.start()

    key_size, value_size = ny * kc, ny * vc

    loads[5].wait()
    for load in small_loads:
        load.wait()
    rows, count = 4 * heads, 8 * heads
    head_of = iota((rows, 1), 0) & (heads - 1)

    def by_head(shape):
        head = iota(shape, 0) & (heads - 1)
        table = jnp.zeros(shape, F32)
        for h in range(heads):
            table = jnp.where(head == h, -decay[h], table)
        return table

    taken_decay = by_head((rows, 128))
    before = iota((rows, 128), 0) >> (heads.bit_length() - 1)
    for s in range(2):
        power = jnp.maximum(accepted[s] - 1 - before, 0).astype(F32)
        key_weights = jnp.where(before < accepted[s], jnp.exp(taken_decay * power), 0.0)
        weighted = last_k[s].astype(F32) * key_weights
        high = weighted.astype(BF16).astype(F32)
        weighted_keys[s, 0] = high
        weighted_keys[s, 1] = weighted - high

    def one_head(h):
        mine = head_of == h
        for s in range(2):
            both = jnp.concatenate(
                [jnp.where(mine, weighted_keys[s, part], 0.0) for part in range(2)], axis=0
            )
            values = jnp.concatenate([last_v[s], last_v[s]], axis=0)
            update = lax.dot_general(
                both.astype(BF16), values, (((0,), (0,)), ((), ())), preferred_element_type=F32
            )
            at = s * heads + h
            power = jnp.full((1, value_size), -decay[h] * accepted[s].astype(F32), F32)
            fresh = jnp.exp(power) * prior_v[at] + update
            state_out[at] = fresh
            state_b[at] = fresh.astype(BF16)

    blocks = span // 16

    def scale_rows(i):
        at = pl.ds(i * 16, 16)
        for side in range(2):
            weights[side, at] = (weights[side, at].astype(F32) * gain[...]).astype(BF16)

    def first_scale():
        swap.wait()
        gain[...] = gain_v[...].astype(F32).reshape(1, width)
        scale_rows(0)

    one_head(0)
    one_head(1)
    work = [functools.partial(one_head, h) for h in range(2, heads)]
    work += [first_scale] + [functools.partial(scale_rows, i) for i in range(1, blocks)]
    work = iter(work)

    def beside():
        piece = next(work, None)
        if piece is not None:
            piece()

    for w in range(tokens.waves()):
        tokens.wave(w, beside)
        if 1 <= w <= tokens.hops:
            ring.step(w)
    tokens.last_arrivals()

    for p in range(2):
        total = jnp.zeros((2 * span, seqs), F32)
        squares = jnp.zeros((1, seqs), F32)
        for c in range(nz):
            block = tokens_all[p, c].reshape(ny * depth, seqs)
            cut = pl.ds(c * ny * depth, ny * depth)
            total += jnp.dot(
                weights[:, :, cut].reshape(2 * span, ny * depth), block, preferred_element_type=F32
            )
            floats = block.astype(F32)
            squares += jnp.sum(floats * floats, axis=0, keepdims=True)
        scaled = total * lax.rsqrt(squares / width + epsilon)
        for side in range(2):
            part = jnp.concatenate(
                [scaled[side * span : (side + 1) * span], jnp.zeros((128 - span, seqs), F32)], axis=0
            )
            turned = part.T.astype(BF16)
            for to in range(nz):
                out_a[to, side, p] = turned[2 * ny * to : 2 * ny * (to + 1)]

    def a_copy(d):
        to = wrap(z + d, nz)
        return pltpu.make_async_remote_copy(
            src_ref=out_a.at[to],
            dst_ref=in_a.at[z],
            send_sem=a_sent.at[d],
            recv_sem=a_got.at[z],
            device_id={"kv_0": to},
            device_id_type=MESH,
        )

    def a_wait(d):
        came = wrap(z + d, nz)
        pltpu.make_async_remote_copy(
            src_ref=in_a.at[came],
            dst_ref=in_a.at[came],
            send_sem=a_sent.at[0],
            recv_sem=a_got.at[came],
            device_id=partner,
            device_id_type=MESH,
        ).wait_recv()

    tokens.loop(1, nz, lambda i: a_copy(far_first(i, nz)).start())
    own_a = pltpu.make_async_copy(out_a.at[z], in_a.at[z], local.at[10])
    own_a.start()
    ring.share_on()

    shift = heads.bit_length() - 1

    def prop_of(i):
        return 2 * (i >> (shift + 2)) + ((i >> shift) & 1)

    def at_of(i):
        return ((i >> (shift + 1)) & 1) * heads + (i & (heads - 1))

    row = iota((count, 128), 0)
    first = jnp.where((row >> (shift + 1)) & 1 == 0, lengths[0] + accepted[0], lengths[1] + accepted[1])
    angles = (first + prop_of(row)).astype(F32) * frequency[...]
    cosine = jnp.cos(angles)
    lane_sign = jnp.where(iota((count, 128), 1) < key_size // 2, -1.0, 1.0)
    sine = jnp.sin(angles) * lane_sign
    decays = by_head((count, 128))
    query_decay = jnp.exp(decays * (prop_of(row) + 1).astype(F32))
    other = iota((count, count), 1)
    here = row[:, :count]
    offset = prop_of(here) - prop_of(other)
    grid = jnp.where(
        (at_of(here) == at_of(other)) & (offset >= 0),
        jnp.exp(decays[:, :count] * jnp.maximum(offset, 0).astype(F32)),
        0.0,
    )

    own_a.wait()
    tokens.loop(1, nz, a_wait)

    mid[...] = in_a[...].reshape(nz * 4 * 2 * ny, 128).astype(F32)
    stride = 4 * 2 * ny
    for to in range(ny):
        for side in range(2):
            for s in range(2):
                parts = [
                    mid[pl.ds(side * 4 * ny + p * 2 * ny + 2 * to + s, nz, stride=stride), :]
                    for p in range(2)
                ]
                out_b[to, side, s] = jnp.concatenate(parts, axis=0).astype(BF16)

    def b_copy(d, same):
        to = wrap(y + d, ny)
        side = tp if same else 1 - tp
        return pltpu.make_async_remote_copy(
            src_ref=out_b.at[to, side],
            dst_ref=in_b.at[y, tp],
            send_sem=b_sent.at[d, side],
            recv_sem=b_got.at[y, tp],
            device_id={"kv_1": to, "tp": side},
            device_id_type=MESH,
        )

    def b_wait(d, same):
        came = wrap(y + d, ny)
        side = tp if same else 1 - tp
        pltpu.make_async_remote_copy(
            src_ref=in_b.at[came, side],
            dst_ref=in_b.at[came, side],
            send_sem=b_sent.at[0, 0],
            recv_sem=b_got.at[came, side],
            device_id=partner,
            device_id_type=MESH,
        ).wait_recv()

    def b_start(i):
        d = far_first(i, ny)
        b_copy(d, True).start()
        b_copy(d, False).start()

    tokens.loop(1, ny, b_start)
    b_copy(0, False).start()
    own_b = pltpu.make_async_copy(out_b.at[y, tp], in_b.at[y, tp], local.at[11])
    own_b.start()

    lane = iota((128, 2 * key_size + 2 * value_size), 0)
    column = iota((128, 2 * key_size + 2 * value_size), 1)
    for j in range(ny):
        goal = jnp.where(
            lane < kc,
            kc * j + lane,
            jnp.where(
                lane < 2 * kc,
                key_size + kc * j + lane - kc,
                jnp.where(
                    lane < 2 * kc + vc,
                    2 * key_size + vc * j + lane - 2 * kc,
                    2 * key_size + value_size + vc * j + lane - 2 * kc - vc,
                ),
            ),
        )
        hit = (goal == column) & (lane < span)
        place[pl.ds(128 * j, 128)] = jnp.where(hit, 1.0, 0.0).astype(BF16)
    own_b.wait()
    b_wait(0, False)

    def b_take(d):
        b_wait(d, True)
        b_wait(d, False)

    tokens.loop(1, ny, b_take)

    packed = jnp.concatenate([in_b[j].reshape(count, 128) for j in range(ny)], axis=1)
    fields = jnp.dot(packed, place[...], preferred_element_type=F32)
    query = fields[:, :key_size]
    key = fields[:, key_size : 2 * key_size]
    value = fields[:, 2 * key_size : 2 * key_size + value_size]
    gate = fields[:, 2 * key_size + value_size :]
    half = key_size // 2

    def turned_by(x):
        swapped = jnp.concatenate([x[:, half:], x[:, :half]], axis=1)
        return x * cosine + swapped * sine

    query_rot = turned_by(query).astype(BF16)
    key_f = turned_by(key) * key_size ** (-0.5)
    key_rot = key_f.astype(BF16)
    value_b = value.astype(BF16)
    scores = lax.dot_general(
        query_rot, key_rot, (((1,), (1,)), ((), ())), preferred_element_type=F32
    )
    inner = jnp.dot((scores * grid).astype(BF16), value_b, preferred_element_type=F32)
    decayed = query_rot.astype(F32) * query_decay
    row_at = at_of(iota((count, 1), 0))
    spread = jnp.concatenate(
        [jnp.where(row_at == at, decayed, 0.0).astype(BF16) for at in range(2 * heads)], axis=1
    )
    states = state_b[...].reshape(2 * heads * key_size, value_size)
    heads_out = inner + jnp.dot(spread, states, preferred_element_type=F32)
    normed = heads_out * lax.rsqrt(jnp.mean(heads_out * heads_out, axis=-1, keepdims=True) + epsilon)
    product = gate / (1.0 + jnp.exp(-gate)) * normed
    for c in range(value_size // 128):
        rows_f[c] = product[:, 128 * c : 128 * (c + 1)]
    for i in range(8):
        prop, seq = 2 * (i // 4) + i % 2, (i // 2) % 2
        keys_out[seq, prop] = key_f[i * heads : (i + 1) * heads].astype(BF16)
        values_out[seq, prop] = value[i * heads : (i + 1) * heads].astype(BF16)
    cut = heads * value_size // 2
    for h in range(heads):
        part, at = divmod(h * value_size, cut)
        for c in range(value_size // 128):
            piece = rows_f[c, pl.ds(h, 8, stride=heads), :]
            chunk[part, :, at + 128 * c : at + 128 * (c + 1)] = piece.astype(BF16)

    first = ((y, ny, "kv_1"), (z, nz, "kv_0"))
    second = ((z, nz, "kv_0"), (y, ny, "kv_1"))

    def g_copy(p, d):
        f, n, axis = first[p]
        return pltpu.make_async_remote_copy(
            src_ref=chunk.at[p],
            dst_ref=gated_all.at[p, f],
            send_sem=g_sent.at[p, d],
            recv_sem=g_got.at[p, f],
            device_id={axis: wrap(f + d, n)},
            device_id_type=MESH,
        )

    def g_start(i):
        for p in range(2):
            g_copy(p, far_first(i, first[p][1])).start()

    tokens.loop(1, ny, g_start)
    for p in range(2):
        f = first[p][0]
        pltpu.make_async_copy(chunk.at[p], gated_all.at[p, f], g_got.at[p, f]).start()

    source = iota((4 * seqs, seqs), 0)
    target = iota((4 * seqs, seqs), 1)
    low_ring, high_ring = (source >> 3) & (ny - 1), source >> (2 + ny.bit_length())
    for part, group in enumerate((high_ring * ny + low_ring, low_ring * ny + high_ring)):
        row_seq = 2 * group + ((source >> 1) & 1)
        row_prop = 2 * ((source >> 2) & 1) + (source & 1)
        for p in range(4):
            hit = (row_seq == target) & (row_prop == p)
            order[part, :, pl.ds(seqs * p, seqs)] = jnp.where(hit, 1.0, 0.0).astype(BF16)
    ring.all_here()

    def c_copy(p, d, same):
        s, n, axis = second[p]
        to = wrap(s + d, n)
        side = tp if same else 1 - tp
        return pltpu.make_async_remote_copy(
            src_ref=out_c.at[p, to, side],
            dst_ref=in_c.at[p, tp, s],
            send_sem=c_sent.at[p, d, side],
            recv_sem=c_got.at[p, tp, s],
            device_id={axis: to, "tp": side},
            device_id_type=MESH,
        )

    def wait_for(block, arrived):
        pltpu.make_async_remote_copy(
            src_ref=block,
            dst_ref=block,
            send_sem=a_sent.at[0],
            recv_sem=arrived,
            device_id=partner,
            device_id_type=MESH,
        ).wait_recv()

    out_cols = wo.shape[0]
    for p in range(2):
        n = first[p][1]
        tokens.loop(0, n, lambda f, p=p: wait_for(gated_all.at[p, f], g_got.at[p, f]))
        product = lax.dot_general(
            wo_all[p].reshape(second[p][1] * out_cols, cut),
            gated_all[p].reshape(n * 8, cut),
            (((1,), (1,)), ((), ())),
            preferred_element_type=F32,
        )
        part = out_cols // 2
        for to in range(second[p][1]):
            for side in range(2):
                at = to * out_cols + side * part
                halves = [product[at + e : at + e + part // 2] for e in (0, part // 2)]
                out_c[p, to, side] = jnp.concatenate(halves, axis=1).astype(BF16)

        def c_start(i, p=p, n=n):
            d = far_first(i, n)
            c_copy(p, d, True).start()
            c_copy(p, d, False).start()

        tokens.loop(1, n, c_start)
        c_copy(p, 0, False).start()
        s = second[p][0]
        pltpu.make_async_copy(
            out_c.at[p, s, tp], in_c.at[p, tp, s], c_got.at[p, tp, s]
        ).start()
    result = jnp.zeros((out_cols // 2, 4 * seqs), F32)
    for p in range(2):
        n = second[p][1]
        for side in range(2):
            tokens.loop(
                0, n, lambda s, p=p, side=side: wait_for(in_c.at[p, side, s], c_got.at[p, side, s])
            )
        sums = []
        for side in range(2):
            pairs = [[in_c[p, side, 2 * j + e].astype(F32) for e in range(2)] for j in range(n // 2)]
            for cut_at in (slice(0, 64), slice(64, 128)):
                sums.append(
                    jnp.concatenate([each[:, cut_at] for pair in pairs for each in pair], axis=1)
                )
        sums = jnp.concatenate(sums, axis=0).astype(BF16)
        moved = jnp.dot(sums, order[p], preferred_element_type=F32)
        result += moved[: out_cols // 2] + moved[out_cols // 2 :]
    result = result.astype(BF16)
    for p in range(4):
        ret_out[p] = result[:, p * seqs : (p + 1) * seqs]
    tokens.finish()
    ring.finish()

    def late_done(d):
        for p in range(2):
            g_copy(p, d).wait_send()
            for same in (True, False):
                c_copy(p, d, same).wait_send()

    tokens.loop(1, ny, late_done)
    for p in range(2):
        c_copy(p, 0, False).wait_send()
    tokens.loop(1, nz, lambda d: a_copy(d).wait_send())

    def b_done(d):
        b_copy(d, True).wait_send()
        b_copy(d, False).wait_send()

    tokens.loop(1, ny, b_done)
    b_copy(0, False).wait_send()


def in_hbm(value):
    return pltpu.with_memory_space_constraint(value, pltpu.HBM)


def put_kernel(*refs):
    count = (len(refs) - 1) // 2
    sems = refs[-1]
    copies = [
        pltpu.make_async_copy(refs[i], refs[count + i], sems.at[i]) for i in range(count)
    ]
    for copy in copies:
        copy.start()
    for copy in copies:
        copy.wait()


def put_out(*values):
    return pl.pallas_call(
        put_kernel,
        out_shape=tuple(jax.ShapeDtypeStruct(v.shape, v.dtype) for v in values),
        in_specs=[pl.BlockSpec(memory_space=pl.ANY)] * len(values),
        out_specs=(pl.BlockSpec(memory_space=pltpu.HBM),) * len(values),
        scratch_shapes=[pltpu.SemaphoreType.DMA((len(values),))],
        compiler_params=pltpu.CompilerParams(vmem_limit_bytes=8 * 1024 * 1024),
    )(*values)


def shards(
    nx,
    nz,
    ny,
    tokens,
    norm_gain,
    query_weight,
    key_weight,
    value_weight,
    gate_weight,
    out_weight,
    decay_rate,
    prior_state,
    last_keys,
    last_values,
    accepted,
    lengths,
):
    _, heads, key_size, value_size = prior_state.shape
    seqs, _, depth = tokens.shape
    width = norm_gain.shape[0]
    kc, vc = query_weight.shape[1], value_weight.shape[1]
    span = 2 * kc + 2 * vc
    count = 8 * heads
    half = key_size // 2
    frequency = jnp.power(10000.0, -jnp.arange(half, dtype=F32) / half)
    frequency = jnp.concatenate([frequency, frequency])[None, :]

    hbm = pl.BlockSpec(memory_space=pltpu.HBM)
    vmem = pl.BlockSpec(memory_space=pltpu.VMEM)
    dma = pltpu.SemaphoreType.DMA
    cut = heads * value_size // 2
    out_cols = out_weight.shape[1]
    retained, state, new_keys, new_values = pl.pallas_call(
        functools.partial(kernel, nx, nz, ny),
        out_shape=(
            jax.ShapeDtypeStruct((4, out_cols // 2, seqs), BF16),
            jax.ShapeDtypeStruct((2 * heads, key_size, value_size), F32),
            jax.ShapeDtypeStruct((2, 4, heads, key_size), BF16),
            jax.ShapeDtypeStruct((2, 4, heads, value_size), BF16),
        ),
        in_specs=[hbm] * 13 + [vmem],
        out_specs=(vmem,) * 4,
        scratch_shapes=[
            pltpu.VMEM((2, depth, seqs), BF16),
            pltpu.VMEM((2, span, width), BF16),
            pltpu.VMEM((2, nz, out_cols, cut), BF16),
            pltpu.VMEM((2 * heads, key_size, value_size), F32),
            pltpu.VMEM((2, 4 * heads, key_size), BF16),
            pltpu.VMEM((2, 4 * heads, value_size), BF16),
            pltpu.SMEM((heads,), F32),
            pltpu.SMEM((2,), jnp.int32),
            pltpu.SMEM((2,), jnp.int32),
            pltpu.VMEM((width,), BF16),
            pltpu.VMEM((1, width), F32),
            pltpu.VMEM((2, 2, 4 * heads, key_size), F32),
            pltpu.VMEM((2 * heads, key_size, value_size), BF16),
            pltpu.VMEM((2, nz, ny, depth, seqs), BF16),
            pltpu.VMEM((128 * ny, 2 * key_size + 2 * value_size), BF16),
            pltpu.VMEM((2, 4 * seqs, 4 * seqs), BF16),
            pltpu.VMEM((nz, 2, 2, 2 * ny, 128), BF16),
            pltpu.VMEM((nz, 2, 2, 2 * ny, 128), BF16),
            pltpu.VMEM((nz * 8 * ny, 128), F32),
            pltpu.VMEM((ny, 2, 2, 2 * nz, 128), BF16),
            pltpu.VMEM((ny, 2, 2, 2 * nz, 128), BF16),
            pltpu.VMEM((value_size // 128, count, 128), F32),
            pltpu.VMEM((2, 8, cut), BF16),
            pltpu.VMEM((2, nz, 8, cut), BF16),
            pltpu.VMEM((2, nz, 2, out_cols // 4, 128), BF16),
            pltpu.VMEM((2, 2, nz, out_cols // 4, 128), BF16),
            dma((23,)),
            dma((2, nz, ny)),
            dma((2, max(nz, ny), TorusGather.groups)),
            dma((2, max(nz, ny))),
            dma((2, 2, nz // 2, TorusGather.groups)),
            dma((2, nz)),
            dma((2, 2, nz // 2)),
            dma((2, 2, nz)),
            dma((2, 2, nz)),
            dma((2,)),
            dma((2,)),
            dma((2, nz)),
            dma((2, nz)),
            dma((2, nz, 2)),
            dma((2, 2, nz)),
            dma((4,)),
            dma((nz,)),
            dma((nz,)),
            dma((ny, 2)),
            dma((ny, 2)),
        ],
        compiler_params=pltpu.CompilerParams(
            collective_id=0, has_side_effects=True, vmem_limit_bytes=48 * 1024 * 1024
        ),
    )(
        *map(
            in_hbm,
            (
                tokens.transpose(1, 2, 0),
                query_weight.T,
                key_weight.T,
                value_weight.T,
                gate_weight.T,
                out_weight.T,
                prior_state.reshape(2 * heads, key_size, value_size),
                last_keys.reshape(2, 4 * heads, key_size),
                last_values.reshape(2, 4 * heads, value_size),
                decay_rate,
                accepted,
                lengths,
                norm_gain,
            ),
        ),
        frequency,
    )
    retained, state, new_keys, new_values = put_out(retained, state, new_keys, new_values)
    return (
        retained.transpose(2, 0, 1),
        state.reshape(prior_state.shape),
        new_keys,
        new_values,
    )


def solution(mesh):
    nz = ny = 8
    finer = Mesh(
        mesh.devices.reshape(mesh.shape["dp"], nz, ny, mesh.shape["tp"]),
        ("dp", "kv_0", "kv_1", "tp"),
    )
    return jax.shard_map(
        functools.partial(shards, mesh.shape["dp"], nz, ny),
        mesh=finer,
        in_specs=(
            P("dp", None, KV),
            P(),
            P(None, TP_KV),
            P(None, TP_KV),
            P(None, TP_KV),
            P(None, TP_KV),
            P("tp", KV),
            P("tp"),
            P(DP_KV, "tp", None, None),
            P(DP_KV, None, "tp", None),
            P(DP_KV, None, "tp", None),
            P(DP_KV),
            P(DP_KV),
        ),
        out_specs=(
            P("dp", None, KV_TP),
            P(DP_KV, "tp", None, None),
            P(DP_KV, None, "tp", None),
            P(DP_KV, None, "tp", None),
        ),
        check_vma=False,
    )
```

```python
import functools

import jax
import jax.numpy as jnp
from jax import lax
from jax.experimental import pallas as pl
from jax.experimental.pallas import tpu as pltpu
from jax.sharding import Mesh
from jax.sharding import PartitionSpec as P

KV = ("kv_0", "kv_1")
TP_KV = ("tp", "kv_0", "kv_1")
DP_KV = ("dp", "kv_0", "kv_1")
KV_TP = ("kv_0", "kv_1", "tp")
MESH = pl.DeviceIdType.MESH
F32, BF16 = jnp.float32, jnp.bfloat16

epsilon = 1e-06


def wrap(i, n):
    return i & (n - 1)


def far_first(i, n):
    return wrap(n // 2 + (1 - 2 * (i & 1)) * (i >> 1), n)


def near_first(i, n):
    odd = i & 1
    return wrap(odd * ((i + 1) >> 1) + (1 - odd) * (n - (i >> 1)), n)


class TorusGather:
    groups = 4
    turn = (0, 1, 3, 2)

    def __init__(self, own, held, arrived, ring_arrived, first_sent, ring_sent, nz, ny):
        self.own, self.held, self.arrived, self.ring_arrived = own, held, arrived, ring_arrived
        self.first_sent, self.ring_sent = first_sent, ring_sent
        z, y = lax.axis_index("kv_0"), lax.axis_index("kv_1")
        self.partner = {"tp": 1 - lax.axis_index("tp")}
        self.first = ((y, ny, "kv_1"), (z, nz, "kv_0"))
        self.second = ((z, nz, "kv_0"), (y, ny, "kv_1"))
        self.hops = nz // 2
        self.size = ny // self.groups

    def at(self, ref, p, f, s):
        return ref.at[p, s, f] if p == 0 else ref.at[p, f, s]

    def copy(self, target, source, sent, arrived, device):
        return pltpu.make_async_remote_copy(
            src_ref=source,
            dst_ref=target,
            send_sem=sent,
            recv_sem=arrived,
            device_id=device,
            device_id_type=MESH,
        )

    def first_copy(self, p, d):
        (f, n, axis), (s, _, _) = self.first[p], self.second[p]
        return self.copy(
            self.at(self.held, p, f, s),
            self.own(p),
            self.first_sent.at[p, d],
            self.at(self.arrived, p, f, s),
            {axis: wrap(f + d, n)},
        )

    def start_first(self):
        def send(i):
            for p in range(2):
                self.first_copy(p, near_first(i, self.first[p][1])).start()

        self.loop(1, self.first[0][1], send)
        for p in range(2):
            (f, _, _), (s, _, _) = self.first[p], self.second[p]
            pltpu.make_async_copy(
                self.own(p), self.at(self.held, p, f, s), self.at(self.arrived, p, f, s)
            ).start()

    def group(self, p, i):
        f = self.first[p][0]
        return wrap(f // self.size + self.turn[i], self.groups)

    def group_at(self, p, q, s):
        return self.at(self.held, p, pl.ds(q * self.size, self.size), s)

    def ring_copy(self, p, k, i, way):
        s, n, axis = self.second[p]
        q, origin = self.group(p, i), wrap(s - way * k + n, n)
        block = self.group_at(p, q, origin)
        return self.copy(
            block,
            block,
            self.ring_sent.at[p, (1 + way) // 2, k, i],
            self.ring_arrived.at[p, origin, q],
            {axis: wrap(s + way + n, n)},
        )

    def wait_chunk(self, p, f, s):
        chunk = self.at(self.held, p, f, s)
        self.copy(
            chunk, chunk, self.first_sent.at[0, 0], self.at(self.arrived, p, f, s), self.partner
        ).wait_recv()

    def wait_group(self, p, i, s):
        q = self.group(p, i)
        block = self.group_at(p, q, s)
        self.copy(
            block, block, self.first_sent.at[0, 0], self.ring_arrived.at[p, s, q], self.partner
        ).wait_recv()

    def pass_on(self, k, i, ways):
        for p in range(2):
            s, n, _ = self.second[p]
            if k == 0:
                for e in range(self.size):
                    self.wait_chunk(p, self.group(p, i) * self.size + e, s)
                for way in ways:
                    self.ring_copy(p, k, i, way).start()
            else:
                for way in (1, -1):
                    self.wait_group(p, i, wrap(s - way * k + n, n))
                    if way in ways:
                        self.ring_copy(p, k, i, way).start()

    def loop(self, low, high, step):
        def body(i, _):
            step(i)
            return 0

        lax.fori_loop(low, high, body, 0)

    def ways(self, k, i):
        if k < self.hops - 1:
            return (1, -1)
        return (1,) if i < self.groups // 2 else (-1,)

    def round(self, k, beside=None):
        for i in range(self.groups):
            self.pass_on(k, i, self.ways(k, i))
            if beside is not None:
                beside()

    def last_arrivals(self):
        for i in range(self.groups):
            for p in range(2):
                s, n, _ = self.second[p]
                self.wait_group(p, i, wrap(s + self.hops, n))

    def finish(self):
        def first_done(d):
            for p in range(2):
                self.first_copy(p, d).wait_send()

        self.loop(1, self.first[0][1], first_done)
        for k in range(self.hops):
            for i in range(self.groups):
                for p in range(2):
                    for way in self.ways(k, i):
                        self.ring_copy(p, k, i, way).wait_send()


class WeightRing:
    def __init__(self, held, arrived, sent, side_arrived, side_sent, on_arrived, on_sent, nx, nz, ny):
        self.held, self.arrived, self.sent = held, arrived, sent
        self.side_arrived, self.side_sent = side_arrived, side_sent
        self.on_arrived, self.on_sent = on_arrived, on_sent
        self.x, self.nx = lax.axis_index("dp"), nx
        z, y = lax.axis_index("kv_0"), lax.axis_index("kv_1")
        self.partner = {"tp": 1 - lax.axis_index("tp")}
        self.second = ((z, nz, "kv_0"), (y, ny, "kv_1"))
        self.hops = nz // 2
        self.rows = held.shape[2] // nx

    def block(self, p, origin, x):
        return self.held.at[p, origin, pl.ds(pl.multiple_of(self.rows * x, self.rows), self.rows)]

    def copy(self, block, sent, arrived, device):
        return pltpu.make_async_remote_copy(
            src_ref=block,
            dst_ref=block,
            send_sem=sent,
            recv_sem=arrived,
            device_id=device,
            device_id_type=MESH,
        )

    def ring_copy(self, p, k, way):
        s, n, axis = self.second[p]
        origin = wrap(s - way * k + n, n)
        return self.copy(
            self.block(p, origin, self.x),
            self.sent.at[p, (1 + way) // 2, k],
            self.arrived.at[p, origin],
            {axis: wrap(s + way + n, n)},
        )

    def side_copy(self, p, origin, way):
        at = (1 + way) // 2
        return self.copy(
            self.block(p, origin, self.x),
            self.side_sent.at[p, at, origin],
            self.side_arrived.at[p, at, origin],
            {"dp": wrap(self.x + way + self.nx, self.nx)},
        )

    def on_way(self, p):
        return 1 - 2 * p

    def on_copy(self, p):
        way = self.on_way(p)
        x = wrap(self.x - way + self.nx, self.nx)
        block = self.held.at[p, :, pl.ds(pl.multiple_of(self.rows * x, self.rows), self.rows)]
        return self.copy(
            block,
            self.on_sent.at[p],
            self.on_arrived.at[p],
            {"dp": wrap(self.x + way + self.nx, self.nx)},
        )

    def forward_ways(self, p, k):
        if k < self.hops - 1:
            return (1, -1)
        return (self.on_way(p),) if k == self.hops - 1 else ()

    def step(self, k):
        for p in range(2):
            s, n, _ = self.second[p]
            for way in (1,) if k in (0, self.hops) else (1, -1):
                origin = wrap(s - way * k + n, n)
                if k > 0:
                    self.copy(
                        self.block(p, origin, self.x),
                        self.sent.at[0, 0, 0],
                        self.arrived.at[p, origin],
                        self.partner,
                    ).wait_recv()
                ways = self.forward_ways(p, k)
                for to in ways if k == 0 else (way,):
                    if to in ways:
                        self.ring_copy(p, k, to).start()
                for to in (1, -1):
                    self.side_copy(p, origin, to).start()

    def side_wait(self, p, way):
        x = wrap(self.x - way + self.nx, self.nx)

        def take(origin, _):
            self.copy(
                self.block(p, origin, x),
                self.sent.at[0, 0, 0],
                self.side_arrived.at[p, (1 + way) // 2, origin],
                self.partner,
            ).wait_recv()
            return 0

        lax.fori_loop(0, self.second[p][1], take, 0)

    def share_on(self):
        for p in range(2):
            self.side_wait(p, self.on_way(p))
            self.on_copy(p).start()

    def all_here(self):
        for p in range(2):
            self.side_wait(p, -self.on_way(p))
            self.on_copy(p).wait_recv()

    def finish(self):
        for p in range(2):
            for k in range(self.hops):
                for way in self.forward_ways(p, k):
                    self.ring_copy(p, k, way).wait_send()

            def done(origin, _, p=p):
                for way in (1, -1):
                    self.side_copy(p, origin, way).wait_send()
                return 0

            lax.fori_loop(0, self.second[p][1], done, 0)
            self.on_copy(p).wait_send()


def iota(shape, dim):
    return lax.broadcasted_iota(jnp.int32, shape, dim)


def kernel(
    nx,
    nz,
    ny,
    tok,
    wq,
    wk,
    wv,
    wg,
    wo,
    prior,
    last_k_in,
    last_v_in,
    decay_in,
    accepted_in,
    lengths_in,
    gain_in,
    frequency,
    ret_out,
    state_out,
    keys_out,
    values_out,
    tok_v,
    weights,
    wo_all,
    prior_v,
    last_k,
    last_v,
    decay,
    accepted,
    lengths,
    gain_v,
    gain,
    weighted_keys,
    state_b,
    tokens_all,
    place,
    order,
    out_a,
    in_a,
    mid,
    out_b,
    in_b,
    rows_f,
    chunk,
    gated_all,
    out_c,
    in_c,
    local,
    tok_arrived,
    tok_passed,
    tok_first,
    tok_ring,
    wo_arrived,
    wo_sent,
    wo_side,
    wo_side_sent,
    wo_on,
    wo_on_sent,
    g_sent,
    g_got,
    c_sent,
    c_got,
    pair_sems,
    a_sent,
    a_got,
    b_sent,
    b_got,
):
    x, z, y, tp = (lax.axis_index(axis) for axis in ("dp", "kv_0", "kv_1", "tp"))
    heads, seqs = nz, 2 * nz * ny
    kc = wq.shape[0]
    vc = wv.shape[0]
    span = 2 * kc + 2 * vc
    depth = tok_v.shape[1]
    width = nz * ny * depth
    partner = {"tp": 1 - tp}

    loads = [
        pltpu.make_async_copy(tok.at[pl.ds(2 * tp, 2)], tok_v, local.at[0]),
        pltpu.make_async_copy(wq, weights.at[tp, pl.ds(0, kc)], local.at[1]),
        pltpu.make_async_copy(wk, weights.at[tp, pl.ds(kc, kc)], local.at[2]),
        pltpu.make_async_copy(wv, weights.at[tp, pl.ds(2 * kc, vc)], local.at[3]),
        pltpu.make_async_copy(wg, weights.at[tp, pl.ds(2 * kc + vc, vc)], local.at[4]),
        pltpu.make_async_copy(prior, prior_v, local.at[5]),
    ]
    small_loads = [
        pltpu.make_async_copy(source, target, local.at[17 + i])
        for i, (source, target) in enumerate(
            (
                (last_k_in, last_k),
                (last_v_in, last_v),
                (decay_in, decay),
                (accepted_in, accepted),
                (lengths_in, lengths),
                (gain_in, gain_v),
            )
        )
    ]
    share = wo.shape[0] // nx
    mine = pl.ds(pl.multiple_of(share * x, share), share)
    half_k = wo.shape[1] // 2
    own_out = [
        pltpu.make_async_copy(
            wo.at[mine, pl.ds(p * half_k, half_k)], wo_all.at[p, (z, y)[p], mine], local.at[7 + p]
        )
        for p in range(2)
    ]
    for load in loads + own_out + small_loads:
        load.start()

    barrier = pltpu.get_barrier_semaphore()

    def greet(device):
        pl.semaphore_signal(barrier, inc=1, device_id=device, device_id_type=MESH)

    def greet_y(d, _):
        other = wrap(y + d, ny)
        greet({"kv_1": other})
        greet({"kv_1": other, "tp": 1 - tp})
        return 0

    def greet_z(d, _):
        greet({"kv_0": wrap(z + d, nz)})
        return 0

    lax.fori_loop(1, ny, greet_y, 0)
    lax.fori_loop(1, nz, greet_z, 0)
    def greet_tall(d, _):
        greet({"kv_0": wrap(z + d, nz), "tp": 1 - tp})
        return 0

    lax.fori_loop(1, nz, greet_tall, 0)
    greet(partner)
    for way in (1, nx - 1):
        greet({"dp": wrap(x + way, nx)})
    pl.semaphore_wait(barrier, 2 * (ny - 1) + 2 * (nz - 1) + 3)

    loads[0].wait()
    tokens = TorusGather(
        lambda p: tok_v.at[p], tokens_all, tok_arrived, tok_passed, tok_first, tok_ring, nz, ny
    )
    tokens.start_first()
    ring = WeightRing(
        wo_all, wo_arrived, wo_sent, wo_side, wo_side_sent, wo_on, wo_on_sent, nx, nz, ny
    )
    for load in own_out:
        load.wait()
    ring.step(0)
    for load in loads[1:5]:
        load.wait()
    swap = pltpu.make_async_remote_copy(
        src_ref=weights.at[tp],
        dst_ref=weights.at[tp],
        send_sem=pair_sems.at[0],
        recv_sem=pair_sems.at[1],
        device_id=partner,
        device_id_type=MESH,
    )
    swap.start()

    key_size, value_size = ny * kc, ny * vc

    loads[5].wait()
    for load in small_loads:
        load.wait()
    rows, count = 4 * heads, 8 * heads
    head_of = iota((rows, 1), 0) & (heads - 1)

    def by_head(shape):
        head = iota(shape, 0) & (heads - 1)
        table = jnp.zeros(shape, F32)
        for h in range(heads):
            table = jnp.where(head == h, -decay[h], table)
        return table

    taken_decay = by_head((rows, 128))
    before = iota((rows, 128), 0) >> (heads.bit_length() - 1)
    for s in range(2):
        power = jnp.maximum(accepted[s] - 1 - before, 0).astype(F32)
        key_weights = jnp.where(before < accepted[s], jnp.exp(taken_decay * power), 0.0)
        weighted = last_k[s].astype(F32) * key_weights
        high = weighted.astype(BF16).astype(F32)
        weighted_keys[s, 0] = high
        weighted_keys[s, 1] = weighted - high

    def one_head(h):
        mine = head_of == h
        for s in range(2):
            both = jnp.concatenate(
                [jnp.where(mine, weighted_keys[s, part], 0.0) for part in range(2)], axis=0
            )
            values = jnp.concatenate([last_v[s], last_v[s]], axis=0)
            update = lax.dot_general(
                both.astype(BF16), values, (((0,), (0,)), ((), ())), preferred_element_type=F32
            )
            at = s * heads + h
            power = jnp.full((1, value_size), -decay[h] * accepted[s].astype(F32), F32)
            fresh = jnp.exp(power) * prior_v[at] + update
            state_out[at] = fresh
            state_b[at] = fresh.astype(BF16)

    blocks = span // 16

    def scale_rows(i):
        at = pl.ds(i * 16, 16)
        for side in range(2):
            weights[side, at] = (weights[side, at].astype(F32) * gain[...]).astype(BF16)

    def first_scale():
        swap.wait()
        gain[...] = gain_v[...].astype(F32).reshape(1, width)
        scale_rows(0)

    one_head(0)
    one_head(1)
    work = [functools.partial(one_head, h) for h in range(2, heads)]
    work += [first_scale] + [functools.partial(scale_rows, i) for i in range(1, blocks)]
    work = iter(work)

    def beside():
        piece = next(work, None)
        if piece is not None:
            piece()

    for k in range(tokens.hops):
        if k > 0:
            ring.step(k)
        tokens.round(k, beside)
    ring.step(tokens.hops)
    tokens.last_arrivals()

    for p in range(2):
        total = jnp.zeros((2 * span, seqs), F32)
        squares = jnp.zeros((1, seqs), F32)
        for c in range(nz):
            block = tokens_all[p, c].reshape(ny * depth, seqs)
            cut = pl.ds(c * ny * depth, ny * depth)
            total += jnp.dot(
                weights[:, :, cut].reshape(2 * span, ny * depth), block, preferred_element_type=F32
            )
            floats = block.astype(F32)
            squares += jnp.sum(floats * floats, axis=0, keepdims=True)
        scaled = total * lax.rsqrt(squares / width + epsilon)
        for side in range(2):
            part = jnp.concatenate(
                [scaled[side * span : (side + 1) * span], jnp.zeros((128 - span, seqs), F32)], axis=0
            )
            turned = part.T.astype(BF16)
            for to in range(nz):
                out_a[to, side, p] = turned[2 * ny * to : 2 * ny * (to + 1)]

    def a_copy(d):
        to = wrap(z + d, nz)
        return pltpu.make_async_remote_copy(
            src_ref=out_a.at[to],
            dst_ref=in_a.at[z],
            send_sem=a_sent.at[d],
            recv_sem=a_got.at[z],
            device_id={"kv_0": to},
            device_id_type=MESH,
        )

    def a_wait(d):
        came = wrap(z + d, nz)
        pltpu.make_async_remote_copy(
            src_ref=in_a.at[came],
            dst_ref=in_a.at[came],
            send_sem=a_sent.at[0],
            recv_sem=a_got.at[came],
            device_id=partner,
            device_id_type=MESH,
        ).wait_recv()

    tokens.loop(1, nz, lambda i: a_copy(far_first(i, nz)).start())
    own_a = pltpu.make_async_copy(out_a.at[z], in_a.at[z], local.at[10])
    own_a.start()
    ring.share_on()

    shift = heads.bit_length() - 1

    def prop_of(i):
        return 2 * (i >> (shift + 2)) + ((i >> shift) & 1)

    def at_of(i):
        return ((i >> (shift + 1)) & 1) * heads + (i & (heads - 1))

    row = iota((count, 128), 0)
    first = jnp.where((row >> (shift + 1)) & 1 == 0, lengths[0] + accepted[0], lengths[1] + accepted[1])
    angles = (first + prop_of(row)).astype(F32) * frequency[...]
    cosine = jnp.cos(angles)
    lane_sign = jnp.where(iota((count, 128), 1) < key_size // 2, -1.0, 1.0)
    sine = jnp.sin(angles) * lane_sign
    decays = by_head((count, 128))
    query_decay = jnp.exp(decays * (prop_of(row) + 1).astype(F32))
    other = iota((count, count), 1)
    here = row[:, :count]
    offset = prop_of(here) - prop_of(other)
    grid = jnp.where(
        (at_of(here) == at_of(other)) & (offset >= 0),
        jnp.exp(decays[:, :count] * jnp.maximum(offset, 0).astype(F32)),
        0.0,
    )

    own_a.wait()
    tokens.loop(1, nz, a_wait)

    mid[...] = in_a[...].reshape(nz * 4 * 2 * ny, 128).astype(F32)
    stride = 4 * 2 * ny
    for to in range(ny):
        for side in range(2):
            for s in range(2):
                parts = [
                    mid[pl.ds(side * 4 * ny + p * 2 * ny + 2 * to + s, nz, stride=stride), :]
                    for p in range(2)
                ]
                out_b[to, side, s] = jnp.concatenate(parts, axis=0).astype(BF16)

    def b_copy(d, same):
        to = wrap(y + d, ny)
        side = tp if same else 1 - tp
        return pltpu.make_async_remote_copy(
            src_ref=out_b.at[to, side],
            dst_ref=in_b.at[y, tp],
            send_sem=b_sent.at[d, side],
            recv_sem=b_got.at[y, tp],
            device_id={"kv_1": to, "tp": side},
            device_id_type=MESH,
        )

    def b_wait(d, same):
        came = wrap(y + d, ny)
        side = tp if same else 1 - tp
        pltpu.make_async_remote_copy(
            src_ref=in_b.at[came, side],
            dst_ref=in_b.at[came, side],
            send_sem=b_sent.at[0, 0],
            recv_sem=b_got.at[came, side],
            device_id=partner,
            device_id_type=MESH,
        ).wait_recv()

    def b_start(i):
        d = far_first(i, ny)
        b_copy(d, True).start()
        b_copy(d, False).start()

    tokens.loop(1, ny, b_start)
    b_copy(0, False).start()
    own_b = pltpu.make_async_copy(out_b.at[y, tp], in_b.at[y, tp], local.at[11])
    own_b.start()

    lane = iota((128, 2 * key_size + 2 * value_size), 0)
    column = iota((128, 2 * key_size + 2 * value_size), 1)
    for j in range(ny):
        goal = jnp.where(
            lane < kc,
            kc * j + lane,
            jnp.where(
                lane < 2 * kc,
                key_size + kc * j + lane - kc,
                jnp.where(
                    lane < 2 * kc + vc,
                    2 * key_size + vc * j + lane - 2 * kc,
                    2 * key_size + value_size + vc * j + lane - 2 * kc - vc,
                ),
            ),
        )
        hit = (goal == column) & (lane < span)
        place[pl.ds(128 * j, 128)] = jnp.where(hit, 1.0, 0.0).astype(BF16)
    own_b.wait()
    b_wait(0, False)

    def b_take(d):
        b_wait(d, True)
        b_wait(d, False)

    tokens.loop(1, ny, b_take)

    packed = jnp.concatenate([in_b[j].reshape(count, 128) for j in range(ny)], axis=1)
    fields = jnp.dot(packed, place[...], preferred_element_type=F32)
    query = fields[:, :key_size]
    key = fields[:, key_size : 2 * key_size]
    value = fields[:, 2 * key_size : 2 * key_size + value_size]
    gate = fields[:, 2 * key_size + value_size :]
    half = key_size // 2

    def turned_by(x):
        swapped = jnp.concatenate([x[:, half:], x[:, :half]], axis=1)
        return x * cosine + swapped * sine

    query_rot = turned_by(query).astype(BF16)
    key_f = turned_by(key) * key_size ** (-0.5)
    key_rot = key_f.astype(BF16)
    value_b = value.astype(BF16)
    scores = lax.dot_general(
        query_rot, key_rot, (((1,), (1,)), ((), ())), preferred_element_type=F32
    )
    inner = jnp.dot((scores * grid).astype(BF16), value_b, preferred_element_type=F32)
    decayed = query_rot.astype(F32) * query_decay
    row_at = at_of(iota((count, 1), 0))
    spread = jnp.concatenate(
        [jnp.where(row_at == at, decayed, 0.0).astype(BF16) for at in range(2 * heads)], axis=1
    )
    states = state_b[...].reshape(2 * heads * key_size, value_size)
    heads_out = inner + jnp.dot(spread, states, preferred_element_type=F32)
    normed = heads_out * lax.rsqrt(jnp.mean(heads_out * heads_out, axis=-1, keepdims=True) + epsilon)
    product = gate / (1.0 + jnp.exp(-gate)) * normed
    for c in range(value_size // 128):
        rows_f[c] = product[:, 128 * c : 128 * (c + 1)]
    for i in range(8):
        prop, seq = 2 * (i // 4) + i % 2, (i // 2) % 2
        keys_out[seq, prop] = key_f[i * heads : (i + 1) * heads].astype(BF16)
        values_out[seq, prop] = value[i * heads : (i + 1) * heads].astype(BF16)
    cut = heads * value_size // 2
    for h in range(heads):
        part, at = divmod(h * value_size, cut)
        for c in range(value_size // 128):
            piece = rows_f[c, pl.ds(h, 8, stride=heads), :]
            chunk[part, :, at + 128 * c : at + 128 * (c + 1)] = piece.astype(BF16)

    first = ((y, ny, "kv_1"), (z, nz, "kv_0"))
    second = ((z, nz, "kv_0"), (y, ny, "kv_1"))

    def g_copy(p, d):
        f, n, axis = first[p]
        return pltpu.make_async_remote_copy(
            src_ref=chunk.at[p],
            dst_ref=gated_all.at[p, f],
            send_sem=g_sent.at[p, d],
            recv_sem=g_got.at[p, f],
            device_id={axis: wrap(f + d, n)},
            device_id_type=MESH,
        )

    def g_start(i):
        for p in range(2):
            g_copy(p, far_first(i, first[p][1])).start()

    tokens.loop(1, ny, g_start)
    for p in range(2):
        f = first[p][0]
        pltpu.make_async_copy(chunk.at[p], gated_all.at[p, f], g_got.at[p, f]).start()

    source = iota((4 * seqs, seqs), 0)
    target = iota((4 * seqs, seqs), 1)
    low_ring, high_ring = (source >> 3) & (ny - 1), source >> (2 + ny.bit_length())
    for part, group in enumerate((high_ring * ny + low_ring, low_ring * ny + high_ring)):
        row_seq = 2 * group + ((source >> 1) & 1)
        row_prop = 2 * ((source >> 2) & 1) + (source & 1)
        for p in range(4):
            hit = (row_seq == target) & (row_prop == p)
            order[part, :, pl.ds(seqs * p, seqs)] = jnp.where(hit, 1.0, 0.0).astype(BF16)
    ring.all_here()

    def c_copy(p, d, same):
        s, n, axis = second[p]
        to = wrap(s + d, n)
        side = tp if same else 1 - tp
        return pltpu.make_async_remote_copy(
            src_ref=out_c.at[p, to, side],
            dst_ref=in_c.at[p, tp, s],
            send_sem=c_sent.at[p, d, side],
            recv_sem=c_got.at[p, tp, s],
            device_id={axis: to, "tp": side},
            device_id_type=MESH,
        )

    def wait_for(block, arrived):
        pltpu.make_async_remote_copy(
            src_ref=block,
            dst_ref=block,
            send_sem=a_sent.at[0],
            recv_sem=arrived,
            device_id=partner,
            device_id_type=MESH,
        ).wait_recv()

    out_cols = wo.shape[0]
    for p in range(2):
        n = first[p][1]
        tokens.loop(0, n, lambda f, p=p: wait_for(gated_all.at[p, f], g_got.at[p, f]))
        product = lax.dot_general(
            wo_all[p].reshape(second[p][1] * out_cols, cut),
            gated_all[p].reshape(n * 8, cut),
            (((1,), (1,)), ((), ())),
            preferred_element_type=F32,
        )
        part = out_cols // 2
        for to in range(second[p][1]):
            for side in range(2):
                at = to * out_cols + side * part
                halves = [product[at + e : at + e + part // 2] for e in (0, part // 2)]
                out_c[p, to, side] = jnp.concatenate(halves, axis=1).astype(BF16)

        def c_start(i, p=p, n=n):
            d = far_first(i, n)
            c_copy(p, d, True).start()
            c_copy(p, d, False).start()

        tokens.loop(1, n, c_start)
        c_copy(p, 0, False).start()
        s = second[p][0]
        pltpu.make_async_copy(
            out_c.at[p, s, tp], in_c.at[p, tp, s], c_got.at[p, tp, s]
        ).start()
    result = jnp.zeros((out_cols // 2, 4 * seqs), F32)
    for p in range(2):
        n = second[p][1]
        for side in range(2):
            tokens.loop(
                0, n, lambda s, p=p, side=side: wait_for(in_c.at[p, side, s], c_got.at[p, side, s])
            )
        sums = []
        for side in range(2):
            pairs = [[in_c[p, side, 2 * j + e].astype(F32) for e in range(2)] for j in range(n // 2)]
            for cut_at in (slice(0, 64), slice(64, 128)):
                sums.append(
                    jnp.concatenate([each[:, cut_at] for pair in pairs for each in pair], axis=1)
                )
        sums = jnp.concatenate(sums, axis=0).astype(BF16)
        moved = jnp.dot(sums, order[p], preferred_element_type=F32)
        result += moved[: out_cols // 2] + moved[out_cols // 2 :]
    result = result.astype(BF16)
    for p in range(4):
        ret_out[p] = result[:, p * seqs : (p + 1) * seqs]
    tokens.finish()
    ring.finish()

    def late_done(d):
        for p in range(2):
            g_copy(p, d).wait_send()
            for same in (True, False):
                c_copy(p, d, same).wait_send()

    tokens.loop(1, ny, late_done)
    for p in range(2):
        c_copy(p, 0, False).wait_send()
    tokens.loop(1, nz, lambda d: a_copy(d).wait_send())

    def b_done(d):
        b_copy(d, True).wait_send()
        b_copy(d, False).wait_send()

    tokens.loop(1, ny, b_done)
    b_copy(0, False).wait_send()


def in_hbm(value):
    return pltpu.with_memory_space_constraint(value, pltpu.HBM)


def put_kernel(*refs):
    count = (len(refs) - 1) // 2
    sems = refs[-1]
    copies = [
        pltpu.make_async_copy(refs[i], refs[count + i], sems.at[i]) for i in range(count)
    ]
    for copy in copies:
        copy.start()
    for copy in copies:
        copy.wait()


def put_out(*values):
    return pl.pallas_call(
        put_kernel,
        out_shape=tuple(jax.ShapeDtypeStruct(v.shape, v.dtype) for v in values),
        in_specs=[pl.BlockSpec(memory_space=pl.ANY)] * len(values),
        out_specs=(pl.BlockSpec(memory_space=pltpu.HBM),) * len(values),
        scratch_shapes=[pltpu.SemaphoreType.DMA((len(values),))],
        compiler_params=pltpu.CompilerParams(vmem_limit_bytes=8 * 1024 * 1024),
    )(*values)


def shards(
    nx,
    nz,
    ny,
    tokens,
    norm_gain,
    query_weight,
    key_weight,
    value_weight,
    gate_weight,
    out_weight,
    decay_rate,
    prior_state,
    last_keys,
    last_values,
    accepted,
    lengths,
):
    _, heads, key_size, value_size = prior_state.shape
    seqs, _, depth = tokens.shape
    width = norm_gain.shape[0]
    kc, vc = query_weight.shape[1], value_weight.shape[1]
    span = 2 * kc + 2 * vc
    count = 8 * heads
    half = key_size // 2
    frequency = jnp.power(10000.0, -jnp.arange(half, dtype=F32) / half)
    frequency = jnp.concatenate([frequency, frequency])[None, :]

    hbm = pl.BlockSpec(memory_space=pltpu.HBM)
    vmem = pl.BlockSpec(memory_space=pltpu.VMEM)
    dma = pltpu.SemaphoreType.DMA
    cut = heads * value_size // 2
    out_cols = out_weight.shape[1]
    retained, state, new_keys, new_values = pl.pallas_call(
        functools.partial(kernel, nx, nz, ny),
        out_shape=(
            jax.ShapeDtypeStruct((4, out_cols // 2, seqs), BF16),
            jax.ShapeDtypeStruct((2 * heads, key_size, value_size), F32),
            jax.ShapeDtypeStruct((2, 4, heads, key_size), BF16),
            jax.ShapeDtypeStruct((2, 4, heads, value_size), BF16),
        ),
        in_specs=[hbm] * 13 + [vmem],
        out_specs=(vmem,) * 4,
        scratch_shapes=[
            pltpu.VMEM((2, depth, seqs), BF16),
            pltpu.VMEM((2, span, width), BF16),
            pltpu.VMEM((2, nz, out_cols, cut), BF16),
            pltpu.VMEM((2 * heads, key_size, value_size), F32),
            pltpu.VMEM((2, 4 * heads, key_size), BF16),
            pltpu.VMEM((2, 4 * heads, value_size), BF16),
            pltpu.SMEM((heads,), F32),
            pltpu.SMEM((2,), jnp.int32),
            pltpu.SMEM((2,), jnp.int32),
            pltpu.VMEM((width,), BF16),
            pltpu.VMEM((1, width), F32),
            pltpu.VMEM((2, 2, 4 * heads, key_size), F32),
            pltpu.VMEM((2 * heads, key_size, value_size), BF16),
            pltpu.VMEM((2, nz, ny, depth, seqs), BF16),
            pltpu.VMEM((128 * ny, 2 * key_size + 2 * value_size), BF16),
            pltpu.VMEM((2, 4 * seqs, 4 * seqs), BF16),
            pltpu.VMEM((nz, 2, 2, 2 * ny, 128), BF16),
            pltpu.VMEM((nz, 2, 2, 2 * ny, 128), BF16),
            pltpu.VMEM((nz * 8 * ny, 128), F32),
            pltpu.VMEM((ny, 2, 2, 2 * nz, 128), BF16),
            pltpu.VMEM((ny, 2, 2, 2 * nz, 128), BF16),
            pltpu.VMEM((value_size // 128, count, 128), F32),
            pltpu.VMEM((2, 8, cut), BF16),
            pltpu.VMEM((2, nz, 8, cut), BF16),
            pltpu.VMEM((2, nz, 2, out_cols // 4, 128), BF16),
            pltpu.VMEM((2, 2, nz, out_cols // 4, 128), BF16),
            dma((23,)),
            dma((2, nz, ny)),
            dma((2, max(nz, ny), TorusGather.groups)),
            dma((2, max(nz, ny))),
            dma((2, 2, nz // 2, TorusGather.groups)),
            dma((2, nz)),
            dma((2, 2, nz // 2)),
            dma((2, 2, nz)),
            dma((2, 2, nz)),
            dma((2,)),
            dma((2,)),
            dma((2, nz)),
            dma((2, nz)),
            dma((2, nz, 2)),
            dma((2, 2, nz)),
            dma((4,)),
            dma((nz,)),
            dma((nz,)),
            dma((ny, 2)),
            dma((ny, 2)),
        ],
        compiler_params=pltpu.CompilerParams(
            collective_id=0, has_side_effects=True, vmem_limit_bytes=48 * 1024 * 1024
        ),
    )(
        *map(
            in_hbm,
            (
                tokens.transpose(1, 2, 0),
                query_weight.T,
                key_weight.T,
                value_weight.T,
                gate_weight.T,
                out_weight.T,
                prior_state.reshape(2 * heads, key_size, value_size),
                last_keys.reshape(2, 4 * heads, key_size),
                last_values.reshape(2, 4 * heads, value_size),
                decay_rate,
                accepted,
                lengths,
                norm_gain,
            ),
        ),
        frequency,
    )
    retained, state, new_keys, new_values = put_out(retained, state, new_keys, new_values)
    return (
        retained.transpose(2, 0, 1),
        state.reshape(prior_state.shape),
        new_keys,
        new_values,
    )


def solution(mesh):
    nz = ny = 8
    finer = Mesh(
        mesh.devices.reshape(mesh.shape["dp"], nz, ny, mesh.shape["tp"]),
        ("dp", "kv_0", "kv_1", "tp"),
    )
    return jax.shard_map(
        functools.partial(shards, mesh.shape["dp"], nz, ny),
        mesh=finer,
        in_specs=(
            P("dp", None, KV),
            P(),
            P(None, TP_KV),
            P(None, TP_KV),
            P(None, TP_KV),
            P(None, TP_KV),
            P("tp", KV),
            P("tp"),
            P(DP_KV, "tp", None, None),
            P(DP_KV, None, "tp", None),
            P(DP_KV, None, "tp", None),
            P(DP_KV),
            P(DP_KV),
        ),
        out_specs=(
            P("dp", None, KV_TP),
            P(DP_KV, "tp", None, None),
            P(DP_KV, None, "tp", None),
            P(DP_KV, None, "tp", None),
        ),
        check_vma=False,
    )
```

```python
import functools

import jax
import jax.numpy as jnp
from jax import lax
from jax.experimental import pallas as pl
from jax.experimental.pallas import tpu as pltpu
from jax.sharding import Mesh
from jax.sharding import PartitionSpec as P

KV = ("kv_0", "kv_1")
TP_KV = ("tp", "kv_0", "kv_1")
DP_KV = ("dp", "kv_0", "kv_1")
KV_TP = ("kv_0", "kv_1", "tp")
MESH = pl.DeviceIdType.MESH
F32, BF16 = jnp.float32, jnp.bfloat16

epsilon = 1e-06


def wrap(i, n):
    return i & (n - 1)


def far_first(i, n):
    return wrap(n // 2 + (1 - 2 * (i & 1)) * (i >> 1), n)


def near_first(i, n):
    odd = i & 1
    return wrap(odd * ((i + 1) >> 1) + (1 - odd) * (n - (i >> 1)), n)


class TorusGather:
    groups = 8
    turn = (0, 1, 7, 2, 6, 3, 5, 4)

    def __init__(self, own, held, arrived, ring_arrived, first_sent, ring_sent, nz, ny):
        self.own, self.held, self.arrived, self.ring_arrived = own, held, arrived, ring_arrived
        self.first_sent, self.ring_sent = first_sent, ring_sent
        z, y = lax.axis_index("kv_0"), lax.axis_index("kv_1")
        self.partner = {"tp": 1 - lax.axis_index("tp")}
        self.first = ((y, ny, "kv_1"), (z, nz, "kv_0"))
        self.second = ((z, nz, "kv_0"), (y, ny, "kv_1"))
        self.hops = nz // 2
        self.size = ny // self.groups

    def at(self, ref, p, f, s):
        return ref.at[p, s, f] if p == 0 else ref.at[p, f, s]

    def copy(self, target, source, sent, arrived, device):
        return pltpu.make_async_remote_copy(
            src_ref=source,
            dst_ref=target,
            send_sem=sent,
            recv_sem=arrived,
            device_id=device,
            device_id_type=MESH,
        )

    def first_copy(self, p, d):
        (f, n, axis), (s, _, _) = self.first[p], self.second[p]
        return self.copy(
            self.at(self.held, p, f, s),
            self.own(p),
            self.first_sent.at[p, d],
            self.at(self.arrived, p, f, s),
            {axis: wrap(f + d, n)},
        )

    def start_first(self):
        def send(i):
            for p in range(2):
                self.first_copy(p, near_first(i, self.first[p][1])).start()

        self.loop(1, self.first[0][1], send)
        for p in range(2):
            (f, _, _), (s, _, _) = self.first[p], self.second[p]
            pltpu.make_async_copy(
                self.own(p), self.at(self.held, p, f, s), self.at(self.arrived, p, f, s)
            ).start()

    def group(self, p, i):
        f = self.first[p][0]
        return wrap(f // self.size + self.turn[i], self.groups)

    def group_at(self, p, q, s):
        return self.at(self.held, p, pl.ds(q * self.size, self.size), s)

    def ring_copy(self, p, k, i, way, reach=1):
        s, n, axis = self.second[p]
        q, origin = self.group(p, i), wrap(s - way * k + n, n)
        block = self.group_at(p, q, origin)
        return self.copy(
            block,
            block,
            self.ring_sent.at[p, (1 + way) // 2, k + reach - 1, i],
            self.ring_arrived.at[p, origin, q],
            {axis: wrap(s + reach * way + n, n)},
        )

    def wait_chunk(self, p, f, s):
        chunk = self.at(self.held, p, f, s)
        self.copy(
            chunk, chunk, self.first_sent.at[0, 0], self.at(self.arrived, p, f, s), self.partner
        ).wait_recv()

    def wait_group(self, p, i, s):
        q = self.group(p, i)
        block = self.group_at(p, q, s)
        self.copy(
            block, block, self.first_sent.at[0, 0], self.ring_arrived.at[p, s, q], self.partner
        ).wait_recv()

    def pass_on(self, k, i, ways):
        for p in range(2):
            s, n, _ = self.second[p]
            if k == 0:
                for e in range(self.size):
                    self.wait_chunk(p, self.group(p, i) * self.size + e, s)
                for way in ways:
                    self.ring_copy(p, k, i, way).start()
            else:
                for way in (1, -1):
                    self.wait_group(p, i, wrap(s - way * k + n, n))
                    if k == self.hops - 2 and way == self.far_way(i):
                        self.ring_copy(p, k, i, way, 2).start()
                    if way in ways:
                        self.ring_copy(p, k, i, way).start()

    def loop(self, low, high, step):
        def body(i, _):
            step(i)
            return 0

        lax.fori_loop(low, high, body, 0)

    def ways(self, k, i):
        return (1, -1) if k < self.hops - 1 else ()

    def far_way(self, i):
        return 1 if i % 2 else -1

    def round(self, k, beside=None):
        for i in range(self.groups):
            self.pass_on(k, i, self.ways(k, i))
            if beside is not None:
                beside()

    def last_arrivals(self):
        for i in range(self.groups):
            for p in range(2):
                s, n, _ = self.second[p]
                self.wait_group(p, i, wrap(s + self.hops, n))

    def finish(self):
        def first_done(d):
            for p in range(2):
                self.first_copy(p, d).wait_send()

        self.loop(1, self.first[0][1], first_done)
        for k in range(self.hops):
            for i in range(self.groups):
                for p in range(2):
                    for way in self.ways(k, i):
                        self.ring_copy(p, k, i, way).wait_send()
                    if k == self.hops - 2:
                        self.ring_copy(p, k, i, self.far_way(i), 2).wait_send()


class WeightRing:
    def __init__(self, held, arrived, sent, side_arrived, side_sent, on_arrived, on_sent, nx, nz, ny):
        self.held, self.arrived, self.sent = held, arrived, sent
        self.side_arrived, self.side_sent = side_arrived, side_sent
        self.on_arrived, self.on_sent = on_arrived, on_sent
        self.x, self.nx = lax.axis_index("dp"), nx
        z, y = lax.axis_index("kv_0"), lax.axis_index("kv_1")
        self.partner = {"tp": 1 - lax.axis_index("tp")}
        self.second = ((z, nz, "kv_0"), (y, ny, "kv_1"))
        self.hops = nz // 2
        self.rows = held.shape[2] // nx

    def block(self, p, origin, x):
        return self.held.at[p, origin, pl.ds(pl.multiple_of(self.rows * x, self.rows), self.rows)]

    def copy(self, block, sent, arrived, device):
        return pltpu.make_async_remote_copy(
            src_ref=block,
            dst_ref=block,
            send_sem=sent,
            recv_sem=arrived,
            device_id=device,
            device_id_type=MESH,
        )

    def ring_copy(self, p, k, way, reach=1):
        s, n, axis = self.second[p]
        origin = wrap(s - way * k + n, n)
        return self.copy(
            self.block(p, origin, self.x),
            self.sent.at[p, (1 + way) // 2, k + reach - 1],
            self.arrived.at[p, origin],
            {axis: wrap(s + reach * way + n, n)},
        )

    def side_copy(self, p, origin, way):
        at = (1 + way) // 2
        return self.copy(
            self.block(p, origin, self.x),
            self.side_sent.at[p, at, origin],
            self.side_arrived.at[p, at, origin],
            {"dp": wrap(self.x + way + self.nx, self.nx)},
        )

    def on_way(self, p):
        return 1 - 2 * p

    def on_copy(self, p):
        way = self.on_way(p)
        x = wrap(self.x - way + self.nx, self.nx)
        block = self.held.at[p, :, pl.ds(pl.multiple_of(self.rows * x, self.rows), self.rows)]
        return self.copy(
            block,
            self.on_sent.at[p],
            self.on_arrived.at[p],
            {"dp": wrap(self.x + way + self.nx, self.nx)},
        )

    def forward_ways(self, p, k):
        return (1, -1) if k < self.hops - 1 else ()

    def step(self, k):
        for p in range(2):
            s, n, _ = self.second[p]
            for way in (1,) if k in (0, self.hops) else (1, -1):
                origin = wrap(s - way * k + n, n)
                if k > 0:
                    self.copy(
                        self.block(p, origin, self.x),
                        self.sent.at[0, 0, 0],
                        self.arrived.at[p, origin],
                        self.partner,
                    ).wait_recv()
                ways = self.forward_ways(p, k)
                for to in ways if k == 0 else (way,):
                    if to in ways:
                        self.ring_copy(p, k, to).start()
                        if k == self.hops - 2 and to == self.on_way(p):
                            self.ring_copy(p, k, to, 2).start()
                for to in (1, -1):
                    self.side_copy(p, origin, to).start()

    def side_wait(self, p, way):
        x = wrap(self.x - way + self.nx, self.nx)

        def take(origin, _):
            self.copy(
                self.block(p, origin, x),
                self.sent.at[0, 0, 0],
                self.side_arrived.at[p, (1 + way) // 2, origin],
                self.partner,
            ).wait_recv()
            return 0

        lax.fori_loop(0, self.second[p][1], take, 0)

    def share_on(self):
        for p in range(2):
            self.side_wait(p, self.on_way(p))
            self.on_copy(p).start()

    def all_here(self):
        for p in range(2):
            self.side_wait(p, -self.on_way(p))
            self.on_copy(p).wait_recv()

    def finish(self):
        for p in range(2):
            for k in range(self.hops):
                for way in self.forward_ways(p, k):
                    self.ring_copy(p, k, way).wait_send()
            self.ring_copy(p, self.hops - 2, self.on_way(p), 2).wait_send()

            def done(origin, _, p=p):
                for way in (1, -1):
                    self.side_copy(p, origin, way).wait_send()
                return 0

            lax.fori_loop(0, self.second[p][1], done, 0)
            self.on_copy(p).wait_send()


def iota(shape, dim):
    return lax.broadcasted_iota(jnp.int32, shape, dim)


def kernel(
    nx,
    nz,
    ny,
    tok,
    wq,
    wk,
    wv,
    wg,
    wo,
    prior,
    last_k_in,
    last_v_in,
    decay_in,
    accepted_in,
    lengths_in,
    gain_in,
    frequency,
    ret_out,
    state_out,
    keys_out,
    values_out,
    tok_v,
    weights,
    wo_all,
    prior_v,
    last_k,
    last_v,
    decay,
    accepted,
    lengths,
    gain_v,
    gain,
    weighted_keys,
    state_b,
    tokens_all,
    place,
    order,
    out_a,
    in_a,
    mid,
    out_b,
    in_b,
    rows_f,
    chunk,
    gated_all,
    out_c,
    in_c,
    local,
    tok_arrived,
    tok_passed,
    tok_first,
    tok_ring,
    wo_arrived,
    wo_sent,
    wo_side,
    wo_side_sent,
    wo_on,
    wo_on_sent,
    g_sent,
    g_got,
    c_sent,
    c_got,
    pair_sems,
    a_sent,
    a_got,
    b_sent,
    b_got,
):
    x, z, y, tp = (lax.axis_index(axis) for axis in ("dp", "kv_0", "kv_1", "tp"))
    heads, seqs = nz, 2 * nz * ny
    kc = wq.shape[0]
    vc = wv.shape[0]
    span = 2 * kc + 2 * vc
    depth = tok_v.shape[1]
    width = nz * ny * depth
    partner = {"tp": 1 - tp}

    loads = [
        pltpu.make_async_copy(tok.at[pl.ds(2 * tp, 2)], tok_v, local.at[0]),
        pltpu.make_async_copy(wq, weights.at[tp, pl.ds(0, kc)], local.at[1]),
        pltpu.make_async_copy(wk, weights.at[tp, pl.ds(kc, kc)], local.at[2]),
        pltpu.make_async_copy(wv, weights.at[tp, pl.ds(2 * kc, vc)], local.at[3]),
        pltpu.make_async_copy(wg, weights.at[tp, pl.ds(2 * kc + vc, vc)], local.at[4]),
        pltpu.make_async_copy(prior, prior_v, local.at[5]),
    ]
    small_loads = [
        pltpu.make_async_copy(source, target, local.at[17 + i])
        for i, (source, target) in enumerate(
            (
                (last_k_in, last_k),
                (last_v_in, last_v),
                (decay_in, decay),
                (accepted_in, accepted),
                (lengths_in, lengths),
                (gain_in, gain_v),
            )
        )
    ]
    share = wo.shape[0] // nx
    mine = pl.ds(pl.multiple_of(share * x, share), share)
    half_k = wo.shape[1] // 2
    own_out = [
        pltpu.make_async_copy(
            wo.at[mine, pl.ds(p * half_k, half_k)], wo_all.at[p, (z, y)[p], mine], local.at[7 + p]
        )
        for p in range(2)
    ]
    for load in loads + own_out + small_loads:
        load.start()

    barrier = pltpu.get_barrier_semaphore()

    def greet(device):
        pl.semaphore_signal(barrier, inc=1, device_id=device, device_id_type=MESH)

    def greet_y(d, _):
        other = wrap(y + d, ny)
        greet({"kv_1": other})
        greet({"kv_1": other, "tp": 1 - tp})
        return 0

    def greet_z(d, _):
        greet({"kv_0": wrap(z + d, nz)})
        return 0

    lax.fori_loop(1, ny, greet_y, 0)
    lax.fori_loop(1, nz, greet_z, 0)
    def greet_tall(d, _):
        greet({"kv_0": wrap(z + d, nz), "tp": 1 - tp})
        return 0

    lax.fori_loop(1, nz, greet_tall, 0)
    greet(partner)
    for way in (1, nx - 1):
        greet({"dp": wrap(x + way, nx)})
    pl.semaphore_wait(barrier, 2 * (ny - 1) + 2 * (nz - 1) + 3)

    loads[0].wait()
    tokens = TorusGather(
        lambda p: tok_v.at[p], tokens_all, tok_arrived, tok_passed, tok_first, tok_ring, nz, ny
    )
    tokens.start_first()
    ring = WeightRing(
        wo_all, wo_arrived, wo_sent, wo_side, wo_side_sent, wo_on, wo_on_sent, nx, nz, ny
    )
    for load in own_out:
        load.wait()
    ring.step(0)
    for load in loads[1:5]:
        load.wait()
    swap = pltpu.make_async_remote_copy(
        src_ref=weights.at[tp],
        dst_ref=weights.at[tp],
        send_sem=pair_sems.at[0],
        recv_sem=pair_sems.at[1],
        device_id=partner,
        device_id_type=MESH,
    )
    swap.start()

    key_size, value_size = ny * kc, ny * vc

    loads[5].wait()
    for load in small_loads:
        load.wait()
    rows, count = 4 * heads, 8 * heads
    head_of = iota((rows, 1), 0) & (heads - 1)

    def by_head(shape):
        head = iota(shape, 0) & (heads - 1)
        table = jnp.zeros(shape, F32)
        for h in range(heads):
            table = jnp.where(head == h, -decay[h], table)
        return table

    taken_decay = by_head((rows, 128))
    before = iota((rows, 128), 0) >> (heads.bit_length() - 1)
    for s in range(2):
        power = jnp.maximum(accepted[s] - 1 - before, 0).astype(F32)
        key_weights = jnp.where(before < accepted[s], jnp.exp(taken_decay * power), 0.0)
        weighted = last_k[s].astype(F32) * key_weights
        high = weighted.astype(BF16).astype(F32)
        weighted_keys[s, 0] = high
        weighted_keys[s, 1] = weighted - high

    def one_head(h):
        mine = head_of == h
        for s in range(2):
            both = jnp.concatenate(
                [jnp.where(mine, weighted_keys[s, part], 0.0) for part in range(2)], axis=0
            )
            values = jnp.concatenate([last_v[s], last_v[s]], axis=0)
            update = lax.dot_general(
                both.astype(BF16), values, (((0,), (0,)), ((), ())), preferred_element_type=F32
            )
            at = s * heads + h
            power = jnp.full((1, value_size), -decay[h] * accepted[s].astype(F32), F32)
            fresh = jnp.exp(power) * prior_v[at] + update
            state_out[at] = fresh
            state_b[at] = fresh.astype(BF16)

    blocks = span // 16

    def scale_rows(i):
        at = pl.ds(i * 16, 16)
        for side in range(2):
            weights[side, at] = (weights[side, at].astype(F32) * gain[...]).astype(BF16)

    def first_scale():
        swap.wait()
        gain[...] = gain_v[...].astype(F32).reshape(1, width)
        scale_rows(0)

    one_head(0)
    one_head(1)
    work = [functools.partial(one_head, h) for h in range(2, heads)]
    work += [first_scale] + [functools.partial(scale_rows, i) for i in range(1, blocks)]
    work = iter(work)

    def beside():
        piece = next(work, None)
        if piece is not None:
            piece()

    for k in range(tokens.hops):
        if k > 0:
            ring.step(k)
        tokens.round(k, beside)
    ring.step(tokens.hops)
    tokens.last_arrivals()

    for p in range(2):
        total = jnp.zeros((2 * span, seqs), F32)
        squares = jnp.zeros((1, seqs), F32)
        for c in range(nz):
            block = tokens_all[p, c].reshape(ny * depth, seqs)
            cut = pl.ds(c * ny * depth, ny * depth)
            total += jnp.dot(
                weights[:, :, cut].reshape(2 * span, ny * depth), block, preferred_element_type=F32
            )
            floats = block.astype(F32)
            squares += jnp.sum(floats * floats, axis=0, keepdims=True)
        scaled = total * lax.rsqrt(squares / width + epsilon)
        for side in range(2):
            part = jnp.concatenate(
                [scaled[side * span : (side + 1) * span], jnp.zeros((128 - span, seqs), F32)], axis=0
            )
            turned = part.T.astype(BF16)
            for to in range(nz):
                out_a[to, side, p] = turned[2 * ny * to : 2 * ny * (to + 1)]

    def a_copy(d):
        to = wrap(z + d, nz)
        return pltpu.make_async_remote_copy(
            src_ref=out_a.at[to],
            dst_ref=in_a.at[z],
            send_sem=a_sent.at[d],
            recv_sem=a_got.at[z],
            device_id={"kv_0": to},
            device_id_type=MESH,
        )

    def a_wait(d):
        came = wrap(z + d, nz)
        pltpu.make_async_remote_copy(
            src_ref=in_a.at[came],
            dst_ref=in_a.at[came],
            send_sem=a_sent.at[0],
            recv_sem=a_got.at[came],
            device_id=partner,
            device_id_type=MESH,
        ).wait_recv()

    tokens.loop(1, nz, lambda i: a_copy(far_first(i, nz)).start())
    own_a = pltpu.make_async_copy(out_a.at[z], in_a.at[z], local.at[10])
    own_a.start()
    ring.share_on()

    shift = heads.bit_length() - 1

    def prop_of(i):
        return 2 * (i >> (shift + 2)) + ((i >> shift) & 1)

    def at_of(i):
        return ((i >> (shift + 1)) & 1) * heads + (i & (heads - 1))

    row = iota((count, 128), 0)
    first = jnp.where((row >> (shift + 1)) & 1 == 0, lengths[0] + accepted[0], lengths[1] + accepted[1])
    angles = (first + prop_of(row)).astype(F32) * frequency[...]
    cosine = jnp.cos(angles)
    lane_sign = jnp.where(iota((count, 128), 1) < key_size // 2, -1.0, 1.0)
    sine = jnp.sin(angles) * lane_sign
    decays = by_head((count, 128))
    query_decay = jnp.exp(decays * (prop_of(row) + 1).astype(F32))
    other = iota((count, count), 1)
    here = row[:, :count]
    offset = prop_of(here) - prop_of(other)
    grid = jnp.where(
        (at_of(here) == at_of(other)) & (offset >= 0),
        jnp.exp(decays[:, :count] * jnp.maximum(offset, 0).astype(F32)),
        0.0,
    )

    own_a.wait()
    tokens.loop(1, nz, a_wait)

    mid[...] = in_a[...].reshape(nz * 4 * 2 * ny, 128).astype(F32)
    stride = 4 * 2 * ny
    for to in range(ny):
        for side in range(2):
            for s in range(2):
                parts = [
                    mid[pl.ds(side * 4 * ny + p * 2 * ny + 2 * to + s, nz, stride=stride), :]
                    for p in range(2)
                ]
                out_b[to, side, s] = jnp.concatenate(parts, axis=0).astype(BF16)

    def b_copy(d, same):
        to = wrap(y + d, ny)
        side = tp if same else 1 - tp
        return pltpu.make_async_remote_copy(
            src_ref=out_b.at[to, side],
            dst_ref=in_b.at[y, tp],
            send_sem=b_sent.at[d, side],
            recv_sem=b_got.at[y, tp],
            device_id={"kv_1": to, "tp": side},
            device_id_type=MESH,
        )

    def b_wait(d, same):
        came = wrap(y + d, ny)
        side = tp if same else 1 - tp
        pltpu.make_async_remote_copy(
            src_ref=in_b.at[came, side],
            dst_ref=in_b.at[came, side],
            send_sem=b_sent.at[0, 0],
            recv_sem=b_got.at[came, side],
            device_id=partner,
            device_id_type=MESH,
        ).wait_recv()

    def b_start(i):
        d = far_first(i, ny)
        b_copy(d, True).start()
        b_copy(d, False).start()

    tokens.loop(1, ny, b_start)
    b_copy(0, False).start()
    own_b = pltpu.make_async_copy(out_b.at[y, tp], in_b.at[y, tp], local.at[11])
    own_b.start()

    lane = iota((128, 2 * key_size + 2 * value_size), 0)
    column = iota((128, 2 * key_size + 2 * value_size), 1)
    for j in range(ny):
        goal = jnp.where(
            lane < kc,
            kc * j + lane,
            jnp.where(
                lane < 2 * kc,
                key_size + kc * j + lane - kc,
                jnp.where(
                    lane < 2 * kc + vc,
                    2 * key_size + vc * j + lane - 2 * kc,
                    2 * key_size + value_size + vc * j + lane - 2 * kc - vc,
                ),
            ),
        )
        hit = (goal == column) & (lane < span)
        place[pl.ds(128 * j, 128)] = jnp.where(hit, 1.0, 0.0).astype(BF16)
    own_b.wait()
    b_wait(0, False)

    def b_take(d):
        b_wait(d, True)
        b_wait(d, False)

    tokens.loop(1, ny, b_take)

    packed = jnp.concatenate([in_b[j].reshape(count, 128) for j in range(ny)], axis=1)
    fields = jnp.dot(packed, place[...], preferred_element_type=F32)
    query = fields[:, :key_size]
    key = fields[:, key_size : 2 * key_size]
    value = fields[:, 2 * key_size : 2 * key_size + value_size]
    gate = fields[:, 2 * key_size + value_size :]
    half = key_size // 2

    def turned_by(x):
        swapped = jnp.concatenate([x[:, half:], x[:, :half]], axis=1)
        return x * cosine + swapped * sine

    query_rot = turned_by(query).astype(BF16)
    key_f = turned_by(key) * key_size ** (-0.5)
    key_rot = key_f.astype(BF16)
    value_b = value.astype(BF16)
    scores = lax.dot_general(
        query_rot, key_rot, (((1,), (1,)), ((), ())), preferred_element_type=F32
    )
    inner = jnp.dot((scores * grid).astype(BF16), value_b, preferred_element_type=F32)
    decayed = query_rot.astype(F32) * query_decay
    row_at = at_of(iota((count, 1), 0))
    spread = jnp.concatenate(
        [jnp.where(row_at == at, decayed, 0.0).astype(BF16) for at in range(2 * heads)], axis=1
    )
    states = state_b[...].reshape(2 * heads * key_size, value_size)
    heads_out = inner + jnp.dot(spread, states, preferred_element_type=F32)
    normed = heads_out * lax.rsqrt(jnp.mean(heads_out * heads_out, axis=-1, keepdims=True) + epsilon)
    product = gate / (1.0 + jnp.exp(-gate)) * normed
    for c in range(value_size // 128):
        rows_f[c] = product[:, 128 * c : 128 * (c + 1)]
    for i in range(8):
        prop, seq = 2 * (i // 4) + i % 2, (i // 2) % 2
        keys_out[seq, prop] = key_f[i * heads : (i + 1) * heads].astype(BF16)
        values_out[seq, prop] = value[i * heads : (i + 1) * heads].astype(BF16)
    cut = heads * value_size // 2
    for h in range(heads):
        part, at = divmod(h * value_size, cut)
        for c in range(value_size // 128):
            piece = rows_f[c, pl.ds(h, 8, stride=heads), :]
            chunk[part, :, at + 128 * c : at + 128 * (c + 1)] = piece.astype(BF16)

    first = ((y, ny, "kv_1"), (z, nz, "kv_0"))
    second = ((z, nz, "kv_0"), (y, ny, "kv_1"))

    def g_copy(p, d):
        f, n, axis = first[p]
        return pltpu.make_async_remote_copy(
            src_ref=chunk.at[p],
            dst_ref=gated_all.at[p, f],
            send_sem=g_sent.at[p, d],
            recv_sem=g_got.at[p, f],
            device_id={axis: wrap(f + d, n)},
            device_id_type=MESH,
        )

    def g_start(i):
        for p in range(2):
            g_copy(p, far_first(i, first[p][1])).start()

    tokens.loop(1, ny, g_start)
    for p in range(2):
        f = first[p][0]
        pltpu.make_async_copy(chunk.at[p], gated_all.at[p, f], g_got.at[p, f]).start()

    source = iota((4 * seqs, seqs), 0)
    target = iota((4 * seqs, seqs), 1)
    low_ring, high_ring = (source >> 3) & (ny - 1), source >> (2 + ny.bit_length())
    for part, group in enumerate((high_ring * ny + low_ring, low_ring * ny + high_ring)):
        row_seq = 2 * group + ((source >> 1) & 1)
        row_prop = 2 * ((source >> 2) & 1) + (source & 1)
        for p in range(4):
            hit = (row_seq == target) & (row_prop == p)
            order[part, :, pl.ds(seqs * p, seqs)] = jnp.where(hit, 1.0, 0.0).astype(BF16)
    ring.all_here()

    def c_copy(p, d, same):
        s, n, axis = second[p]
        to = wrap(s + d, n)
        side = tp if same else 1 - tp
        return pltpu.make_async_remote_copy(
            src_ref=out_c.at[p, to, side],
            dst_ref=in_c.at[p, tp, s],
            send_sem=c_sent.at[p, d, side],
            recv_sem=c_got.at[p, tp, s],
            device_id={axis: to, "tp": side},
            device_id_type=MESH,
        )

    def wait_for(block, arrived):
        pltpu.make_async_remote_copy(
            src_ref=block,
            dst_ref=block,
            send_sem=a_sent.at[0],
            recv_sem=arrived,
            device_id=partner,
            device_id_type=MESH,
        ).wait_recv()

    out_cols = wo.shape[0]
    for p in range(2):
        n = first[p][1]
        tokens.loop(0, n, lambda f, p=p: wait_for(gated_all.at[p, f], g_got.at[p, f]))
        product = lax.dot_general(
            wo_all[p].reshape(second[p][1] * out_cols, cut),
            gated_all[p].reshape(n * 8, cut),
            (((1,), (1,)), ((), ())),
            preferred_element_type=F32,
        )
        part = out_cols // 2
        for to in range(second[p][1]):
            for side in range(2):
                at = to * out_cols + side * part
                halves = [product[at + e : at + e + part // 2] for e in (0, part // 2)]
                out_c[p, to, side] = jnp.concatenate(halves, axis=1).astype(BF16)

        def c_start(i, p=p, n=n):
            d = far_first(i, n)
            c_copy(p, d, True).start()
            c_copy(p, d, False).start()

        tokens.loop(1, n, c_start)
        c_copy(p, 0, False).start()
        s = second[p][0]
        pltpu.make_async_copy(
            out_c.at[p, s, tp], in_c.at[p, tp, s], c_got.at[p, tp, s]
        ).start()
    result = jnp.zeros((out_cols // 2, 4 * seqs), F32)
    for p in range(2):
        n = second[p][1]
        for side in range(2):
            tokens.loop(
                0, n, lambda s, p=p, side=side: wait_for(in_c.at[p, side, s], c_got.at[p, side, s])
            )
        sums = []
        for side in range(2):
            pairs = [[in_c[p, side, 2 * j + e].astype(F32) for e in range(2)] for j in range(n // 2)]
            for cut_at in (slice(0, 64), slice(64, 128)):
                sums.append(
                    jnp.concatenate([each[:, cut_at] for pair in pairs for each in pair], axis=1)
                )
        sums = jnp.concatenate(sums, axis=0).astype(BF16)
        moved = jnp.dot(sums, order[p], preferred_element_type=F32)
        result += moved[: out_cols // 2] + moved[out_cols // 2 :]
    result = result.astype(BF16)
    for p in range(4):
        ret_out[p] = result[:, p * seqs : (p + 1) * seqs]
    tokens.finish()
    ring.finish()

    def late_done(d):
        for p in range(2):
            g_copy(p, d).wait_send()
            for same in (True, False):
                c_copy(p, d, same).wait_send()

    tokens.loop(1, ny, late_done)
    for p in range(2):
        c_copy(p, 0, False).wait_send()
    tokens.loop(1, nz, lambda d: a_copy(d).wait_send())

    def b_done(d):
        b_copy(d, True).wait_send()
        b_copy(d, False).wait_send()

    tokens.loop(1, ny, b_done)
    b_copy(0, False).wait_send()


def in_hbm(value):
    return pltpu.with_memory_space_constraint(value, pltpu.HBM)


def put_kernel(*refs):
    count = (len(refs) - 1) // 2
    sems = refs[-1]
    copies = [
        pltpu.make_async_copy(refs[i], refs[count + i], sems.at[i]) for i in range(count)
    ]
    for copy in copies:
        copy.start()
    for copy in copies:
        copy.wait()


def put_out(*values):
    return pl.pallas_call(
        put_kernel,
        out_shape=tuple(jax.ShapeDtypeStruct(v.shape, v.dtype) for v in values),
        in_specs=[pl.BlockSpec(memory_space=pl.ANY)] * len(values),
        out_specs=(pl.BlockSpec(memory_space=pltpu.HBM),) * len(values),
        scratch_shapes=[pltpu.SemaphoreType.DMA((len(values),))],
        compiler_params=pltpu.CompilerParams(vmem_limit_bytes=8 * 1024 * 1024),
    )(*values)


def shards(
    nx,
    nz,
    ny,
    tokens,
    norm_gain,
    query_weight,
    key_weight,
    value_weight,
    gate_weight,
    out_weight,
    decay_rate,
    prior_state,
    last_keys,
    last_values,
    accepted,
    lengths,
):
    _, heads, key_size, value_size = prior_state.shape
    seqs, _, depth = tokens.shape
    width = norm_gain.shape[0]
    kc, vc = query_weight.shape[1], value_weight.shape[1]
    span = 2 * kc + 2 * vc
    count = 8 * heads
    half = key_size // 2
    frequency = jnp.power(10000.0, -jnp.arange(half, dtype=F32) / half)
    frequency = jnp.concatenate([frequency, frequency])[None, :]

    hbm = pl.BlockSpec(memory_space=pltpu.HBM)
    vmem = pl.BlockSpec(memory_space=pltpu.VMEM)
    dma = pltpu.SemaphoreType.DMA
    cut = heads * value_size // 2
    out_cols = out_weight.shape[1]
    retained, state, new_keys, new_values = pl.pallas_call(
        functools.partial(kernel, nx, nz, ny),
        out_shape=(
            jax.ShapeDtypeStruct((4, out_cols // 2, seqs), BF16),
            jax.ShapeDtypeStruct((2 * heads, key_size, value_size), F32),
            jax.ShapeDtypeStruct((2, 4, heads, key_size), BF16),
            jax.ShapeDtypeStruct((2, 4, heads, value_size), BF16),
        ),
        in_specs=[hbm] * 13 + [vmem],
        out_specs=(vmem,) * 4,
        scratch_shapes=[
            pltpu.VMEM((2, depth, seqs), BF16),
            pltpu.VMEM((2, span, width), BF16),
            pltpu.VMEM((2, nz, out_cols, cut), BF16),
            pltpu.VMEM((2 * heads, key_size, value_size), F32),
            pltpu.VMEM((2, 4 * heads, key_size), BF16),
            pltpu.VMEM((2, 4 * heads, value_size), BF16),
            pltpu.SMEM((heads,), F32),
            pltpu.SMEM((2,), jnp.int32),
            pltpu.SMEM((2,), jnp.int32),
            pltpu.VMEM((width,), BF16),
            pltpu.VMEM((1, width), F32),
            pltpu.VMEM((2, 2, 4 * heads, key_size), F32),
            pltpu.VMEM((2 * heads, key_size, value_size), BF16),
            pltpu.VMEM((2, nz, ny, depth, seqs), BF16),
            pltpu.VMEM((128 * ny, 2 * key_size + 2 * value_size), BF16),
            pltpu.VMEM((2, 4 * seqs, 4 * seqs), BF16),
            pltpu.VMEM((nz, 2, 2, 2 * ny, 128), BF16),
            pltpu.VMEM((nz, 2, 2, 2 * ny, 128), BF16),
            pltpu.VMEM((nz * 8 * ny, 128), F32),
            pltpu.VMEM((ny, 2, 2, 2 * nz, 128), BF16),
            pltpu.VMEM((ny, 2, 2, 2 * nz, 128), BF16),
            pltpu.VMEM((value_size // 128, count, 128), F32),
            pltpu.VMEM((2, 8, cut), BF16),
            pltpu.VMEM((2, nz, 8, cut), BF16),
            pltpu.VMEM((2, nz, 2, out_cols // 4, 128), BF16),
            pltpu.VMEM((2, 2, nz, out_cols // 4, 128), BF16),
            dma((23,)),
            dma((2, nz, ny)),
            dma((2, max(nz, ny), TorusGather.groups)),
            dma((2, max(nz, ny))),
            dma((2, 2, nz // 2, TorusGather.groups)),
            dma((2, nz)),
            dma((2, 2, nz // 2)),
            dma((2, 2, nz)),
            dma((2, 2, nz)),
            dma((2,)),
            dma((2,)),
            dma((2, nz)),
            dma((2, nz)),
            dma((2, nz, 2)),
            dma((2, 2, nz)),
            dma((4,)),
            dma((nz,)),
            dma((nz,)),
            dma((ny, 2)),
            dma((ny, 2)),
        ],
        compiler_params=pltpu.CompilerParams(
            collective_id=0, has_side_effects=True, vmem_limit_bytes=48 * 1024 * 1024
        ),
    )(
        *map(
            in_hbm,
            (
                tokens.transpose(1, 2, 0),
                query_weight.T,
                key_weight.T,
                value_weight.T,
                gate_weight.T,
                out_weight.T,
                prior_state.reshape(2 * heads, key_size, value_size),
                last_keys.reshape(2, 4 * heads, key_size),
                last_values.reshape(2, 4 * heads, value_size),
                decay_rate,
                accepted,
                lengths,
                norm_gain,
            ),
        ),
        frequency,
    )
    retained, state, new_keys, new_values = put_out(retained, state, new_keys, new_values)
    return (
        retained.transpose(2, 0, 1),
        state.reshape(prior_state.shape),
        new_keys,
        new_values,
    )


def solution(mesh):
    nz = ny = 8
    finer = Mesh(
        mesh.devices.reshape(mesh.shape["dp"], nz, ny, mesh.shape["tp"]),
        ("dp", "kv_0", "kv_1", "tp"),
    )
    return jax.shard_map(
        functools.partial(shards, mesh.shape["dp"], nz, ny),
        mesh=finer,
        in_specs=(
            P("dp", None, KV),
            P(),
            P(None, TP_KV),
            P(None, TP_KV),
            P(None, TP_KV),
            P(None, TP_KV),
            P("tp", KV),
            P("tp"),
            P(DP_KV, "tp", None, None),
            P(DP_KV, None, "tp", None),
            P(DP_KV, None, "tp", None),
            P(DP_KV),
            P(DP_KV),
        ),
        out_specs=(
            P("dp", None, KV_TP),
            P(DP_KV, "tp", None, None),
            P(DP_KV, None, "tp", None),
            P(DP_KV, None, "tp", None),
        ),
        check_vma=False,
    )
```

```python
import functools

import jax
import jax.numpy as jnp
from jax import lax
from jax.experimental import pallas as pl
from jax.experimental.pallas import tpu as pltpu
from jax.sharding import Mesh
from jax.sharding import PartitionSpec as P

KV = ("kv_0", "kv_1")
TP_KV = ("tp", "kv_0", "kv_1")
DP_KV = ("dp", "kv_0", "kv_1")
KV_TP = ("kv_0", "kv_1", "tp")
MESH = pl.DeviceIdType.MESH
F32, BF16 = jnp.float32, jnp.bfloat16

epsilon = 1e-06


def wrap(i, n):
    return i & (n - 1)


def far_first(i, n):
    return wrap(n // 2 + (1 - 2 * (i & 1)) * (i >> 1), n)


def near_first(i, n):
    odd = i & 1
    return wrap(odd * ((i + 1) >> 1) + (1 - odd) * (n - (i >> 1)), n)


class TorusGather:
    groups = 8
    turn = (0, 1, 7, 2, 6, 3, 5, 4)

    def __init__(self, own, held, arrived, ring_arrived, first_sent, ring_sent, nz, ny):
        self.own, self.held, self.arrived, self.ring_arrived = own, held, arrived, ring_arrived
        self.first_sent, self.ring_sent = first_sent, ring_sent
        z, y = lax.axis_index("kv_0"), lax.axis_index("kv_1")
        self.partner = {"tp": 1 - lax.axis_index("tp")}
        self.first = ((y, ny, "kv_1"), (z, nz, "kv_0"))
        self.second = ((z, nz, "kv_0"), (y, ny, "kv_1"))
        self.hops = nz // 2
        self.size = ny // self.groups

    def at(self, ref, p, f, s):
        return ref.at[p, s, f] if p == 0 else ref.at[p, f, s]

    def copy(self, target, source, sent, arrived, device):
        return pltpu.make_async_remote_copy(
            src_ref=source,
            dst_ref=target,
            send_sem=sent,
            recv_sem=arrived,
            device_id=device,
            device_id_type=MESH,
        )

    def first_copy(self, p, d):
        (f, n, axis), (s, _, _) = self.first[p], self.second[p]
        return self.copy(
            self.at(self.held, p, f, s),
            self.own(p),
            self.first_sent.at[p, d],
            self.at(self.arrived, p, f, s),
            {axis: wrap(f + d, n)},
        )

    def start_first(self):
        def send(i):
            for p in range(2):
                self.first_copy(p, near_first(i, self.first[p][1])).start()

        self.loop(1, self.first[0][1], send)
        for p in range(2):
            (f, _, _), (s, _, _) = self.first[p], self.second[p]
            pltpu.make_async_copy(
                self.own(p), self.at(self.held, p, f, s), self.at(self.arrived, p, f, s)
            ).start()

    def group(self, p, i):
        f = self.first[p][0]
        return wrap(f // self.size + self.turn[i], self.groups)

    def group_at(self, p, q, s):
        return self.at(self.held, p, pl.ds(q * self.size, self.size), s)

    def ring_copy(self, p, k, i, way, reach=1):
        s, n, axis = self.second[p]
        q, origin = self.group(p, i), wrap(s - way * k + n, n)
        block = self.group_at(p, q, origin)
        return self.copy(
            block,
            block,
            self.ring_sent.at[p, (1 + way) // 2, k + reach - 1, i],
            self.ring_arrived.at[p, origin, q],
            {axis: wrap(s + reach * way + n, n)},
        )

    def wait_chunk(self, p, f, s):
        chunk = self.at(self.held, p, f, s)
        self.copy(
            chunk, chunk, self.first_sent.at[0, 0], self.at(self.arrived, p, f, s), self.partner
        ).wait_recv()

    def wait_group(self, p, i, s):
        q = self.group(p, i)
        block = self.group_at(p, q, s)
        self.copy(
            block, block, self.first_sent.at[0, 0], self.ring_arrived.at[p, s, q], self.partner
        ).wait_recv()

    def pass_on(self, k, i, ways):
        for p in range(2):
            s, n, _ = self.second[p]
            if k == 0:
                for e in range(self.size):
                    self.wait_chunk(p, self.group(p, i) * self.size + e, s)
                for way in ways:
                    self.ring_copy(p, k, i, way).start()
            else:
                for way in (1, -1):
                    self.wait_group(p, i, wrap(s - way * k + n, n))
                    if k == self.hops - 2 and way == self.far_way(i):
                        self.ring_copy(p, k, i, way, 2).start()
                    if way in ways:
                        self.ring_copy(p, k, i, way).start()

    def loop(self, low, high, step):
        def body(i, _):
            step(i)
            return 0

        lax.fori_loop(low, high, body, 0)

    def ways(self, k, i):
        return (1, -1) if k < self.hops - 1 else ()

    def far_way(self, i):
        return 1 if i % 2 else -1

    def steps(self):
        lag = self.groups // 2
        every = [(k, i) for k in range(self.hops) for i in range(self.groups)]
        return sorted(every, key=lambda at: (at[1] + lag * at[0], at[0]))

    def last_arrivals(self):
        for i in range(self.groups):
            for p in range(2):
                s, n, _ = self.second[p]
                self.wait_group(p, i, wrap(s + self.hops, n))

    def finish(self):
        def first_done(d):
            for p in range(2):
                self.first_copy(p, d).wait_send()

        self.loop(1, self.first[0][1], first_done)
        for k in range(self.hops):
            for i in range(self.groups):
                for p in range(2):
                    for way in self.ways(k, i):
                        self.ring_copy(p, k, i, way).wait_send()
                    if k == self.hops - 2:
                        self.ring_copy(p, k, i, self.far_way(i), 2).wait_send()


class WeightRing:
    def __init__(self, held, arrived, sent, side_arrived, side_sent, on_arrived, on_sent, nx, nz, ny):
        self.held, self.arrived, self.sent = held, arrived, sent
        self.side_arrived, self.side_sent = side_arrived, side_sent
        self.on_arrived, self.on_sent = on_arrived, on_sent
        self.x, self.nx = lax.axis_index("dp"), nx
        z, y = lax.axis_index("kv_0"), lax.axis_index("kv_1")
        self.partner = {"tp": 1 - lax.axis_index("tp")}
        self.second = ((z, nz, "kv_0"), (y, ny, "kv_1"))
        self.hops = nz // 2
        self.rows = held.shape[2] // nx

    def block(self, p, origin, x):
        return self.held.at[p, origin, pl.ds(pl.multiple_of(self.rows * x, self.rows), self.rows)]

    def copy(self, block, sent, arrived, device):
        return pltpu.make_async_remote_copy(
            src_ref=block,
            dst_ref=block,
            send_sem=sent,
            recv_sem=arrived,
            device_id=device,
            device_id_type=MESH,
        )

    def ring_copy(self, p, k, way, reach=1):
        s, n, axis = self.second[p]
        origin = wrap(s - way * k + n, n)
        return self.copy(
            self.block(p, origin, self.x),
            self.sent.at[p, (1 + way) // 2, k + reach - 1],
            self.arrived.at[p, origin],
            {axis: wrap(s + reach * way + n, n)},
        )

    def side_copy(self, p, origin, way):
        at = (1 + way) // 2
        return self.copy(
            self.block(p, origin, self.x),
            self.side_sent.at[p, at, origin],
            self.side_arrived.at[p, at, origin],
            {"dp": wrap(self.x + way + self.nx, self.nx)},
        )

    def on_way(self, p):
        return 1 - 2 * p

    def on_copy(self, p):
        way = self.on_way(p)
        x = wrap(self.x - way + self.nx, self.nx)
        block = self.held.at[p, :, pl.ds(pl.multiple_of(self.rows * x, self.rows), self.rows)]
        return self.copy(
            block,
            self.on_sent.at[p],
            self.on_arrived.at[p],
            {"dp": wrap(self.x + way + self.nx, self.nx)},
        )

    def forward_ways(self, p, k):
        return (1, -1) if k < self.hops - 1 else ()

    def step(self, k):
        for p in range(2):
            s, n, _ = self.second[p]
            for way in (1,) if k in (0, self.hops) else (1, -1):
                origin = wrap(s - way * k + n, n)
                if k > 0:
                    self.copy(
                        self.block(p, origin, self.x),
                        self.sent.at[0, 0, 0],
                        self.arrived.at[p, origin],
                        self.partner,
                    ).wait_recv()
                ways = self.forward_ways(p, k)
                for to in ways if k == 0 else (way,):
                    if to in ways:
                        self.ring_copy(p, k, to).start()
                        if k == self.hops - 2 and to == self.on_way(p):
                            self.ring_copy(p, k, to, 2).start()
                for to in (1, -1):
                    self.side_copy(p, origin, to).start()

    def side_wait(self, p, way):
        x = wrap(self.x - way + self.nx, self.nx)

        def take(origin, _):
            self.copy(
                self.block(p, origin, x),
                self.sent.at[0, 0, 0],
                self.side_arrived.at[p, (1 + way) // 2, origin],
                self.partner,
            ).wait_recv()
            return 0

        lax.fori_loop(0, self.second[p][1], take, 0)

    def share_on(self):
        for p in range(2):
            self.side_wait(p, self.on_way(p))
            self.on_copy(p).start()

    def all_here(self):
        for p in range(2):
            self.side_wait(p, -self.on_way(p))
            self.on_copy(p).wait_recv()

    def finish(self):
        for p in range(2):
            for k in range(self.hops):
                for way in self.forward_ways(p, k):
                    self.ring_copy(p, k, way).wait_send()
            self.ring_copy(p, self.hops - 2, self.on_way(p), 2).wait_send()

            def done(origin, _, p=p):
                for way in (1, -1):
                    self.side_copy(p, origin, way).wait_send()
                return 0

            lax.fori_loop(0, self.second[p][1], done, 0)
            self.on_copy(p).wait_send()


def iota(shape, dim):
    return lax.broadcasted_iota(jnp.int32, shape, dim)


def kernel(
    nx,
    nz,
    ny,
    tok,
    wq,
    wk,
    wv,
    wg,
    wo,
    prior,
    last_k_in,
    last_v_in,
    decay_in,
    accepted_in,
    lengths_in,
    gain_in,
    frequency,
    ret_out,
    state_out,
    keys_out,
    values_out,
    tok_v,
    weights,
    wo_all,
    prior_v,
    last_k,
    last_v,
    decay,
    accepted,
    lengths,
    gain_v,
    gain,
    weighted_keys,
    state_b,
    tokens_all,
    place,
    order,
    out_a,
    in_a,
    mid,
    out_b,
    in_b,
    rows_f,
    chunk,
    gated_all,
    out_c,
    in_c,
    local,
    tok_arrived,
    tok_passed,
    tok_first,
    tok_ring,
    wo_arrived,
    wo_sent,
    wo_side,
    wo_side_sent,
    wo_on,
    wo_on_sent,
    g_sent,
    g_got,
    c_sent,
    c_got,
    pair_sems,
    a_sent,
    a_got,
    b_sent,
    b_got,
):
    x, z, y, tp = (lax.axis_index(axis) for axis in ("dp", "kv_0", "kv_1", "tp"))
    heads, seqs = nz, 2 * nz * ny
    kc = wq.shape[0]
    vc = wv.shape[0]
    span = 2 * kc + 2 * vc
    depth = tok_v.shape[1]
    width = nz * ny * depth
    partner = {"tp": 1 - tp}

    loads = [
        pltpu.make_async_copy(tok.at[pl.ds(2 * tp, 2)], tok_v, local.at[0]),
        pltpu.make_async_copy(wq, weights.at[tp, pl.ds(0, kc)], local.at[1]),
        pltpu.make_async_copy(wk, weights.at[tp, pl.ds(kc, kc)], local.at[2]),
        pltpu.make_async_copy(wv, weights.at[tp, pl.ds(2 * kc, vc)], local.at[3]),
        pltpu.make_async_copy(wg, weights.at[tp, pl.ds(2 * kc + vc, vc)], local.at[4]),
        pltpu.make_async_copy(prior, prior_v, local.at[5]),
    ]
    small_loads = [
        pltpu.make_async_copy(source, target, local.at[17 + i])
        for i, (source, target) in enumerate(
            (
                (last_k_in, last_k),
                (last_v_in, last_v),
                (decay_in, decay),
                (accepted_in, accepted),
                (lengths_in, lengths),
                (gain_in, gain_v),
            )
        )
    ]
    share = wo.shape[0] // nx
    mine = pl.ds(pl.multiple_of(share * x, share), share)
    half_k = wo.shape[1] // 2
    own_out = [
        pltpu.make_async_copy(
            wo.at[mine, pl.ds(p * half_k, half_k)], wo_all.at[p, (z, y)[p], mine], local.at[7 + p]
        )
        for p in range(2)
    ]
    for load in loads + own_out + small_loads:
        load.start()

    barrier = pltpu.get_barrier_semaphore()

    def greet(device):
        pl.semaphore_signal(barrier, inc=1, device_id=device, device_id_type=MESH)

    def greet_y(d, _):
        other = wrap(y + d, ny)
        greet({"kv_1": other})
        greet({"kv_1": other, "tp": 1 - tp})
        return 0

    def greet_z(d, _):
        greet({"kv_0": wrap(z + d, nz)})
        return 0

    lax.fori_loop(1, ny, greet_y, 0)
    lax.fori_loop(1, nz, greet_z, 0)
    def greet_tall(d, _):
        greet({"kv_0": wrap(z + d, nz), "tp": 1 - tp})
        return 0

    lax.fori_loop(1, nz, greet_tall, 0)
    greet(partner)
    for way in (1, nx - 1):
        greet({"dp": wrap(x + way, nx)})
    pl.semaphore_wait(barrier, 2 * (ny - 1) + 2 * (nz - 1) + 3)

    loads[0].wait()
    tokens = TorusGather(
        lambda p: tok_v.at[p], tokens_all, tok_arrived, tok_passed, tok_first, tok_ring, nz, ny
    )
    tokens.start_first()
    ring = WeightRing(
        wo_all, wo_arrived, wo_sent, wo_side, wo_side_sent, wo_on, wo_on_sent, nx, nz, ny
    )
    for load in own_out:
        load.wait()
    ring.step(0)
    for load in loads[1:5]:
        load.wait()
    swap = pltpu.make_async_remote_copy(
        src_ref=weights.at[tp],
        dst_ref=weights.at[tp],
        send_sem=pair_sems.at[0],
        recv_sem=pair_sems.at[1],
        device_id=partner,
        device_id_type=MESH,
    )
    swap.start()

    key_size, value_size = ny * kc, ny * vc

    loads[5].wait()
    for load in small_loads:
        load.wait()
    rows, count = 4 * heads, 8 * heads
    head_of = iota((rows, 1), 0) & (heads - 1)

    def by_head(shape):
        head = iota(shape, 0) & (heads - 1)
        table = jnp.zeros(shape, F32)
        for h in range(heads):
            table = jnp.where(head == h, -decay[h], table)
        return table

    taken_decay = by_head((rows, 128))
    before = iota((rows, 128), 0) >> (heads.bit_length() - 1)
    for s in range(2):
        power = jnp.maximum(accepted[s] - 1 - before, 0).astype(F32)
        key_weights = jnp.where(before < accepted[s], jnp.exp(taken_decay * power), 0.0)
        weighted = last_k[s].astype(F32) * key_weights
        high = weighted.astype(BF16).astype(F32)
        weighted_keys[s, 0] = high
        weighted_keys[s, 1] = weighted - high

    def one_head(h):
        mine = head_of == h
        for s in range(2):
            both = jnp.concatenate(
                [jnp.where(mine, weighted_keys[s, part], 0.0) for part in range(2)], axis=0
            )
            values = jnp.concatenate([last_v[s], last_v[s]], axis=0)
            update = lax.dot_general(
                both.astype(BF16), values, (((0,), (0,)), ((), ())), preferred_element_type=F32
            )
            at = s * heads + h
            power = jnp.full((1, value_size), -decay[h] * accepted[s].astype(F32), F32)
            fresh = jnp.exp(power) * prior_v[at] + update
            state_out[at] = fresh
            state_b[at] = fresh.astype(BF16)

    blocks = span // 16

    def scale_rows(i):
        at = pl.ds(i * 16, 16)
        for side in range(2):
            weights[side, at] = (weights[side, at].astype(F32) * gain[...]).astype(BF16)

    def first_scale():
        swap.wait()
        gain[...] = gain_v[...].astype(F32).reshape(1, width)
        scale_rows(0)

    one_head(0)
    one_head(1)
    work = [functools.partial(one_head, h) for h in range(2, heads)]
    work += [first_scale] + [functools.partial(scale_rows, i) for i in range(1, blocks)]
    work = iter(work)

    def beside():
        piece = next(work, None)
        if piece is not None:
            piece()

    for k, i in tokens.steps():
        if k > 0 and i == 0:
            ring.step(k)
        tokens.pass_on(k, i, tokens.ways(k, i))
        beside()
    ring.step(tokens.hops)
    tokens.last_arrivals()

    for p in range(2):
        total = jnp.zeros((2 * span, seqs), F32)
        squares = jnp.zeros((1, seqs), F32)
        for c in range(nz):
            block = tokens_all[p, c].reshape(ny * depth, seqs)
            cut = pl.ds(c * ny * depth, ny * depth)
            total += jnp.dot(
                weights[:, :, cut].reshape(2 * span, ny * depth), block, preferred_element_type=F32
            )
            floats = block.astype(F32)
            squares += jnp.sum(floats * floats, axis=0, keepdims=True)
        scaled = total * lax.rsqrt(squares / width + epsilon)
        for side in range(2):
            part = jnp.concatenate(
                [scaled[side * span : (side + 1) * span], jnp.zeros((128 - span, seqs), F32)], axis=0
            )
            turned = part.T.astype(BF16)
            for to in range(nz):
                out_a[to, side, p] = turned[2 * ny * to : 2 * ny * (to + 1)]

    def a_copy(d):
        to = wrap(z + d, nz)
        return pltpu.make_async_remote_copy(
            src_ref=out_a.at[to],
            dst_ref=in_a.at[z],
            send_sem=a_sent.at[d],
            recv_sem=a_got.at[z],
            device_id={"kv_0": to},
            device_id_type=MESH,
        )

    def a_wait(d):
        came = wrap(z + d, nz)
        pltpu.make_async_remote_copy(
            src_ref=in_a.at[came],
            dst_ref=in_a.at[came],
            send_sem=a_sent.at[0],
            recv_sem=a_got.at[came],
            device_id=partner,
            device_id_type=MESH,
        ).wait_recv()

    tokens.loop(1, nz, lambda i: a_copy(far_first(i, nz)).start())
    own_a = pltpu.make_async_copy(out_a.at[z], in_a.at[z], local.at[10])
    own_a.start()
    ring.share_on()

    shift = heads.bit_length() - 1

    def prop_of(i):
        return 2 * (i >> (shift + 2)) + ((i >> shift) & 1)

    def at_of(i):
        return ((i >> (shift + 1)) & 1) * heads + (i & (heads - 1))

    row = iota((count, 128), 0)
    first = jnp.where((row >> (shift + 1)) & 1 == 0, lengths[0] + accepted[0], lengths[1] + accepted[1])
    angles = (first + prop_of(row)).astype(F32) * frequency[...]
    cosine = jnp.cos(angles)
    lane_sign = jnp.where(iota((count, 128), 1) < key_size // 2, -1.0, 1.0)
    sine = jnp.sin(angles) * lane_sign
    decays = by_head((count, 128))
    query_decay = jnp.exp(decays * (prop_of(row) + 1).astype(F32))
    other = iota((count, count), 1)
    here = row[:, :count]
    offset = prop_of(here) - prop_of(other)
    grid = jnp.where(
        (at_of(here) == at_of(other)) & (offset >= 0),
        jnp.exp(decays[:, :count] * jnp.maximum(offset, 0).astype(F32)),
        0.0,
    )

    own_a.wait()
    tokens.loop(1, nz, a_wait)

    mid[...] = in_a[...].reshape(nz * 4 * 2 * ny, 128).astype(F32)
    stride = 4 * 2 * ny
    for to in range(ny):
        for side in range(2):
            for s in range(2):
                parts = [
                    mid[pl.ds(side * 4 * ny + p * 2 * ny + 2 * to + s, nz, stride=stride), :]
                    for p in range(2)
                ]
                out_b[to, side, s] = jnp.concatenate(parts, axis=0).astype(BF16)

    def b_copy(d, same):
        to = wrap(y + d, ny)
        side = tp if same else 1 - tp
        return pltpu.make_async_remote_copy(
            src_ref=out_b.at[to, side],
            dst_ref=in_b.at[y, tp],
            send_sem=b_sent.at[d, side],
            recv_sem=b_got.at[y, tp],
            device_id={"kv_1": to, "tp": side},
            device_id_type=MESH,
        )

    def b_wait(d, same):
        came = wrap(y + d, ny)
        side = tp if same else 1 - tp
        pltpu.make_async_remote_copy(
            src_ref=in_b.at[came, side],
            dst_ref=in_b.at[came, side],
            send_sem=b_sent.at[0, 0],
            recv_sem=b_got.at[came, side],
            device_id=partner,
            device_id_type=MESH,
        ).wait_recv()

    def b_start(i):
        d = far_first(i, ny)
        b_copy(d, True).start()
        b_copy(d, False).start()

    tokens.loop(1, ny, b_start)
    b_copy(0, False).start()
    own_b = pltpu.make_async_copy(out_b.at[y, tp], in_b.at[y, tp], local.at[11])
    own_b.start()

    lane = iota((128, 2 * key_size + 2 * value_size), 0)
    column = iota((128, 2 * key_size + 2 * value_size), 1)
    for j in range(ny):
        goal = jnp.where(
            lane < kc,
            kc * j + lane,
            jnp.where(
                lane < 2 * kc,
                key_size + kc * j + lane - kc,
                jnp.where(
                    lane < 2 * kc + vc,
                    2 * key_size + vc * j + lane - 2 * kc,
                    2 * key_size + value_size + vc * j + lane - 2 * kc - vc,
                ),
            ),
        )
        hit = (goal == column) & (lane < span)
        place[pl.ds(128 * j, 128)] = jnp.where(hit, 1.0, 0.0).astype(BF16)
    own_b.wait()
    b_wait(0, False)

    def b_take(d):
        b_wait(d, True)
        b_wait(d, False)

    tokens.loop(1, ny, b_take)

    packed = jnp.concatenate([in_b[j].reshape(count, 128) for j in range(ny)], axis=1)
    fields = jnp.dot(packed, place[...], preferred_element_type=F32)
    query = fields[:, :key_size]
    key = fields[:, key_size : 2 * key_size]
    value = fields[:, 2 * key_size : 2 * key_size + value_size]
    gate = fields[:, 2 * key_size + value_size :]
    half = key_size // 2

    def turned_by(x):
        swapped = jnp.concatenate([x[:, half:], x[:, :half]], axis=1)
        return x * cosine + swapped * sine

    query_rot = turned_by(query).astype(BF16)
    key_f = turned_by(key) * key_size ** (-0.5)
    key_rot = key_f.astype(BF16)
    value_b = value.astype(BF16)
    scores = lax.dot_general(
        query_rot, key_rot, (((1,), (1,)), ((), ())), preferred_element_type=F32
    )
    inner = jnp.dot((scores * grid).astype(BF16), value_b, preferred_element_type=F32)
    decayed = query_rot.astype(F32) * query_decay
    row_at = at_of(iota((count, 1), 0))
    spread = jnp.concatenate(
        [jnp.where(row_at == at, decayed, 0.0).astype(BF16) for at in range(2 * heads)], axis=1
    )
    states = state_b[...].reshape(2 * heads * key_size, value_size)
    heads_out = inner + jnp.dot(spread, states, preferred_element_type=F32)
    normed = heads_out * lax.rsqrt(jnp.mean(heads_out * heads_out, axis=-1, keepdims=True) + epsilon)
    product = gate / (1.0 + jnp.exp(-gate)) * normed
    for c in range(value_size // 128):
        rows_f[c] = product[:, 128 * c : 128 * (c + 1)]
    for i in range(8):
        prop, seq = 2 * (i // 4) + i % 2, (i // 2) % 2
        keys_out[seq, prop] = key_f[i * heads : (i + 1) * heads].astype(BF16)
        values_out[seq, prop] = value[i * heads : (i + 1) * heads].astype(BF16)
    cut = heads * value_size // 2
    for h in range(heads):
        part, at = divmod(h * value_size, cut)
        for c in range(value_size // 128):
            piece = rows_f[c, pl.ds(h, 8, stride=heads), :]
            chunk[part, :, at + 128 * c : at + 128 * (c + 1)] = piece.astype(BF16)

    first = ((y, ny, "kv_1"), (z, nz, "kv_0"))
    second = ((z, nz, "kv_0"), (y, ny, "kv_1"))

    def g_copy(p, d):
        f, n, axis = first[p]
        return pltpu.make_async_remote_copy(
            src_ref=chunk.at[p],
            dst_ref=gated_all.at[p, f],
            send_sem=g_sent.at[p, d],
            recv_sem=g_got.at[p, f],
            device_id={axis: wrap(f + d, n)},
            device_id_type=MESH,
        )

    def g_start(i):
        for p in range(2):
            g_copy(p, far_first(i, first[p][1])).start()

    tokens.loop(1, ny, g_start)
    for p in range(2):
        f = first[p][0]
        pltpu.make_async_copy(chunk.at[p], gated_all.at[p, f], g_got.at[p, f]).start()

    source = iota((4 * seqs, seqs), 0)
    target = iota((4 * seqs, seqs), 1)
    low_ring, high_ring = (source >> 3) & (ny - 1), source >> (2 + ny.bit_length())
    for part, group in enumerate((high_ring * ny + low_ring, low_ring * ny + high_ring)):
        row_seq = 2 * group + ((source >> 1) & 1)
        row_prop = 2 * ((source >> 2) & 1) + (source & 1)
        for p in range(4):
            hit = (row_seq == target) & (row_prop == p)
            order[part, :, pl.ds(seqs * p, seqs)] = jnp.where(hit, 1.0, 0.0).astype(BF16)
    ring.all_here()

    def c_copy(p, d, same):
        s, n, axis = second[p]
        to = wrap(s + d, n)
        side = tp if same else 1 - tp
        return pltpu.make_async_remote_copy(
            src_ref=out_c.at[p, to, side],
            dst_ref=in_c.at[p, tp, s],
            send_sem=c_sent.at[p, d, side],
            recv_sem=c_got.at[p, tp, s],
            device_id={axis: to, "tp": side},
            device_id_type=MESH,
        )

    def wait_for(block, arrived):
        pltpu.make_async_remote_copy(
            src_ref=block,
            dst_ref=block,
            send_sem=a_sent.at[0],
            recv_sem=arrived,
            device_id=partner,
            device_id_type=MESH,
        ).wait_recv()

    out_cols = wo.shape[0]
    for p in range(2):
        n = first[p][1]
        tokens.loop(0, n, lambda f, p=p: wait_for(gated_all.at[p, f], g_got.at[p, f]))
        product = lax.dot_general(
            wo_all[p].reshape(second[p][1] * out_cols, cut),
            gated_all[p].reshape(n * 8, cut),
            (((1,), (1,)), ((), ())),
            preferred_element_type=F32,
        )
        part = out_cols // 2
        for to in range(second[p][1]):
            for side in range(2):
                at = to * out_cols + side * part
                halves = [product[at + e : at + e + part // 2] for e in (0, part // 2)]
                out_c[p, to, side] = jnp.concatenate(halves, axis=1).astype(BF16)

        def c_start(i, p=p, n=n):
            d = far_first(i, n)
            c_copy(p, d, True).start()
            c_copy(p, d, False).start()

        tokens.loop(1, n, c_start)
        c_copy(p, 0, False).start()
        s = second[p][0]
        pltpu.make_async_copy(
            out_c.at[p, s, tp], in_c.at[p, tp, s], c_got.at[p, tp, s]
        ).start()
    result = jnp.zeros((out_cols // 2, 4 * seqs), F32)
    for p in range(2):
        n = second[p][1]
        for side in range(2):
            tokens.loop(
                0, n, lambda s, p=p, side=side: wait_for(in_c.at[p, side, s], c_got.at[p, side, s])
            )
        sums = []
        for side in range(2):
            pairs = [[in_c[p, side, 2 * j + e].astype(F32) for e in range(2)] for j in range(n // 2)]
            for cut_at in (slice(0, 64), slice(64, 128)):
                sums.append(
                    jnp.concatenate([each[:, cut_at] for pair in pairs for each in pair], axis=1)
                )
        sums = jnp.concatenate(sums, axis=0).astype(BF16)
        moved = jnp.dot(sums, order[p], preferred_element_type=F32)
        result += moved[: out_cols // 2] + moved[out_cols // 2 :]
    result = result.astype(BF16)
    for p in range(4):
        ret_out[p] = result[:, p * seqs : (p + 1) * seqs]
    tokens.finish()
    ring.finish()

    def late_done(d):
        for p in range(2):
            g_copy(p, d).wait_send()
            for same in (True, False):
                c_copy(p, d, same).wait_send()

    tokens.loop(1, ny, late_done)
    for p in range(2):
        c_copy(p, 0, False).wait_send()
    tokens.loop(1, nz, lambda d: a_copy(d).wait_send())

    def b_done(d):
        b_copy(d, True).wait_send()
        b_copy(d, False).wait_send()

    tokens.loop(1, ny, b_done)
    b_copy(0, False).wait_send()


def in_hbm(value):
    return pltpu.with_memory_space_constraint(value, pltpu.HBM)


def put_kernel(*refs):
    count = (len(refs) - 1) // 2
    sems = refs[-1]
    copies = [
        pltpu.make_async_copy(refs[i], refs[count + i], sems.at[i]) for i in range(count)
    ]
    for copy in copies:
        copy.start()
    for copy in copies:
        copy.wait()


def put_out(*values):
    return pl.pallas_call(
        put_kernel,
        out_shape=tuple(jax.ShapeDtypeStruct(v.shape, v.dtype) for v in values),
        in_specs=[pl.BlockSpec(memory_space=pl.ANY)] * len(values),
        out_specs=(pl.BlockSpec(memory_space=pltpu.HBM),) * len(values),
        scratch_shapes=[pltpu.SemaphoreType.DMA((len(values),))],
        compiler_params=pltpu.CompilerParams(vmem_limit_bytes=8 * 1024 * 1024),
    )(*values)


def shards(
    nx,
    nz,
    ny,
    tokens,
    norm_gain,
    query_weight,
    key_weight,
    value_weight,
    gate_weight,
    out_weight,
    decay_rate,
    prior_state,
    last_keys,
    last_values,
    accepted,
    lengths,
):
    _, heads, key_size, value_size = prior_state.shape
    seqs, _, depth = tokens.shape
    width = norm_gain.shape[0]
    kc, vc = query_weight.shape[1], value_weight.shape[1]
    span = 2 * kc + 2 * vc
    count = 8 * heads
    half = key_size // 2
    frequency = jnp.power(10000.0, -jnp.arange(half, dtype=F32) / half)
    frequency = jnp.concatenate([frequency, frequency])[None, :]

    hbm = pl.BlockSpec(memory_space=pltpu.HBM)
    vmem = pl.BlockSpec(memory_space=pltpu.VMEM)
    dma = pltpu.SemaphoreType.DMA
    cut = heads * value_size // 2
    out_cols = out_weight.shape[1]
    retained, state, new_keys, new_values = pl.pallas_call(
        functools.partial(kernel, nx, nz, ny),
        out_shape=(
            jax.ShapeDtypeStruct((4, out_cols // 2, seqs), BF16),
            jax.ShapeDtypeStruct((2 * heads, key_size, value_size), F32),
            jax.ShapeDtypeStruct((2, 4, heads, key_size), BF16),
            jax.ShapeDtypeStruct((2, 4, heads, value_size), BF16),
        ),
        in_specs=[hbm] * 13 + [vmem],
        out_specs=(vmem,) * 4,
        scratch_shapes=[
            pltpu.VMEM((2, depth, seqs), BF16),
            pltpu.VMEM((2, span, width), BF16),
            pltpu.VMEM((2, nz, out_cols, cut), BF16),
            pltpu.VMEM((2 * heads, key_size, value_size), F32),
            pltpu.VMEM((2, 4 * heads, key_size), BF16),
            pltpu.VMEM((2, 4 * heads, value_size), BF16),
            pltpu.SMEM((heads,), F32),
            pltpu.SMEM((2,), jnp.int32),
            pltpu.SMEM((2,), jnp.int32),
            pltpu.VMEM((width,), BF16),
            pltpu.VMEM((1, width), F32),
            pltpu.VMEM((2, 2, 4 * heads, key_size), F32),
            pltpu.VMEM((2 * heads, key_size, value_size), BF16),
            pltpu.VMEM((2, nz, ny, depth, seqs), BF16),
            pltpu.VMEM((128 * ny, 2 * key_size + 2 * value_size), BF16),
            pltpu.VMEM((2, 4 * seqs, 4 * seqs), BF16),
            pltpu.VMEM((nz, 2, 2, 2 * ny, 128), BF16),
            pltpu.VMEM((nz, 2, 2, 2 * ny, 128), BF16),
            pltpu.VMEM((nz * 8 * ny, 128), F32),
            pltpu.VMEM((ny, 2, 2, 2 * nz, 128), BF16),
            pltpu.VMEM((ny, 2, 2, 2 * nz, 128), BF16),
            pltpu.VMEM((value_size // 128, count, 128), F32),
            pltpu.VMEM((2, 8, cut), BF16),
            pltpu.VMEM((2, nz, 8, cut), BF16),
            pltpu.VMEM((2, nz, 2, out_cols // 4, 128), BF16),
            pltpu.VMEM((2, 2, nz, out_cols // 4, 128), BF16),
            dma((23,)),
            dma((2, nz, ny)),
            dma((2, max(nz, ny), TorusGather.groups)),
            dma((2, max(nz, ny))),
            dma((2, 2, nz // 2, TorusGather.groups)),
            dma((2, nz)),
            dma((2, 2, nz // 2)),
            dma((2, 2, nz)),
            dma((2, 2, nz)),
            dma((2,)),
            dma((2,)),
            dma((2, nz)),
            dma((2, nz)),
            dma((2, nz, 2)),
            dma((2, 2, nz)),
            dma((4,)),
            dma((nz,)),
            dma((nz,)),
            dma((ny, 2)),
            dma((ny, 2)),
        ],
        compiler_params=pltpu.CompilerParams(
            collective_id=0, has_side_effects=True, vmem_limit_bytes=48 * 1024 * 1024
        ),
    )(
        *map(
            in_hbm,
            (
                tokens.transpose(1, 2, 0),
                query_weight.T,
                key_weight.T,
                value_weight.T,
                gate_weight.T,
                out_weight.T,
                prior_state.reshape(2 * heads, key_size, value_size),
                last_keys.reshape(2, 4 * heads, key_size),
                last_values.reshape(2, 4 * heads, value_size),
                decay_rate,
                accepted,
                lengths,
                norm_gain,
            ),
        ),
        frequency,
    )
    retained, state, new_keys, new_values = put_out(retained, state, new_keys, new_values)
    return (
        retained.transpose(2, 0, 1),
        state.reshape(prior_state.shape),
        new_keys,
        new_values,
    )


def solution(mesh):
    nz = ny = 8
    finer = Mesh(
        mesh.devices.reshape(mesh.shape["dp"], nz, ny, mesh.shape["tp"]),
        ("dp", "kv_0", "kv_1", "tp"),
    )
    return jax.shard_map(
        functools.partial(shards, mesh.shape["dp"], nz, ny),
        mesh=finer,
        in_specs=(
            P("dp", None, KV),
            P(),
            P(None, TP_KV),
            P(None, TP_KV),
            P(None, TP_KV),
            P(None, TP_KV),
            P("tp", KV),
            P("tp"),
            P(DP_KV, "tp", None, None),
            P(DP_KV, None, "tp", None),
            P(DP_KV, None, "tp", None),
            P(DP_KV),
            P(DP_KV),
        ),
        out_specs=(
            P("dp", None, KV_TP),
            P(DP_KV, "tp", None, None),
            P(DP_KV, None, "tp", None),
            P(DP_KV, None, "tp", None),
        ),
        check_vma=False,
    )
```

```python
import functools

import jax
import jax.numpy as jnp
from jax import lax
from jax.experimental import pallas as pl
from jax.experimental.pallas import tpu as pltpu
from jax.sharding import Mesh
from jax.sharding import PartitionSpec as P

KV = ("kv_0", "kv_1")
TP_KV = ("tp", "kv_0", "kv_1")
DP_KV = ("dp", "kv_0", "kv_1")
KV_TP = ("kv_0", "kv_1", "tp")
MESH = pl.DeviceIdType.MESH
F32, BF16 = jnp.float32, jnp.bfloat16

epsilon = 1e-06


def wrap(i, n):
    return i & (n - 1)


def far_first(i, n):
    return wrap(n // 2 + (1 - 2 * (i & 1)) * (i >> 1), n)


def near_first(i, n):
    odd = i & 1
    return wrap(odd * ((i + 1) >> 1) + (1 - odd) * (n - (i >> 1)), n)


class TorusGather:
    groups = 8
    turn = (0, 1, 7, 2, 6, 3, 5, 4)

    def __init__(self, own, held, arrived, ring_arrived, first_sent, ring_sent, nz, ny):
        self.own, self.held, self.arrived, self.ring_arrived = own, held, arrived, ring_arrived
        self.first_sent, self.ring_sent = first_sent, ring_sent
        z, y = lax.axis_index("kv_0"), lax.axis_index("kv_1")
        self.partner = {"tp": 1 - lax.axis_index("tp")}
        self.first = ((y, ny, "kv_1"), (z, nz, "kv_0"))
        self.second = ((z, nz, "kv_0"), (y, ny, "kv_1"))
        self.hops = nz // 2
        self.size = ny // self.groups

    def at(self, ref, p, f, s):
        return ref.at[p, s, f] if p == 0 else ref.at[p, f, s]

    def copy(self, target, source, sent, arrived, device):
        return pltpu.make_async_remote_copy(
            src_ref=source,
            dst_ref=target,
            send_sem=sent,
            recv_sem=arrived,
            device_id=device,
            device_id_type=MESH,
        )

    def first_copy(self, p, d):
        (f, n, axis), (s, _, _) = self.first[p], self.second[p]
        return self.copy(
            self.at(self.held, p, f, s),
            self.own(p),
            self.first_sent.at[p, d],
            self.at(self.arrived, p, f, s),
            {axis: wrap(f + d, n)},
        )

    def start_first(self):
        def send(i):
            for p in range(2):
                self.first_copy(p, near_first(i, self.first[p][1])).start()

        self.loop(1, self.first[0][1], send)
        for p in range(2):
            (f, _, _), (s, _, _) = self.first[p], self.second[p]
            pltpu.make_async_copy(
                self.own(p), self.at(self.held, p, f, s), self.at(self.arrived, p, f, s)
            ).start()

    def group(self, p, i):
        f = self.first[p][0]
        return wrap(f // self.size + self.turn[i], self.groups)

    def group_at(self, p, q, s):
        return self.at(self.held, p, pl.ds(q * self.size, self.size), s)

    def ring_copy(self, p, k, i, way, reach=1):
        s, n, axis = self.second[p]
        q, origin = self.group(p, i), wrap(s - way * k + n, n)
        block = self.group_at(p, q, origin)
        return self.copy(
            block,
            block,
            self.ring_sent.at[p, (1 + way) // 2, k + reach - 1, i],
            self.ring_arrived.at[p, origin, q],
            {axis: wrap(s + reach * way + n, n)},
        )

    def wait_chunk(self, p, f, s):
        chunk = self.at(self.held, p, f, s)
        self.copy(
            chunk, chunk, self.first_sent.at[0, 0], self.at(self.arrived, p, f, s), self.partner
        ).wait_recv()

    def wait_group(self, p, i, s):
        q = self.group(p, i)
        block = self.group_at(p, q, s)
        self.copy(
            block, block, self.first_sent.at[0, 0], self.ring_arrived.at[p, s, q], self.partner
        ).wait_recv()

    def pass_on(self, k, i, ways):
        for p in range(2):
            s, n, _ = self.second[p]
            if k == 0:
                for e in range(self.size):
                    self.wait_chunk(p, self.group(p, i) * self.size + e, s)
                for way in ways:
                    self.ring_copy(p, k, i, way).start()
            else:
                for way in (1, -1):
                    self.wait_group(p, i, wrap(s - way * k + n, n))
                    if k == self.hops - 2 and way == self.far_way(i):
                        self.ring_copy(p, k, i, way, 2).start()
                    if way in ways:
                        self.ring_copy(p, k, i, way).start()

    def loop(self, low, high, step):
        def body(i, _):
            step(i)
            return 0

        lax.fori_loop(low, high, body, 0)

    def ways(self, k, i):
        return (1, -1) if k < self.hops - 1 else ()

    def far_way(self, i):
        return 1 if i % 2 else -1

    def round(self, k, beside=None):
        for i in range(self.groups):
            self.pass_on(k, i, self.ways(k, i))
            if beside is not None:
                beside()

    def last_arrivals(self):
        for i in range(self.groups):
            for p in range(2):
                s, n, _ = self.second[p]
                self.wait_group(p, i, wrap(s + self.hops, n))

    def finish(self):
        def first_done(d):
            for p in range(2):
                self.first_copy(p, d).wait_send()

        self.loop(1, self.first[0][1], first_done)
        for k in range(self.hops):
            for i in range(self.groups):
                for p in range(2):
                    for way in self.ways(k, i):
                        self.ring_copy(p, k, i, way).wait_send()
                    if k == self.hops - 2:
                        self.ring_copy(p, k, i, self.far_way(i), 2).wait_send()


class WeightRing:
    def __init__(self, held, arrived, sent, side_arrived, side_sent, on_arrived, on_sent, nx, nz, ny):
        self.held, self.arrived, self.sent = held, arrived, sent
        self.side_arrived, self.side_sent = side_arrived, side_sent
        self.on_arrived, self.on_sent = on_arrived, on_sent
        self.x, self.nx = lax.axis_index("dp"), nx
        z, y = lax.axis_index("kv_0"), lax.axis_index("kv_1")
        self.partner = {"tp": 1 - lax.axis_index("tp")}
        self.second = ((z, nz, "kv_0"), (y, ny, "kv_1"))
        self.hops = nz // 2
        self.rows = held.shape[2] // nx

    def block(self, p, origin, x):
        return self.held.at[p, origin, pl.ds(pl.multiple_of(self.rows * x, self.rows), self.rows)]

    def copy(self, block, sent, arrived, device):
        return pltpu.make_async_remote_copy(
            src_ref=block,
            dst_ref=block,
            send_sem=sent,
            recv_sem=arrived,
            device_id=device,
            device_id_type=MESH,
        )

    def ring_copy(self, p, k, way, reach=1):
        s, n, axis = self.second[p]
        origin = wrap(s - way * k + n, n)
        return self.copy(
            self.block(p, origin, self.x),
            self.sent.at[p, (1 + way) // 2, k + reach - 1],
            self.arrived.at[p, origin],
            {axis: wrap(s + reach * way + n, n)},
        )

    def side_copy(self, p, origin, way):
        at = (1 + way) // 2
        return self.copy(
            self.block(p, origin, self.x),
            self.side_sent.at[p, at, origin],
            self.side_arrived.at[p, at, origin],
            {"dp": wrap(self.x + way + self.nx, self.nx)},
        )

    def on_way(self, p):
        return 1 - 2 * p

    def on_copy(self, p):
        way = self.on_way(p)
        x = wrap(self.x - way + self.nx, self.nx)
        block = self.held.at[p, :, pl.ds(pl.multiple_of(self.rows * x, self.rows), self.rows)]
        return self.copy(
            block,
            self.on_sent.at[p],
            self.on_arrived.at[p],
            {"dp": wrap(self.x + way + self.nx, self.nx)},
        )

    def forward_ways(self, p, k):
        return (1, -1) if k < self.hops - 1 else ()

    def step(self, k):
        for p in range(2):
            s, n, _ = self.second[p]
            for way in (1,) if k in (0, self.hops) else (1, -1):
                origin = wrap(s - way * k + n, n)
                if k > 0:
                    self.copy(
                        self.block(p, origin, self.x),
                        self.sent.at[0, 0, 0],
                        self.arrived.at[p, origin],
                        self.partner,
                    ).wait_recv()
                ways = self.forward_ways(p, k)
                for to in ways if k == 0 else (way,):
                    if to in ways:
                        self.ring_copy(p, k, to).start()
                        if k == self.hops - 2 and to == self.on_way(p):
                            self.ring_copy(p, k, to, 2).start()
                for to in (1, -1):
                    self.side_copy(p, origin, to).start()

    def side_wait(self, p, way):
        x = wrap(self.x - way + self.nx, self.nx)

        def take(origin, _):
            self.copy(
                self.block(p, origin, x),
                self.sent.at[0, 0, 0],
                self.side_arrived.at[p, (1 + way) // 2, origin],
                self.partner,
            ).wait_recv()
            return 0

        lax.fori_loop(0, self.second[p][1], take, 0)

    def share_on(self):
        for p in range(2):
            self.side_wait(p, self.on_way(p))
            self.on_copy(p).start()

    def all_here(self):
        for p in range(2):
            self.side_wait(p, -self.on_way(p))
            self.on_copy(p).wait_recv()

    def finish(self):
        for p in range(2):
            for k in range(self.hops):
                for way in self.forward_ways(p, k):
                    self.ring_copy(p, k, way).wait_send()
            self.ring_copy(p, self.hops - 2, self.on_way(p), 2).wait_send()

            def done(origin, _, p=p):
                for way in (1, -1):
                    self.side_copy(p, origin, way).wait_send()
                return 0

            lax.fori_loop(0, self.second[p][1], done, 0)
            self.on_copy(p).wait_send()


def iota(shape, dim):
    return lax.broadcasted_iota(jnp.int32, shape, dim)


def kernel(
    nx,
    nz,
    ny,
    tok,
    wq,
    wk,
    wv,
    wg,
    wo,
    prior,
    last_k_in,
    last_v_in,
    decay_in,
    accepted_in,
    lengths_in,
    gain_in,
    frequency,
    ret_out,
    state_out,
    keys_out,
    values_out,
    tok_v,
    weights,
    wo_all,
    prior_v,
    last_k,
    last_v,
    decay,
    accepted,
    lengths,
    gain_v,
    gain,
    weighted_keys,
    state_b,
    tokens_all,
    place,
    order,
    out_a,
    in_a,
    mid,
    out_b,
    in_b,
    rows_f,
    chunk,
    gated_all,
    out_c,
    in_c,
    local,
    tok_arrived,
    tok_passed,
    tok_first,
    tok_ring,
    wo_arrived,
    wo_sent,
    wo_side,
    wo_side_sent,
    wo_on,
    wo_on_sent,
    g_sent,
    g_got,
    c_sent,
    c_got,
    pair_sems,
    a_sent,
    a_got,
    b_sent,
    b_got,
):
    x, z, y, tp = (lax.axis_index(axis) for axis in ("dp", "kv_0", "kv_1", "tp"))
    heads, seqs = nz, 2 * nz * ny
    kc = wq.shape[0]
    vc = wv.shape[0]
    span = 2 * kc + 2 * vc
    depth = tok_v.shape[1]
    width = nz * ny * depth
    partner = {"tp": 1 - tp}

    loads = [
        pltpu.make_async_copy(tok.at[pl.ds(2 * tp, 2)], tok_v, local.at[0]),
        pltpu.make_async_copy(wq, weights.at[tp, pl.ds(0, kc)], local.at[1]),
        pltpu.make_async_copy(wk, weights.at[tp, pl.ds(kc, kc)], local.at[2]),
        pltpu.make_async_copy(wv, weights.at[tp, pl.ds(2 * kc, vc)], local.at[3]),
        pltpu.make_async_copy(wg, weights.at[tp, pl.ds(2 * kc + vc, vc)], local.at[4]),
        pltpu.make_async_copy(prior, prior_v, local.at[5]),
    ]
    small_loads = [
        pltpu.make_async_copy(source, target, local.at[17 + i])
        for i, (source, target) in enumerate(
            (
                (last_k_in, last_k),
                (last_v_in, last_v),
                (decay_in, decay),
                (accepted_in, accepted),
                (lengths_in, lengths),
                (gain_in, gain_v),
            )
        )
    ]
    share = wo.shape[0] // nx
    mine = pl.ds(pl.multiple_of(share * x, share), share)
    half_k = wo.shape[1] // 2
    own_out = [
        pltpu.make_async_copy(
            wo.at[mine, pl.ds(p * half_k, half_k)], wo_all.at[p, (z, y)[p], mine], local.at[7 + p]
        )
        for p in range(2)
    ]
    for load in loads + own_out + small_loads:
        load.start()

    barrier = pltpu.get_barrier_semaphore()

    def greet(device):
        pl.semaphore_signal(barrier, inc=1, device_id=device, device_id_type=MESH)

    def greet_y(d, _):
        other = wrap(y + d, ny)
        greet({"kv_1": other})
        greet({"kv_1": other, "tp": 1 - tp})
        return 0

    def greet_z(d, _):
        greet({"kv_0": wrap(z + d, nz)})
        return 0

    lax.fori_loop(1, ny, greet_y, 0)
    lax.fori_loop(1, nz, greet_z, 0)
    def greet_tall(d, _):
        greet({"kv_0": wrap(z + d, nz), "tp": 1 - tp})
        return 0

    lax.fori_loop(1, nz, greet_tall, 0)
    greet(partner)
    for way in (1, nx - 1):
        greet({"dp": wrap(x + way, nx)})
    pl.semaphore_wait(barrier, 2 * (ny - 1) + 2 * (nz - 1) + 3)

    loads[0].wait()
    tokens = TorusGather(
        lambda p: tok_v.at[p], tokens_all, tok_arrived, tok_passed, tok_first, tok_ring, nz, ny
    )
    tokens.start_first()
    ring = WeightRing(
        wo_all, wo_arrived, wo_sent, wo_side, wo_side_sent, wo_on, wo_on_sent, nx, nz, ny
    )
    for load in own_out:
        load.wait()
    ring.step(0)
    for load in loads[1:5]:
        load.wait()
    swap = pltpu.make_async_remote_copy(
        src_ref=weights.at[tp],
        dst_ref=weights.at[tp],
        send_sem=pair_sems.at[0],
        recv_sem=pair_sems.at[1],
        device_id=partner,
        device_id_type=MESH,
    )
    swap.start()

    key_size, value_size = ny * kc, ny * vc

    loads[5].wait()
    for load in small_loads:
        load.wait()
    rows, count = 4 * heads, 8 * heads
    head_of = iota((rows, 1), 0) & (heads - 1)

    def by_head(shape):
        head = iota(shape, 0) & (heads - 1)
        table = jnp.zeros(shape, F32)
        for h in range(heads):
            table = jnp.where(head == h, -decay[h], table)
        return table

    taken_decay = by_head((rows, 128))
    before = iota((rows, 128), 0) >> (heads.bit_length() - 1)
    for s in range(2):
        power = jnp.maximum(accepted[s] - 1 - before, 0).astype(F32)
        key_weights = jnp.where(before < accepted[s], jnp.exp(taken_decay * power), 0.0)
        weighted = last_k[s].astype(F32) * key_weights
        high = weighted.astype(BF16).astype(F32)
        weighted_keys[s, 0] = high
        weighted_keys[s, 1] = weighted - high

    def one_head(h):
        mine = head_of == h
        for s in range(2):
            both = jnp.concatenate(
                [jnp.where(mine, weighted_keys[s, part], 0.0) for part in range(2)], axis=0
            )
            values = jnp.concatenate([last_v[s], last_v[s]], axis=0)
            update = lax.dot_general(
                both.astype(BF16), values, (((0,), (0,)), ((), ())), preferred_element_type=F32
            )
            at = s * heads + h
            power = jnp.full((1, value_size), -decay[h] * accepted[s].astype(F32), F32)
            fresh = jnp.exp(power) * prior_v[at] + update
            state_out[at] = fresh
            state_b[at] = fresh.astype(BF16)

    blocks = span // 16

    def scale_rows(i):
        at = pl.ds(i * 16, 16)
        for side in range(2):
            weights[side, at] = (weights[side, at].astype(F32) * gain[...]).astype(BF16)

    def first_scale():
        swap.wait()
        gain[...] = gain_v[...].astype(F32).reshape(1, width)
        scale_rows(0)

    one_head(0)
    one_head(1)
    work = [functools.partial(one_head, h) for h in range(2, heads)]
    work += [first_scale] + [functools.partial(scale_rows, i) for i in range(1, blocks)]
    work = iter(work)

    def beside():
        piece = next(work, None)
        if piece is not None:
            piece()

    for k in range(tokens.hops):
        tokens.round(k, beside)
        if k > 0:
            ring.step(k)
    tokens.last_arrivals()

    def a_copy(p, d):
        to = wrap(z + d, nz)
        return pltpu.make_async_remote_copy(
            src_ref=out_a.at[p, to],
            dst_ref=in_a.at[p, z],
            send_sem=a_sent.at[p, d],
            recv_sem=a_got.at[p, z],
            device_id={"kv_0": to},
            device_id_type=MESH,
        )

    for p in range(2):
        total = jnp.zeros((2 * span, seqs), F32)
        squares = jnp.zeros((1, seqs), F32)
        for c in range(nz):
            block = tokens_all[p, c].reshape(ny * depth, seqs)
            cut = pl.ds(c * ny * depth, ny * depth)
            total += jnp.dot(
                weights[:, :, cut].reshape(2 * span, ny * depth), block, preferred_element_type=F32
            )
            floats = block.astype(F32)
            squares += jnp.sum(floats * floats, axis=0, keepdims=True)
        scaled = total * lax.rsqrt(squares / width + epsilon)
        for side in range(2):
            part = jnp.concatenate(
                [scaled[side * span : (side + 1) * span], jnp.zeros((128 - span, seqs), F32)], axis=0
            )
            turned = part.T.astype(BF16)
            for to in range(nz):
                out_a[p, to, side] = turned[2 * ny * to : 2 * ny * (to + 1)]
        tokens.loop(1, nz, lambda i, p=p: a_copy(p, far_first(i, nz)).start())
        pltpu.make_async_copy(out_a.at[p, z], in_a.at[p, z], a_got.at[p, z]).start()

    def a_wait(came):
        for p in range(2):
            pltpu.make_async_remote_copy(
                src_ref=in_a.at[p, came],
                dst_ref=in_a.at[p, came],
                send_sem=a_sent.at[0, 0],
                recv_sem=a_got.at[p, came],
                device_id=partner,
                device_id_type=MESH,
            ).wait_recv()

    ring.step(tokens.hops)

    shift = heads.bit_length() - 1

    def prop_of(i):
        return 2 * (i >> (shift + 2)) + ((i >> shift) & 1)

    def at_of(i):
        return ((i >> (shift + 1)) & 1) * heads + (i & (heads - 1))

    row = iota((count, 128), 0)
    first = jnp.where((row >> (shift + 1)) & 1 == 0, lengths[0] + accepted[0], lengths[1] + accepted[1])
    angles = (first + prop_of(row)).astype(F32) * frequency[...]
    cosine = jnp.cos(angles)
    lane_sign = jnp.where(iota((count, 128), 1) < key_size // 2, -1.0, 1.0)
    sine = jnp.sin(angles) * lane_sign
    decays = by_head((count, 128))
    query_decay = jnp.exp(decays * (prop_of(row) + 1).astype(F32))
    other = iota((count, count), 1)
    here = row[:, :count]
    offset = prop_of(here) - prop_of(other)
    grid = jnp.where(
        (at_of(here) == at_of(other)) & (offset >= 0),
        jnp.exp(decays[:, :count] * jnp.maximum(offset, 0).astype(F32)),
        0.0,
    )

    tokens.loop(0, nz, a_wait)

    mid[...] = in_a[...].reshape(nz * 4 * 2 * ny, 128).astype(F32)
    stride = 2 * 2 * ny
    for to in range(ny):
        for side in range(2):
            for s in range(2):
                parts = [
                    mid[pl.ds(p * nz * stride + side * 2 * ny + 2 * to + s, nz, stride=stride), :]
                    for p in range(2)
                ]
                out_b[to, side, s] = jnp.concatenate(parts, axis=0).astype(BF16)

    def b_copy(d, same):
        to = wrap(y + d, ny)
        side = tp if same else 1 - tp
        return pltpu.make_async_remote_copy(
            src_ref=out_b.at[to, side],
            dst_ref=in_b.at[y, tp],
            send_sem=b_sent.at[d, side],
            recv_sem=b_got.at[y, tp],
            device_id={"kv_1": to, "tp": side},
            device_id_type=MESH,
        )

    def b_wait(d, same):
        came = wrap(y + d, ny)
        side = tp if same else 1 - tp
        pltpu.make_async_remote_copy(
            src_ref=in_b.at[came, side],
            dst_ref=in_b.at[came, side],
            send_sem=b_sent.at[0, 0],
            recv_sem=b_got.at[came, side],
            device_id=partner,
            device_id_type=MESH,
        ).wait_recv()

    def b_start(i):
        d = far_first(i, ny)
        b_copy(d, True).start()
        b_copy(d, False).start()

    tokens.loop(1, ny, b_start)
    b_copy(0, False).start()
    own_b = pltpu.make_async_copy(out_b.at[y, tp], in_b.at[y, tp], local.at[11])
    own_b.start()
    ring.share_on()

    lane = iota((128, 2 * key_size + 2 * value_size), 0)
    column = iota((128, 2 * key_size + 2 * value_size), 1)
    for j in range(ny):
        goal = jnp.where(
            lane < kc,
            kc * j + lane,
            jnp.where(
                lane < 2 * kc,
                key_size + kc * j + lane - kc,
                jnp.where(
                    lane < 2 * kc + vc,
                    2 * key_size + vc * j + lane - 2 * kc,
                    2 * key_size + value_size + vc * j + lane - 2 * kc - vc,
                ),
            ),
        )
        hit = (goal == column) & (lane < span)
        place[pl.ds(128 * j, 128)] = jnp.where(hit, 1.0, 0.0).astype(BF16)
    own_b.wait()
    b_wait(0, False)

    def b_take(d):
        b_wait(d, True)
        b_wait(d, False)

    tokens.loop(1, ny, b_take)

    packed = jnp.concatenate([in_b[j].reshape(count, 128) for j in range(ny)], axis=1)
    fields = jnp.dot(packed, place[...], preferred_element_type=F32)
    query = fields[:, :key_size]
    key = fields[:, key_size : 2 * key_size]
    value = fields[:, 2 * key_size : 2 * key_size + value_size]
    gate = fields[:, 2 * key_size + value_size :]
    half = key_size // 2

    def turned_by(x):
        swapped = jnp.concatenate([x[:, half:], x[:, :half]], axis=1)
        return x * cosine + swapped * sine

    query_rot = turned_by(query).astype(BF16)
    key_f = turned_by(key) * key_size ** (-0.5)
    key_rot = key_f.astype(BF16)
    value_b = value.astype(BF16)
    scores = lax.dot_general(
        query_rot, key_rot, (((1,), (1,)), ((), ())), preferred_element_type=F32
    )
    inner = jnp.dot((scores * grid).astype(BF16), value_b, preferred_element_type=F32)
    decayed = query_rot.astype(F32) * query_decay
    row_at = at_of(iota((count, 1), 0))
    spread = jnp.concatenate(
        [jnp.where(row_at == at, decayed, 0.0).astype(BF16) for at in range(2 * heads)], axis=1
    )
    states = state_b[...].reshape(2 * heads * key_size, value_size)
    heads_out = inner + jnp.dot(spread, states, preferred_element_type=F32)
    normed = heads_out * lax.rsqrt(jnp.mean(heads_out * heads_out, axis=-1, keepdims=True) + epsilon)
    product = gate / (1.0 + jnp.exp(-gate)) * normed
    for c in range(value_size // 128):
        rows_f[c] = product[:, 128 * c : 128 * (c + 1)]
    for i in range(8):
        prop, seq = 2 * (i // 4) + i % 2, (i // 2) % 2
        keys_out[seq, prop] = key_f[i * heads : (i + 1) * heads].astype(BF16)
        values_out[seq, prop] = value[i * heads : (i + 1) * heads].astype(BF16)
    cut = heads * value_size // 2
    for h in range(heads):
        part, at = divmod(h * value_size, cut)
        for c in range(value_size // 128):
            piece = rows_f[c, pl.ds(h, 8, stride=heads), :]
            chunk[part, :, at + 128 * c : at + 128 * (c + 1)] = piece.astype(BF16)

    first = ((y, ny, "kv_1"), (z, nz, "kv_0"))
    second = ((z, nz, "kv_0"), (y, ny, "kv_1"))

    def g_copy(p, d):
        f, n, axis = first[p]
        return pltpu.make_async_remote_copy(
            src_ref=chunk.at[p],
            dst_ref=gated_all.at[p, f],
            send_sem=g_sent.at[p, d],
            recv_sem=g_got.at[p, f],
            device_id={axis: wrap(f + d, n)},
            device_id_type=MESH,
        )

    def g_start(i):
        for p in range(2):
            g_copy(p, far_first(i, first[p][1])).start()

    tokens.loop(1, ny, g_start)
    for p in range(2):
        f = first[p][0]
        pltpu.make_async_copy(chunk.at[p], gated_all.at[p, f], g_got.at[p, f]).start()

    source = iota((4 * seqs, seqs), 0)
    target = iota((4 * seqs, seqs), 1)
    low_ring, high_ring = (source >> 3) & (ny - 1), source >> (2 + ny.bit_length())
    for part, group in enumerate((high_ring * ny + low_ring, low_ring * ny + high_ring)):
        row_seq = 2 * group + ((source >> 1) & 1)
        row_prop = 2 * ((source >> 2) & 1) + (source & 1)
        for p in range(4):
            hit = (row_seq == target) & (row_prop == p)
            order[part, :, pl.ds(seqs * p, seqs)] = jnp.where(hit, 1.0, 0.0).astype(BF16)
    ring.all_here()

    def c_copy(p, d, same):
        s, n, axis = second[p]
        to = wrap(s + d, n)
        side = tp if same else 1 - tp
        return pltpu.make_async_remote_copy(
            src_ref=out_c.at[p, to, side],
            dst_ref=in_c.at[p, tp, s],
            send_sem=c_sent.at[p, d, side],
            recv_sem=c_got.at[p, tp, s],
            device_id={axis: to, "tp": side},
            device_id_type=MESH,
        )

    def wait_for(block, arrived):
        pltpu.make_async_remote_copy(
            src_ref=block,
            dst_ref=block,
            send_sem=a_sent.at[0, 0],
            recv_sem=arrived,
            device_id=partner,
            device_id_type=MESH,
        ).wait_recv()

    out_cols = wo.shape[0]
    for p in range(2):
        n = first[p][1]
        tokens.loop(0, n, lambda f, p=p: wait_for(gated_all.at[p, f], g_got.at[p, f]))
        product = lax.dot_general(
            wo_all[p].reshape(second[p][1] * out_cols, cut),
            gated_all[p].reshape(n * 8, cut),
            (((1,), (1,)), ((), ())),
            preferred_element_type=F32,
        )
        part = out_cols // 2
        for to in range(second[p][1]):
            for side in range(2):
                at = to * out_cols + side * part
                halves = [product[at + e : at + e + part // 2] for e in (0, part // 2)]
                out_c[p, to, side] = jnp.concatenate(halves, axis=1).astype(BF16)

        def c_start(i, p=p, n=n):
            d = far_first(i, n)
            c_copy(p, d, True).start()
            c_copy(p, d, False).start()

        tokens.loop(1, n, c_start)
        c_copy(p, 0, False).start()
        s = second[p][0]
        pltpu.make_async_copy(
            out_c.at[p, s, tp], in_c.at[p, tp, s], c_got.at[p, tp, s]
        ).start()
    result = jnp.zeros((out_cols // 2, 4 * seqs), F32)
    for p in range(2):
        n = second[p][1]
        for side in range(2):
            tokens.loop(
                0, n, lambda s, p=p, side=side: wait_for(in_c.at[p, side, s], c_got.at[p, side, s])
            )
        sums = []
        for side in range(2):
            pairs = [[in_c[p, side, 2 * j + e].astype(F32) for e in range(2)] for j in range(n // 2)]
            for cut_at in (slice(0, 64), slice(64, 128)):
                sums.append(
                    jnp.concatenate([each[:, cut_at] for pair in pairs for each in pair], axis=1)
                )
        sums = jnp.concatenate(sums, axis=0).astype(BF16)
        moved = jnp.dot(sums, order[p], preferred_element_type=F32)
        result += moved[: out_cols // 2] + moved[out_cols // 2 :]
    result = result.astype(BF16)
    for p in range(4):
        ret_out[p] = result[:, p * seqs : (p + 1) * seqs]
    tokens.finish()
    ring.finish()

    def late_done(d):
        for p in range(2):
            g_copy(p, d).wait_send()
            for same in (True, False):
                c_copy(p, d, same).wait_send()

    tokens.loop(1, ny, late_done)
    for p in range(2):
        c_copy(p, 0, False).wait_send()
    for p in range(2):
        tokens.loop(1, nz, lambda d, p=p: a_copy(p, d).wait_send())

    def b_done(d):
        b_copy(d, True).wait_send()
        b_copy(d, False).wait_send()

    tokens.loop(1, ny, b_done)
    b_copy(0, False).wait_send()


def in_hbm(value):
    return pltpu.with_memory_space_constraint(value, pltpu.HBM)


def put_kernel(*refs):
    count = (len(refs) - 1) // 2
    sems = refs[-1]
    copies = [
        pltpu.make_async_copy(refs[i], refs[count + i], sems.at[i]) for i in range(count)
    ]
    for copy in copies:
        copy.start()
    for copy in copies:
        copy.wait()


def put_out(*values):
    return pl.pallas_call(
        put_kernel,
        out_shape=tuple(jax.ShapeDtypeStruct(v.shape, v.dtype) for v in values),
        in_specs=[pl.BlockSpec(memory_space=pl.ANY)] * len(values),
        out_specs=(pl.BlockSpec(memory_space=pltpu.HBM),) * len(values),
        scratch_shapes=[pltpu.SemaphoreType.DMA((len(values),))],
        compiler_params=pltpu.CompilerParams(vmem_limit_bytes=8 * 1024 * 1024),
    )(*values)


def shards(
    nx,
    nz,
    ny,
    tokens,
    norm_gain,
    query_weight,
    key_weight,
    value_weight,
    gate_weight,
    out_weight,
    decay_rate,
    prior_state,
    last_keys,
    last_values,
    accepted,
    lengths,
):
    _, heads, key_size, value_size = prior_state.shape
    seqs, _, depth = tokens.shape
    width = norm_gain.shape[0]
    kc, vc = query_weight.shape[1], value_weight.shape[1]
    span = 2 * kc + 2 * vc
    count = 8 * heads
    half = key_size // 2
    frequency = jnp.power(10000.0, -jnp.arange(half, dtype=F32) / half)
    frequency = jnp.concatenate([frequency, frequency])[None, :]

    hbm = pl.BlockSpec(memory_space=pltpu.HBM)
    vmem = pl.BlockSpec(memory_space=pltpu.VMEM)
    dma = pltpu.SemaphoreType.DMA
    cut = heads * value_size // 2
    out_cols = out_weight.shape[1]
    retained, state, new_keys, new_values = pl.pallas_call(
        functools.partial(kernel, nx, nz, ny),
        out_shape=(
            jax.ShapeDtypeStruct((4, out_cols // 2, seqs), BF16),
            jax.ShapeDtypeStruct((2 * heads, key_size, value_size), F32),
            jax.ShapeDtypeStruct((2, 4, heads, key_size), BF16),
            jax.ShapeDtypeStruct((2, 4, heads, value_size), BF16),
        ),
        in_specs=[hbm] * 13 + [vmem],
        out_specs=(vmem,) * 4,
        scratch_shapes=[
            pltpu.VMEM((2, depth, seqs), BF16),
            pltpu.VMEM((2, span, width), BF16),
            pltpu.VMEM((2, nz, out_cols, cut), BF16),
            pltpu.VMEM((2 * heads, key_size, value_size), F32),
            pltpu.VMEM((2, 4 * heads, key_size), BF16),
            pltpu.VMEM((2, 4 * heads, value_size), BF16),
            pltpu.SMEM((heads,), F32),
            pltpu.SMEM((2,), jnp.int32),
            pltpu.SMEM((2,), jnp.int32),
            pltpu.VMEM((width,), BF16),
            pltpu.VMEM((1, width), F32),
            pltpu.VMEM((2, 2, 4 * heads, key_size), F32),
            pltpu.VMEM((2 * heads, key_size, value_size), BF16),
            pltpu.VMEM((2, nz, ny, depth, seqs), BF16),
            pltpu.VMEM((128 * ny, 2 * key_size + 2 * value_size), BF16),
            pltpu.VMEM((2, 4 * seqs, 4 * seqs), BF16),
            pltpu.VMEM((2, nz, 2, 2 * ny, 128), BF16),
            pltpu.VMEM((2, nz, 2, 2 * ny, 128), BF16),
            pltpu.VMEM((nz * 8 * ny, 128), F32),
            pltpu.VMEM((ny, 2, 2, 2 * nz, 128), BF16),
            pltpu.VMEM((ny, 2, 2, 2 * nz, 128), BF16),
            pltpu.VMEM((value_size // 128, count, 128), F32),
            pltpu.VMEM((2, 8, cut), BF16),
            pltpu.VMEM((2, nz, 8, cut), BF16),
            pltpu.VMEM((2, nz, 2, out_cols // 4, 128), BF16),
            pltpu.VMEM((2, 2, nz, out_cols // 4, 128), BF16),
            dma((23,)),
            dma((2, nz, ny)),
            dma((2, max(nz, ny), TorusGather.groups)),
            dma((2, max(nz, ny))),
            dma((2, 2, nz // 2, TorusGather.groups)),
            dma((2, nz)),
            dma((2, 2, nz // 2)),
            dma((2, 2, nz)),
            dma((2, 2, nz)),
            dma((2,)),
            dma((2,)),
            dma((2, nz)),
            dma((2, nz)),
            dma((2, nz, 2)),
            dma((2, 2, nz)),
            dma((4,)),
            dma((2, nz)),
            dma((2, nz)),
            dma((ny, 2)),
            dma((ny, 2)),
        ],
        compiler_params=pltpu.CompilerParams(
            collective_id=0, has_side_effects=True, vmem_limit_bytes=48 * 1024 * 1024
        ),
    )(
        *map(
            in_hbm,
            (
                tokens.transpose(1, 2, 0),
                query_weight.T,
                key_weight.T,
                value_weight.T,
                gate_weight.T,
                out_weight.T,
                prior_state.reshape(2 * heads, key_size, value_size),
                last_keys.reshape(2, 4 * heads, key_size),
                last_values.reshape(2, 4 * heads, value_size),
                decay_rate,
                accepted,
                lengths,
                norm_gain,
            ),
        ),
        frequency,
    )
    retained, state, new_keys, new_values = put_out(retained, state, new_keys, new_values)
    return (
        retained.transpose(2, 0, 1),
        state.reshape(prior_state.shape),
        new_keys,
        new_values,
    )


def solution(mesh):
    nz = ny = 8
    finer = Mesh(
        mesh.devices.reshape(mesh.shape["dp"], nz, ny, mesh.shape["tp"]),
        ("dp", "kv_0", "kv_1", "tp"),
    )
    return jax.shard_map(
        functools.partial(shards, mesh.shape["dp"], nz, ny),
        mesh=finer,
        in_specs=(
            P("dp", None, KV),
            P(),
            P(None, TP_KV),
            P(None, TP_KV),
            P(None, TP_KV),
            P(None, TP_KV),
            P("tp", KV),
            P("tp"),
            P(DP_KV, "tp", None, None),
            P(DP_KV, None, "tp", None),
            P(DP_KV, None, "tp", None),
            P(DP_KV),
            P(DP_KV),
        ),
        out_specs=(
            P("dp", None, KV_TP),
            P(DP_KV, "tp", None, None),
            P(DP_KV, None, "tp", None),
            P(DP_KV, None, "tp", None),
        ),
        check_vma=False,
    )
```

```python
import functools

import jax
import jax.numpy as jnp
from jax import lax
from jax.experimental import pallas as pl
from jax.experimental.pallas import tpu as pltpu
from jax.sharding import Mesh
from jax.sharding import PartitionSpec as P

KV = ("kv_0", "kv_1")
TP_KV = ("tp", "kv_0", "kv_1")
DP_KV = ("dp", "kv_0", "kv_1")
KV_TP = ("kv_0", "kv_1", "tp")
MESH = pl.DeviceIdType.MESH
F32, BF16 = jnp.float32, jnp.bfloat16

epsilon = 1e-06


def wrap(i, n):
    return i & (n - 1)


def far_first(i, n):
    return wrap(n // 2 + (1 - 2 * (i & 1)) * (i >> 1), n)


def near_first(i, n):
    odd = i & 1
    return wrap(odd * ((i + 1) >> 1) + (1 - odd) * (n - (i >> 1)), n)


class TorusGather:
    groups = 8
    turn = (0, 1, 7, 2, 6, 3, 5, 4)

    def __init__(self, own, held, arrived, ring_arrived, first_sent, ring_sent, nz, ny):
        self.own, self.held, self.arrived, self.ring_arrived = own, held, arrived, ring_arrived
        self.first_sent, self.ring_sent = first_sent, ring_sent
        z, y = lax.axis_index("kv_0"), lax.axis_index("kv_1")
        self.partner = {"tp": 1 - lax.axis_index("tp")}
        self.first = ((y, ny, "kv_1"), (z, nz, "kv_0"))
        self.second = ((z, nz, "kv_0"), (y, ny, "kv_1"))
        self.hops = nz // 2
        self.size = ny // self.groups

    def at(self, ref, p, f, s):
        return ref.at[p, s, f] if p == 0 else ref.at[p, f, s]

    def copy(self, target, source, sent, arrived, device):
        return pltpu.make_async_remote_copy(
            src_ref=source,
            dst_ref=target,
            send_sem=sent,
            recv_sem=arrived,
            device_id=device,
            device_id_type=MESH,
        )

    def first_copy(self, p, d):
        (f, n, axis), (s, _, _) = self.first[p], self.second[p]
        return self.copy(
            self.at(self.held, p, f, s),
            self.own(p),
            self.first_sent.at[p, d],
            self.at(self.arrived, p, f, s),
            {axis: wrap(f + d, n)},
        )

    def start_first(self):
        def send(i):
            for p in range(2):
                self.first_copy(p, near_first(i, self.first[p][1])).start()

        self.loop(1, self.first[0][1], send)
        for p in range(2):
            (f, _, _), (s, _, _) = self.first[p], self.second[p]
            pltpu.make_async_copy(
                self.own(p), self.at(self.held, p, f, s), self.at(self.arrived, p, f, s)
            ).start()

    def group(self, p, i):
        f = self.first[p][0]
        return wrap(f // self.size + self.turn[i], self.groups)

    def group_at(self, p, q, s):
        return self.at(self.held, p, pl.ds(q * self.size, self.size), s)

    def ring_copy(self, p, k, i, way, reach=1):
        s, n, axis = self.second[p]
        q, origin = self.group(p, i), wrap(s - way * k + n, n)
        block = self.group_at(p, q, origin)
        return self.copy(
            block,
            block,
            self.ring_sent.at[p, (1 + way) // 2, k + reach - 1, i],
            self.ring_arrived.at[p, origin, q],
            {axis: wrap(s + reach * way + n, n)},
        )

    def wait_chunk(self, p, f, s):
        chunk = self.at(self.held, p, f, s)
        self.copy(
            chunk, chunk, self.first_sent.at[0, 0], self.at(self.arrived, p, f, s), self.partner
        ).wait_recv()

    def wait_group(self, p, i, s):
        q = self.group(p, i)
        block = self.group_at(p, q, s)
        self.copy(
            block, block, self.first_sent.at[0, 0], self.ring_arrived.at[p, s, q], self.partner
        ).wait_recv()

    def pass_on(self, k, i, ways):
        for p in range(2):
            s, n, _ = self.second[p]
            if k == 0:
                for e in range(self.size):
                    self.wait_chunk(p, self.group(p, i) * self.size + e, s)
                for way in ways:
                    self.ring_copy(p, k, i, way).start()
            else:
                for way in (1, -1):
                    self.wait_group(p, i, wrap(s - way * k + n, n))
                    if k == self.hops - 2 and way == self.far_way(i):
                        self.ring_copy(p, k, i, way, 2).start()
                    if way in ways:
                        self.ring_copy(p, k, i, way).start()

    def loop(self, low, high, step):
        def body(i, _):
            step(i)
            return 0

        lax.fori_loop(low, high, body, 0)

    def ways(self, k, i):
        return (1, -1) if k < self.hops - 1 else ()

    def far_way(self, i):
        return 1 if i % 2 else -1

    def round(self, k, beside=None):
        for i in range(self.groups):
            self.pass_on(k, i, self.ways(k, i))
            if beside is not None:
                beside()

    def last_arrivals(self):
        for i in range(self.groups):
            for p in range(2):
                s, n, _ = self.second[p]
                self.wait_group(p, i, wrap(s + self.hops, n))

    def finish(self):
        def first_done(d):
            for p in range(2):
                self.first_copy(p, d).wait_send()

        self.loop(1, self.first[0][1], first_done)
        for k in range(self.hops):
            for i in range(self.groups):
                for p in range(2):
                    for way in self.ways(k, i):
                        self.ring_copy(p, k, i, way).wait_send()
                    if k == self.hops - 2:
                        self.ring_copy(p, k, i, self.far_way(i), 2).wait_send()


class WeightRing:
    def __init__(self, held, arrived, sent, side_arrived, side_sent, on_arrived, on_sent, nx, nz, ny):
        self.held, self.arrived, self.sent = held, arrived, sent
        self.side_arrived, self.side_sent = side_arrived, side_sent
        self.on_arrived, self.on_sent = on_arrived, on_sent
        self.x, self.nx = lax.axis_index("dp"), nx
        z, y = lax.axis_index("kv_0"), lax.axis_index("kv_1")
        self.partner = {"tp": 1 - lax.axis_index("tp")}
        self.second = ((z, nz, "kv_0"), (y, ny, "kv_1"))
        self.hops = nz // 2
        self.rows = held.shape[2] // nx

    def block(self, p, origin, x):
        return self.held.at[p, origin, pl.ds(pl.multiple_of(self.rows * x, self.rows), self.rows)]

    def copy(self, block, sent, arrived, device):
        return pltpu.make_async_remote_copy(
            src_ref=block,
            dst_ref=block,
            send_sem=sent,
            recv_sem=arrived,
            device_id=device,
            device_id_type=MESH,
        )

    def ring_copy(self, p, k, way, reach=1):
        s, n, axis = self.second[p]
        origin = wrap(s - way * k + n, n)
        return self.copy(
            self.block(p, origin, self.x),
            self.sent.at[p, (1 + way) // 2, k + reach - 1],
            self.arrived.at[p, origin],
            {axis: wrap(s + reach * way + n, n)},
        )

    def side_copy(self, p, origin, way):
        at = (1 + way) // 2
        return self.copy(
            self.block(p, origin, self.x),
            self.side_sent.at[p, at, origin],
            self.side_arrived.at[p, at, origin],
            {"dp": wrap(self.x + way + self.nx, self.nx)},
        )

    def on_way(self, p):
        return 1 - 2 * p

    def on_copy(self, p):
        way = self.on_way(p)
        x = wrap(self.x - way + self.nx, self.nx)
        block = self.held.at[p, :, pl.ds(pl.multiple_of(self.rows * x, self.rows), self.rows)]
        return self.copy(
            block,
            self.on_sent.at[p],
            self.on_arrived.at[p],
            {"dp": wrap(self.x + way + self.nx, self.nx)},
        )

    def forward_ways(self, p, k):
        return (1, -1) if k < self.hops - 1 else ()

    def step(self, k):
        for p in range(2):
            s, n, _ = self.second[p]
            for way in (1,) if k in (0, self.hops) else (1, -1):
                origin = wrap(s - way * k + n, n)
                if k > 0:
                    self.copy(
                        self.block(p, origin, self.x),
                        self.sent.at[0, 0, 0],
                        self.arrived.at[p, origin],
                        self.partner,
                    ).wait_recv()
                ways = self.forward_ways(p, k)
                for to in ways if k == 0 else (way,):
                    if to in ways:
                        self.ring_copy(p, k, to).start()
                        if k == self.hops - 2 and to == self.on_way(p):
                            self.ring_copy(p, k, to, 2).start()
                for to in (1, -1):
                    self.side_copy(p, origin, to).start()

    def side_wait(self, p, way):
        x = wrap(self.x - way + self.nx, self.nx)

        def take(origin, _):
            self.copy(
                self.block(p, origin, x),
                self.sent.at[0, 0, 0],
                self.side_arrived.at[p, (1 + way) // 2, origin],
                self.partner,
            ).wait_recv()
            return 0

        lax.fori_loop(0, self.second[p][1], take, 0)

    def share_on(self):
        for p in range(2):
            self.side_wait(p, self.on_way(p))
            self.on_copy(p).start()

    def all_here(self):
        for p in range(2):
            self.side_wait(p, -self.on_way(p))
            self.on_copy(p).wait_recv()

    def finish(self):
        for p in range(2):
            for k in range(self.hops):
                for way in self.forward_ways(p, k):
                    self.ring_copy(p, k, way).wait_send()
            self.ring_copy(p, self.hops - 2, self.on_way(p), 2).wait_send()

            def done(origin, _, p=p):
                for way in (1, -1):
                    self.side_copy(p, origin, way).wait_send()
                return 0

            lax.fori_loop(0, self.second[p][1], done, 0)
            self.on_copy(p).wait_send()


def iota(shape, dim):
    return lax.broadcasted_iota(jnp.int32, shape, dim)


def kernel(
    nx,
    nz,
    ny,
    tok,
    wq,
    wk,
    wv,
    wg,
    wo,
    prior,
    last_k_in,
    last_v_in,
    decay_in,
    accepted_in,
    lengths_in,
    gain_in,
    frequency,
    ret_out,
    state_out,
    keys_out,
    values_out,
    tok_v,
    weights,
    wo_all,
    prior_v,
    last_k,
    last_v,
    decay,
    accepted,
    lengths,
    gain_v,
    gain,
    weighted_keys,
    state_b,
    tokens_all,
    place,
    order,
    out_a,
    in_a,
    mid,
    out_b,
    in_b,
    rows_f,
    chunk,
    gated_all,
    out_c,
    in_c,
    local,
    tok_arrived,
    tok_passed,
    tok_first,
    tok_ring,
    wo_arrived,
    wo_sent,
    wo_side,
    wo_side_sent,
    wo_on,
    wo_on_sent,
    g_sent,
    g_got,
    c_sent,
    c_got,
    pair_sems,
    a_sent,
    a_got,
    b_sent,
    b_got,
):
    x, z, y, tp = (lax.axis_index(axis) for axis in ("dp", "kv_0", "kv_1", "tp"))
    heads, seqs = nz, 2 * nz * ny
    kc = wq.shape[0]
    vc = wv.shape[0]
    span = 2 * kc + 2 * vc
    depth = tok_v.shape[1]
    width = nz * ny * depth
    partner = {"tp": 1 - tp}

    loads = [
        pltpu.make_async_copy(tok.at[pl.ds(2 * tp, 2)], tok_v, local.at[0]),
        pltpu.make_async_copy(wq, weights.at[tp, pl.ds(0, kc)], local.at[1]),
        pltpu.make_async_copy(wk, weights.at[tp, pl.ds(kc, kc)], local.at[2]),
        pltpu.make_async_copy(wv, weights.at[tp, pl.ds(2 * kc, vc)], local.at[3]),
        pltpu.make_async_copy(wg, weights.at[tp, pl.ds(2 * kc + vc, vc)], local.at[4]),
        pltpu.make_async_copy(prior, prior_v, local.at[5]),
    ]
    small_loads = [
        pltpu.make_async_copy(source, target, local.at[17 + i])
        for i, (source, target) in enumerate(
            (
                (last_k_in, last_k),
                (last_v_in, last_v),
                (decay_in, decay),
                (accepted_in, accepted),
                (lengths_in, lengths),
                (gain_in, gain_v),
            )
        )
    ]
    share = wo.shape[0] // nx
    mine = pl.ds(pl.multiple_of(share * x, share), share)
    half_k = wo.shape[1] // 2
    own_out = [
        pltpu.make_async_copy(
            wo.at[mine, pl.ds(p * half_k, half_k)], wo_all.at[p, (z, y)[p], mine], local.at[7 + p]
        )
        for p in range(2)
    ]
    for load in loads + own_out + small_loads:
        load.start()

    barrier = pltpu.get_barrier_semaphore()

    def greet(device):
        pl.semaphore_signal(barrier, inc=1, device_id=device, device_id_type=MESH)

    def greet_y(d, _):
        other = wrap(y + d, ny)
        greet({"kv_1": other})
        greet({"kv_1": other, "tp": 1 - tp})
        return 0

    def greet_z(d, _):
        greet({"kv_0": wrap(z + d, nz)})
        return 0

    lax.fori_loop(1, ny, greet_y, 0)
    lax.fori_loop(1, nz, greet_z, 0)
    def greet_tall(d, _):
        greet({"kv_0": wrap(z + d, nz), "tp": 1 - tp})
        return 0

    lax.fori_loop(1, nz, greet_tall, 0)
    greet(partner)
    for way in (1, nx - 1):
        greet({"dp": wrap(x + way, nx)})
    pl.semaphore_wait(barrier, 2 * (ny - 1) + 2 * (nz - 1) + 3)

    loads[0].wait()
    tokens = TorusGather(
        lambda p: tok_v.at[p], tokens_all, tok_arrived, tok_passed, tok_first, tok_ring, nz, ny
    )
    tokens.start_first()
    ring = WeightRing(
        wo_all, wo_arrived, wo_sent, wo_side, wo_side_sent, wo_on, wo_on_sent, nx, nz, ny
    )
    for load in own_out:
        load.wait()
    ring.step(0)
    for load in loads[1:5]:
        load.wait()
    swap = pltpu.make_async_remote_copy(
        src_ref=weights.at[tp],
        dst_ref=weights.at[tp],
        send_sem=pair_sems.at[0],
        recv_sem=pair_sems.at[1],
        device_id=partner,
        device_id_type=MESH,
    )
    swap.start()

    key_size, value_size = ny * kc, ny * vc

    loads[5].wait()
    for load in small_loads:
        load.wait()
    rows, count = 4 * heads, 8 * heads
    head_of = iota((rows, 1), 0) & (heads - 1)

    def by_head(shape):
        head = iota(shape, 0) & (heads - 1)
        table = jnp.zeros(shape, F32)
        for h in range(heads):
            table = jnp.where(head == h, -decay[h], table)
        return table

    taken_decay = by_head((rows, 128))
    before = iota((rows, 128), 0) >> (heads.bit_length() - 1)
    for s in range(2):
        power = jnp.maximum(accepted[s] - 1 - before, 0).astype(F32)
        key_weights = jnp.where(before < accepted[s], jnp.exp(taken_decay * power), 0.0)
        weighted = last_k[s].astype(F32) * key_weights
        high = weighted.astype(BF16).astype(F32)
        weighted_keys[s, 0] = high
        weighted_keys[s, 1] = weighted - high

    def one_head(h):
        mine = head_of == h
        for s in range(2):
            both = jnp.concatenate(
                [jnp.where(mine, weighted_keys[s, part], 0.0) for part in range(2)], axis=0
            )
            values = jnp.concatenate([last_v[s], last_v[s]], axis=0)
            update = lax.dot_general(
                both.astype(BF16), values, (((0,), (0,)), ((), ())), preferred_element_type=F32
            )
            at = s * heads + h
            power = jnp.full((1, value_size), -decay[h] * accepted[s].astype(F32), F32)
            fresh = jnp.exp(power) * prior_v[at] + update
            state_out[at] = fresh
            state_b[at] = fresh.astype(BF16)

    blocks = span // 16

    def scale_rows(i):
        at = pl.ds(i * 16, 16)
        for side in range(2):
            weights[side, at] = (weights[side, at].astype(F32) * gain[...]).astype(BF16)

    def first_scale():
        swap.wait()
        gain[...] = gain_v[...].astype(F32).reshape(1, width)
        scale_rows(0)

    one_head(0)
    one_head(1)
    work = [functools.partial(one_head, h) for h in range(2, heads)]
    work += [first_scale] + [functools.partial(scale_rows, i) for i in range(1, blocks)]
    work = iter(work)

    def beside():
        piece = next(work, None)
        if piece is not None:
            piece()

    for k in range(tokens.hops):
        tokens.round(k, beside)
        if k > 0:
            ring.step(k)
    tokens.last_arrivals()

    def a_copy(p, d):
        to = wrap(z + d, nz)
        return pltpu.make_async_remote_copy(
            src_ref=out_a.at[p, to],
            dst_ref=in_a.at[p, z],
            send_sem=a_sent.at[p, d],
            recv_sem=a_got.at[p, z],
            device_id={"kv_0": to},
            device_id_type=MESH,
        )

    for p in range(2):
        total = jnp.zeros((2 * span, seqs), F32)
        squares = jnp.zeros((1, seqs), F32)
        for c in range(nz):
            block = tokens_all[p, c].reshape(ny * depth, seqs)
            cut = pl.ds(c * ny * depth, ny * depth)
            total += jnp.dot(
                weights[:, :, cut].reshape(2 * span, ny * depth), block, preferred_element_type=F32
            )
            floats = block.astype(F32)
            squares += jnp.sum(floats * floats, axis=0, keepdims=True)
        scaled = total * lax.rsqrt(squares / width + epsilon)
        for side in range(2):
            part = jnp.concatenate(
                [scaled[side * span : (side + 1) * span], jnp.zeros((128 - span, seqs), F32)], axis=0
            )
            turned = part.T.astype(BF16)
            for to in range(nz):
                out_a[p, to, side] = turned[2 * ny * to : 2 * ny * (to + 1)]
        tokens.loop(1, nz, lambda i, p=p: a_copy(p, far_first(i, nz)).start())
        pltpu.make_async_copy(out_a.at[p, z], in_a.at[p, z], a_got.at[p, z]).start()

    def a_wait(came):
        for p in range(2):
            pltpu.make_async_remote_copy(
                src_ref=in_a.at[p, came],
                dst_ref=in_a.at[p, came],
                send_sem=a_sent.at[0, 0],
                recv_sem=a_got.at[p, came],
                device_id=partner,
                device_id_type=MESH,
            ).wait_recv()

    ring.step(tokens.hops)
    tokens.finish()

    shift = heads.bit_length() - 1

    def prop_of(i):
        return 2 * (i >> (shift + 2)) + ((i >> shift) & 1)

    def at_of(i):
        return ((i >> (shift + 1)) & 1) * heads + (i & (heads - 1))

    row = iota((count, 128), 0)
    first = jnp.where((row >> (shift + 1)) & 1 == 0, lengths[0] + accepted[0], lengths[1] + accepted[1])
    angles = (first + prop_of(row)).astype(F32) * frequency[...]
    cosine = jnp.cos(angles)
    lane_sign = jnp.where(iota((count, 128), 1) < key_size // 2, -1.0, 1.0)
    sine = jnp.sin(angles) * lane_sign
    decays = by_head((count, 128))
    query_decay = jnp.exp(decays * (prop_of(row) + 1).astype(F32))
    other = iota((count, count), 1)
    here = row[:, :count]
    offset = prop_of(here) - prop_of(other)
    grid = jnp.where(
        (at_of(here) == at_of(other)) & (offset >= 0),
        jnp.exp(decays[:, :count] * jnp.maximum(offset, 0).astype(F32)),
        0.0,
    )

    tokens.loop(0, nz, a_wait)

    mid[...] = in_a[...].reshape(nz * 4 * 2 * ny, 128).astype(F32)
    stride = 2 * 2 * ny
    for to in range(ny):
        for side in range(2):
            for s in range(2):
                parts = [
                    mid[pl.ds(p * nz * stride + side * 2 * ny + 2 * to + s, nz, stride=stride), :]
                    for p in range(2)
                ]
                out_b[to, side, s] = jnp.concatenate(parts, axis=0).astype(BF16)

    def b_copy(d, same):
        to = wrap(y + d, ny)
        side = tp if same else 1 - tp
        return pltpu.make_async_remote_copy(
            src_ref=out_b.at[to, side],
            dst_ref=in_b.at[y, tp],
            send_sem=b_sent.at[d, side],
            recv_sem=b_got.at[y, tp],
            device_id={"kv_1": to, "tp": side},
            device_id_type=MESH,
        )

    def b_wait(d, same):
        came = wrap(y + d, ny)
        side = tp if same else 1 - tp
        pltpu.make_async_remote_copy(
            src_ref=in_b.at[came, side],
            dst_ref=in_b.at[came, side],
            send_sem=b_sent.at[0, 0],
            recv_sem=b_got.at[came, side],
            device_id=partner,
            device_id_type=MESH,
        ).wait_recv()

    def b_start(i):
        d = far_first(i, ny)
        b_copy(d, True).start()
        b_copy(d, False).start()

    tokens.loop(1, ny, b_start)
    b_copy(0, False).start()
    own_b = pltpu.make_async_copy(out_b.at[y, tp], in_b.at[y, tp], local.at[11])
    own_b.start()
    ring.share_on()

    lane = iota((128, 2 * key_size + 2 * value_size), 0)
    column = iota((128, 2 * key_size + 2 * value_size), 1)
    for j in range(ny):
        goal = jnp.where(
            lane < kc,
            kc * j + lane,
            jnp.where(
                lane < 2 * kc,
                key_size + kc * j + lane - kc,
                jnp.where(
                    lane < 2 * kc + vc,
                    2 * key_size + vc * j + lane - 2 * kc,
                    2 * key_size + value_size + vc * j + lane - 2 * kc - vc,
                ),
            ),
        )
        hit = (goal == column) & (lane < span)
        place[pl.ds(128 * j, 128)] = jnp.where(hit, 1.0, 0.0).astype(BF16)
    own_b.wait()
    b_wait(0, False)

    def b_take(d):
        b_wait(d, True)
        b_wait(d, False)

    tokens.loop(1, ny, b_take)

    packed = jnp.concatenate([in_b[j].reshape(count, 128) for j in range(ny)], axis=1)
    fields = jnp.dot(packed, place[...], preferred_element_type=F32)
    query = fields[:, :key_size]
    key = fields[:, key_size : 2 * key_size]
    value = fields[:, 2 * key_size : 2 * key_size + value_size]
    gate = fields[:, 2 * key_size + value_size :]
    half = key_size // 2

    def turned_by(x):
        swapped = jnp.concatenate([x[:, half:], x[:, :half]], axis=1)
        return x * cosine + swapped * sine

    query_rot = turned_by(query).astype(BF16)
    key_f = turned_by(key) * key_size ** (-0.5)
    key_rot = key_f.astype(BF16)
    value_b = value.astype(BF16)
    scores = lax.dot_general(
        query_rot, key_rot, (((1,), (1,)), ((), ())), preferred_element_type=F32
    )
    inner = jnp.dot((scores * grid).astype(BF16), value_b, preferred_element_type=F32)
    decayed = query_rot.astype(F32) * query_decay
    row_at = at_of(iota((count, 1), 0))
    spread = jnp.concatenate(
        [jnp.where(row_at == at, decayed, 0.0).astype(BF16) for at in range(2 * heads)], axis=1
    )
    states = state_b[...].reshape(2 * heads * key_size, value_size)
    heads_out = inner + jnp.dot(spread, states, preferred_element_type=F32)
    normed = heads_out * lax.rsqrt(jnp.mean(heads_out * heads_out, axis=-1, keepdims=True) + epsilon)
    product = gate / (1.0 + jnp.exp(-gate)) * normed
    for c in range(value_size // 128):
        rows_f[c] = product[:, 128 * c : 128 * (c + 1)]
    for i in range(8):
        prop, seq = 2 * (i // 4) + i % 2, (i // 2) % 2
        keys_out[seq, prop] = key_f[i * heads : (i + 1) * heads].astype(BF16)
        values_out[seq, prop] = value[i * heads : (i + 1) * heads].astype(BF16)
    cut = heads * value_size // 2
    for h in range(heads):
        part, at = divmod(h * value_size, cut)
        for c in range(value_size // 128):
            piece = rows_f[c, pl.ds(h, 8, stride=heads), :]
            chunk[part, :, at + 128 * c : at + 128 * (c + 1)] = piece.astype(BF16)

    first = ((y, ny, "kv_1"), (z, nz, "kv_0"))
    second = ((z, nz, "kv_0"), (y, ny, "kv_1"))

    def g_copy(p, d):
        f, n, axis = first[p]
        return pltpu.make_async_remote_copy(
            src_ref=chunk.at[p],
            dst_ref=gated_all.at[p, f],
            send_sem=g_sent.at[p, d],
            recv_sem=g_got.at[p, f],
            device_id={axis: wrap(f + d, n)},
            device_id_type=MESH,
        )

    def g_start(i):
        for p in range(2):
            g_copy(p, far_first(i, first[p][1])).start()

    tokens.loop(1, ny, g_start)
    for p in range(2):
        f = first[p][0]
        pltpu.make_async_copy(chunk.at[p], gated_all.at[p, f], g_got.at[p, f]).start()

    source = iota((4 * seqs, seqs), 0)
    target = iota((4 * seqs, seqs), 1)
    low_ring, high_ring = (source >> 3) & (ny - 1), source >> (2 + ny.bit_length())
    for part, group in enumerate((high_ring * ny + low_ring, low_ring * ny + high_ring)):
        row_seq = 2 * group + ((source >> 1) & 1)
        row_prop = 2 * ((source >> 2) & 1) + (source & 1)
        for p in range(4):
            hit = (row_seq == target) & (row_prop == p)
            order[part, :, pl.ds(seqs * p, seqs)] = jnp.where(hit, 1.0, 0.0).astype(BF16)
    ring.all_here()
    ring.finish()
    for p in range(2):
        tokens.loop(1, nz, lambda d, p=p: a_copy(p, d).wait_send())

    def b_done(d):
        b_copy(d, True).wait_send()
        b_copy(d, False).wait_send()

    tokens.loop(1, ny, b_done)
    b_copy(0, False).wait_send()

    def c_copy(p, d, same):
        s, n, axis = second[p]
        to = wrap(s + d, n)
        side = tp if same else 1 - tp
        return pltpu.make_async_remote_copy(
            src_ref=out_c.at[p, to, side],
            dst_ref=in_c.at[p, tp, s],
            send_sem=c_sent.at[p, d, side],
            recv_sem=c_got.at[p, tp, s],
            device_id={axis: to, "tp": side},
            device_id_type=MESH,
        )

    def wait_for(block, arrived):
        pltpu.make_async_remote_copy(
            src_ref=block,
            dst_ref=block,
            send_sem=a_sent.at[0, 0],
            recv_sem=arrived,
            device_id=partner,
            device_id_type=MESH,
        ).wait_recv()

    out_cols = wo.shape[0]
    for p in range(2):
        n = first[p][1]
        tokens.loop(0, n, lambda f, p=p: wait_for(gated_all.at[p, f], g_got.at[p, f]))
        product = lax.dot_general(
            wo_all[p].reshape(second[p][1] * out_cols, cut),
            gated_all[p].reshape(n * 8, cut),
            (((1,), (1,)), ((), ())),
            preferred_element_type=F32,
        )
        part = out_cols // 2
        for to in range(second[p][1]):
            for side in range(2):
                at = to * out_cols + side * part
                halves = [product[at + e : at + e + part // 2] for e in (0, part // 2)]
                out_c[p, to, side] = jnp.concatenate(halves, axis=1).astype(BF16)

        def c_start(i, p=p, n=n):
            d = far_first(i, n)
            c_copy(p, d, True).start()
            c_copy(p, d, False).start()

        tokens.loop(1, n, c_start)
        c_copy(p, 0, False).start()
        s = second[p][0]
        pltpu.make_async_copy(
            out_c.at[p, s, tp], in_c.at[p, tp, s], c_got.at[p, tp, s]
        ).start()

    def g_done(d):
        for p in range(2):
            g_copy(p, d).wait_send()

    tokens.loop(1, ny, g_done)
    result = jnp.zeros((out_cols // 2, 4 * seqs), F32)
    for p in range(2):
        n = second[p][1]
        for side in range(2):
            tokens.loop(
                0, n, lambda s, p=p, side=side: wait_for(in_c.at[p, side, s], c_got.at[p, side, s])
            )
        sums = []
        for side in range(2):
            pairs = [[in_c[p, side, 2 * j + e].astype(F32) for e in range(2)] for j in range(n // 2)]
            for cut_at in (slice(0, 64), slice(64, 128)):
                sums.append(
                    jnp.concatenate([each[:, cut_at] for pair in pairs for each in pair], axis=1)
                )
        sums = jnp.concatenate(sums, axis=0).astype(BF16)
        moved = jnp.dot(sums, order[p], preferred_element_type=F32)
        result += moved[: out_cols // 2] + moved[out_cols // 2 :]
    result = result.astype(BF16)
    for p in range(4):
        ret_out[p] = result[:, p * seqs : (p + 1) * seqs]
    def c_done(d):
        for p in range(2):
            for same in (True, False):
                c_copy(p, d, same).wait_send()

    tokens.loop(1, ny, c_done)
    for p in range(2):
        c_copy(p, 0, False).wait_send()


def in_hbm(value):
    return pltpu.with_memory_space_constraint(value, pltpu.HBM)


def put_kernel(*refs):
    count = (len(refs) - 1) // 2
    sems = refs[-1]
    copies = [
        pltpu.make_async_copy(refs[i], refs[count + i], sems.at[i]) for i in range(count)
    ]
    for copy in copies:
        copy.start()
    for copy in copies:
        copy.wait()


def put_out(*values):
    return pl.pallas_call(
        put_kernel,
        out_shape=tuple(jax.ShapeDtypeStruct(v.shape, v.dtype) for v in values),
        in_specs=[pl.BlockSpec(memory_space=pl.ANY)] * len(values),
        out_specs=(pl.BlockSpec(memory_space=pltpu.HBM),) * len(values),
        scratch_shapes=[pltpu.SemaphoreType.DMA((len(values),))],
        compiler_params=pltpu.CompilerParams(vmem_limit_bytes=8 * 1024 * 1024),
    )(*values)


def shards(
    nx,
    nz,
    ny,
    tokens,
    norm_gain,
    query_weight,
    key_weight,
    value_weight,
    gate_weight,
    out_weight,
    decay_rate,
    prior_state,
    last_keys,
    last_values,
    accepted,
    lengths,
):
    _, heads, key_size, value_size = prior_state.shape
    seqs, _, depth = tokens.shape
    width = norm_gain.shape[0]
    kc, vc = query_weight.shape[1], value_weight.shape[1]
    span = 2 * kc + 2 * vc
    count = 8 * heads
    half = key_size // 2
    frequency = jnp.power(10000.0, -jnp.arange(half, dtype=F32) / half)
    frequency = jnp.concatenate([frequency, frequency])[None, :]

    hbm = pl.BlockSpec(memory_space=pltpu.HBM)
    vmem = pl.BlockSpec(memory_space=pltpu.VMEM)
    dma = pltpu.SemaphoreType.DMA
    cut = heads * value_size // 2
    out_cols = out_weight.shape[1]
    retained, state, new_keys, new_values = pl.pallas_call(
        functools.partial(kernel, nx, nz, ny),
        out_shape=(
            jax.ShapeDtypeStruct((4, out_cols // 2, seqs), BF16),
            jax.ShapeDtypeStruct((2 * heads, key_size, value_size), F32),
            jax.ShapeDtypeStruct((2, 4, heads, key_size), BF16),
            jax.ShapeDtypeStruct((2, 4, heads, value_size), BF16),
        ),
        in_specs=[hbm] * 13 + [vmem],
        out_specs=(vmem,) * 4,
        scratch_shapes=[
            pltpu.VMEM((2, depth, seqs), BF16),
            pltpu.VMEM((2, span, width), BF16),
            pltpu.VMEM((2, nz, out_cols, cut), BF16),
            pltpu.VMEM((2 * heads, key_size, value_size), F32),
            pltpu.VMEM((2, 4 * heads, key_size), BF16),
            pltpu.VMEM((2, 4 * heads, value_size), BF16),
            pltpu.SMEM((heads,), F32),
            pltpu.SMEM((2,), jnp.int32),
            pltpu.SMEM((2,), jnp.int32),
            pltpu.VMEM((width,), BF16),
            pltpu.VMEM((1, width), F32),
            pltpu.VMEM((2, 2, 4 * heads, key_size), F32),
            pltpu.VMEM((2 * heads, key_size, value_size), BF16),
            pltpu.VMEM((2, nz, ny, depth, seqs), BF16),
            pltpu.VMEM((128 * ny, 2 * key_size + 2 * value_size), BF16),
            pltpu.VMEM((2, 4 * seqs, 4 * seqs), BF16),
            pltpu.VMEM((2, nz, 2, 2 * ny, 128), BF16),
            pltpu.VMEM((2, nz, 2, 2 * ny, 128), BF16),
            pltpu.VMEM((nz * 8 * ny, 128), F32),
            pltpu.VMEM((ny, 2, 2, 2 * nz, 128), BF16),
            pltpu.VMEM((ny, 2, 2, 2 * nz, 128), BF16),
            pltpu.VMEM((value_size // 128, count, 128), F32),
            pltpu.VMEM((2, 8, cut), BF16),
            pltpu.VMEM((2, nz, 8, cut), BF16),
            pltpu.VMEM((2, nz, 2, out_cols // 4, 128), BF16),
            pltpu.VMEM((2, 2, nz, out_cols // 4, 128), BF16),
            dma((23,)),
            dma((2, nz, ny)),
            dma((2, max(nz, ny), TorusGather.groups)),
            dma((2, max(nz, ny))),
            dma((2, 2, nz // 2, TorusGather.groups)),
            dma((2, nz)),
            dma((2, 2, nz // 2)),
            dma((2, 2, nz)),
            dma((2, 2, nz)),
            dma((2,)),
            dma((2,)),
            dma((2, nz)),
            dma((2, nz)),
            dma((2, nz, 2)),
            dma((2, 2, nz)),
            dma((4,)),
            dma((2, nz)),
            dma((2, nz)),
            dma((ny, 2)),
            dma((ny, 2)),
        ],
        compiler_params=pltpu.CompilerParams(
            collective_id=0, has_side_effects=True, vmem_limit_bytes=48 * 1024 * 1024
        ),
    )(
        *map(
            in_hbm,
            (
                tokens.transpose(1, 2, 0),
                query_weight.T,
                key_weight.T,
                value_weight.T,
                gate_weight.T,
                out_weight.T,
                prior_state.reshape(2 * heads, key_size, value_size),
                last_keys.reshape(2, 4 * heads, key_size),
                last_values.reshape(2, 4 * heads, value_size),
                decay_rate,
                accepted,
                lengths,
                norm_gain,
            ),
        ),
        frequency,
    )
    retained, state, new_keys, new_values = put_out(retained, state, new_keys, new_values)
    return (
        retained.transpose(2, 0, 1),
        state.reshape(prior_state.shape),
        new_keys,
        new_values,
    )


def solution(mesh):
    nz = ny = 8
    finer = Mesh(
        mesh.devices.reshape(mesh.shape["dp"], nz, ny, mesh.shape["tp"]),
        ("dp", "kv_0", "kv_1", "tp"),
    )
    return jax.shard_map(
        functools.partial(shards, mesh.shape["dp"], nz, ny),
        mesh=finer,
        in_specs=(
            P("dp", None, KV),
            P(),
            P(None, TP_KV),
            P(None, TP_KV),
            P(None, TP_KV),
            P(None, TP_KV),
            P("tp", KV),
            P("tp"),
            P(DP_KV, "tp", None, None),
            P(DP_KV, None, "tp", None),
            P(DP_KV, None, "tp", None),
            P(DP_KV),
            P(DP_KV),
        ),
        out_specs=(
            P("dp", None, KV_TP),
            P(DP_KV, "tp", None, None),
            P(DP_KV, None, "tp", None),
            P(DP_KV, None, "tp", None),
        ),
        check_vma=False,
    )
```
